32 devices in a mesh: fs: 8 (over z, y), tp: 4 (over x, core).
Axes of the slice: x: 2, y: 2, z: 4, core: 2. Of those that a mesh axis runs over, the one named last changes fastest.
Arguments:
- tokens: bfloat16 [4096, 2048], P('fs', 'tp'), may hold values from -6 to 6
- mixer_gain: float32 [2048], replicated, may hold values from 0.1 to 1.9
- recur_in: bfloat16 [2048, 1024], P('fs', 'tp'), may hold values from -0.125 to 0.125
- branch_in: bfloat16 [2048, 1024], P('fs', 'tp'), may hold values from -0.125 to 0.125
- conv_taps: bfloat16 [4, 1024], replicated, may hold values from -3 to 3
- recur_gate: bfloat16 [2, 16, 64, 64], replicated, may hold values from -0.75 to 0.75
- input_gate: bfloat16 [2, 16, 64, 64], replicated, may hold values from -0.75 to 0.75
- decay_param: float32 [2, 1024], replicated, may hold values from 3.5 to 11
- recur_gain: float32 [1024], replicated, may hold values from 0.1 to 1.9
- recur_out: bfloat16 [1024, 2048], P('tp', 'fs'), may hold values from -0.1875 to 0.1875
- mixer_post: float32 [2048], replicated, may hold values from 0.1 to 1.9
- channel_gain: float32 [2048], replicated, may hold values from 0.1 to 1.9
- hidden_gate: bfloat16 [2048, 5632], P('fs', 'tp'), may hold values from -0.125 to 0.125
- hidden_up: bfloat16 [2048, 5632], P('fs', 'tp'), may hold values from -0.125 to 0.125
- hidden_down: bfloat16 [5632, 2048], P('tp', 'fs'), may hold values from -0.078125 to 0.078125
- channel_post: float32 [2048], replicated, may hold values from 0.1 to 1.9
Outputs:
- layer_out: bfloat16 [4096, 2048], P('fs', 'tp')
The draws below stay inside these ranges and needn't reach their ends.
All inputs are finite; a program needn't handle non-finite values.
Results may differ from the reference program's by a relative error of at most 0.018.
Values may be sent and summed in bfloat16 or wider, within the bound.
A program may use at most 64 MiB of HBM per device.

```python
import math
import jax
import jax.numpy as jnp
from jax import lax

D = 2048
RNN = 1024
BLOCK = 64
CONV = 4
FF = 5632
TOK_DEV = 512
BLOCKS = 16
TOKENS = 4096
PARTS_SIZE = 4
N_FS = 8


def draw_tokens(key, part):
    base_key = jax.random.fold_in(key, 11)
    span_key = jax.random.fold_in(key, 12)
    span_count = (TOKENS + 31) // 32
    base_draw = jnp.clip(jax.random.normal(base_key, (TOKENS, D), jnp.float32), -4.0, 4.0)
    offset = jnp.clip(jax.random.normal(span_key, (span_count, D), jnp.float32), -2.0, 2.0)
    shifted = base_draw + jnp.repeat(offset, 32, axis=0)[:TOKENS]
    return shifted.astype(jnp.bfloat16)


def draw_decay_param(key, part):
    pick_key = jax.random.fold_in(key, 21)
    slow_key = jax.random.fold_in(key, 22)
    fast_key = jax.random.fold_in(key, 23)
    slow_share = 0.5
    slow_mask = jax.random.uniform(pick_key, (2, RNN), jnp.float32) < slow_share
    slow_rate = jnp.exp(jax.random.uniform(slow_key, (2, RNN), jnp.float32, math.log(0.05 / TOK_DEV), math.log(0.3 / TOK_DEV)))
    fast_rate = jnp.exp(jax.random.uniform(fast_key, (2, RNN), jnp.float32, math.log(1.0 / 400.0), math.log(1.0 / 120.0)))
    chosen = jnp.where(slow_mask, slow_rate, fast_rate)
    return (-jnp.log(jnp.expm1(chosen))).astype(jnp.float32)


def level_of(stream_key, dims, pieces, smallest, high):
    def one(axis_at, blocks):
        steps = jax.random.uniform(jax.random.fold_in(jax.random.fold_in(stream_key, 6), axis_at), (blocks,), jnp.float32, smallest / len(pieces), high / len(pieces))
        return jnp.repeat(jnp.exp(steps), dims[axis_at] // blocks).reshape((-1,) + (1,) * (len(dims) - axis_at - 1))

    level = one(*pieces[0])
    for cut in pieces[1:]:
        level = level * one(*cut)
    return level


def noise(key, extent, deviation, most, cuts=(), dtype=jnp.bfloat16):
    drawn = deviation * jax.random.normal(key, extent, jnp.float32)
    if cuts:
        drawn = drawn * level_of(key, extent, cuts, -0.22, 0.18)
    return jnp.clip(drawn, -most, most).astype(dtype)


def setup_inputs(seed: int = 0) -> dict:
    arg_keys = jax.random.split(jax.random.key(seed), 17)
    tokens = draw_tokens(jax.random.fold_in(arg_keys[16], 71), 0)
    mixer_gain = jnp.clip(1.0 + 0.18 * jax.random.normal(arg_keys[1], (D,), jnp.float32), 0.1, 1.9)
    recur_in = noise(arg_keys[2], (D, RNN), D ** -0.5, 0.125, ((0, 8), (1, 4)))
    branch_in = noise(arg_keys[3], (D, RNN), D ** -0.5, 0.125, ((0, 8), (1, 4)))
    conv_taps = noise(arg_keys[4], (CONV, RNN), CONV ** -0.5, 3.0)
    recur_gate = noise(arg_keys[5], (2, BLOCKS, BLOCK, BLOCK), BLOCK ** -0.5, 0.75)
    input_gate = noise(arg_keys[6], (2, BLOCKS, BLOCK, BLOCK), BLOCK ** -0.5, 0.75)
    decay_param = draw_decay_param(jax.random.fold_in(arg_keys[16], 71), 0)
    recur_gain = jnp.clip(1.0 + 0.18 * jax.random.normal(arg_keys[8], (RNN,), jnp.float32), 0.1, 1.9)
    recur_out = noise(arg_keys[9], (RNN, D), RNN ** -0.5, 0.1875, ((0, 4), (1, 8)))
    mixer_post = jnp.clip(1.0 + 0.18 * jax.random.normal(arg_keys[10], (D,), jnp.float32), 0.1, 1.9)
    channel_gain = jnp.clip(1.0 + 0.18 * jax.random.normal(arg_keys[11], (D,), jnp.float32), 0.1, 1.9)
    hidden_gate = noise(arg_keys[12], (D, FF), D ** -0.5, 0.125, ((0, 8), (1, 4)))
    hidden_up = noise(arg_keys[13], (D, FF), D ** -0.5, 0.125, ((0, 8), (1, 4)))
    hidden_down = noise(arg_keys[14], (FF, D), FF ** -0.5, 0.078125, ((0, 4), (1, 8)))
    channel_post = jnp.clip(1.0 + 0.18 * jax.random.normal(arg_keys[15], (D,), jnp.float32), 0.1, 1.9)
    return {"tokens": tokens, "mixer_gain": mixer_gain, "recur_in": recur_in, "branch_in": branch_in, "conv_taps": conv_taps, "recur_gate": recur_gate, "input_gate": input_gate, "decay_param": decay_param, "recur_gain": recur_gain, "recur_out": recur_out, "mixer_post": mixer_post, "channel_gain": channel_gain, "hidden_gate": hidden_gate, "hidden_up": hidden_up, "hidden_down": hidden_down, "channel_post": channel_post}


EPS = 1e-06
SHRINK = 8.0

def rms_scale(values, gain):
    return values * lax.rsqrt(lax.optimization_barrier(jnp.mean(values * values, axis=-1, keepdims=True)) + EPS) * gain

def linear_scan(decay, inflow, reverse):

    def combine(former, latter):
        return (former[0] * latter[0], latter[0] * former[1] + latter[1])
    return lax.associative_scan(combine, (decay, inflow), axis=0, reverse=reverse)[1]

def short_conv(recur_x, taps):
    length = recur_x.shape[0]
    padded = jnp.pad(recur_x.astype(jnp.float32), ((2, 1), (0, 0)))
    total = taps[0] * padded[0:length]
    for position in range(1, taps.shape[0]):
        total = total + taps[position] * padded[position:position + length]
    return total

def recurrence(conv_out, rate_weight, inlet_weight, decay_row, reverse):
    length, width = conv_out.shape
    grouped = conv_out.reshape(length, rate_weight.shape[0], rate_weight.shape[1])
    rate = jax.nn.sigmoid(jnp.einsum('lhi,hij->lhj', grouped, rate_weight.astype(jnp.float32), precision=lax.Precision.HIGHEST).reshape(length, width))
    inlet = jax.nn.sigmoid(jnp.einsum('lhi,hij->lhj', grouped, inlet_weight.astype(jnp.float32), precision=lax.Precision.HIGHEST).reshape(length, width))
    log_decay = -SHRINK * rate * jax.nn.softplus(-decay_row)
    inflow = conv_out * inlet * jnp.sqrt(-jnp.expm1(2.0 * log_decay))
    return linear_scan(jnp.exp(log_decay), inflow, reverse)

def grouped_product(left, right, groups):
    length = left.shape[0]
    inner = left.shape[1] // groups
    left_groups = left.astype(jnp.float32).reshape(length, groups, inner)
    right_groups = right.astype(jnp.float32).reshape(groups, inner, right.shape[1])
    partial_value = jnp.einsum('lgk,gkd->gld', left_groups, right_groups, precision=lax.Precision.HIGHEST)
    rounded = lax.optimization_barrier(partial_value.astype(jnp.bfloat16))
    return lax.optimization_barrier(jnp.sum(rounded.astype(jnp.float32), axis=0))

def reference(tokens, mixer_gain, recur_in, branch_in, conv_taps, recur_gate, input_gate, decay_param, recur_gain, recur_out, mixer_post, channel_gain, hidden_gate, hidden_up, hidden_down, channel_post):
    taps = conv_taps.astype(jnp.float32)

    def one_sequence(sequence):
        seq_float = sequence.astype(jnp.float32)
        normed_in = rms_scale(seq_float, mixer_gain).astype(jnp.bfloat16)
        recur_x = jnp.dot(normed_in, recur_in, preferred_element_type=jnp.float32).astype(jnp.bfloat16)
        branch_x = jnp.dot(normed_in, branch_in, preferred_element_type=jnp.float32).astype(jnp.bfloat16)
        conv_out = short_conv(recur_x, taps)
        forward = recurrence(conv_out, recur_gate[0], input_gate[0], decay_param[0], False)
        backward = recurrence(conv_out, recur_gate[1], input_gate[1], decay_param[1], True)
        mixed = (forward + backward) * jax.nn.gelu(branch_x.astype(jnp.float32))
        recur_y = (mixed * recur_gain).astype(jnp.bfloat16)
        branch_sum = grouped_product(recur_y, recur_out, PARTS_SIZE)
        res_mid = (seq_float + rms_scale(branch_sum, mixer_post)).astype(jnp.bfloat16)
        mid_float = res_mid.astype(jnp.float32)
        channel_in = rms_scale(mid_float, channel_gain).astype(jnp.bfloat16)
        gate = jnp.dot(channel_in, hidden_gate, preferred_element_type=jnp.float32)
        up_value = jnp.dot(channel_in, hidden_up, preferred_element_type=jnp.float32)
        hidden = (jax.nn.silu(gate) * up_value).astype(jnp.bfloat16)
        hidden_sum = grouped_product(hidden, hidden_down, PARTS_SIZE)
        return (mid_float + rms_scale(hidden_sum, channel_post)).astype(jnp.bfloat16)
    result = lax.map(one_sequence, tokens.reshape(N_FS, TOK_DEV, D))
    return result.reshape(N_FS * TOK_DEV, D)
```

```python
import functools

import jax
import jax.numpy as jnp
from jax import lax
from jax.experimental import pallas as pl
from jax.experimental.pallas import tpu as pltpu
from jax.sharding import PartitionSpec as P

EPS = 1e-06
SHRINK = 8.0
CORES = 2
FLIGHT = 5


def rms_scale(values, gain):
    return values * lax.rsqrt(jnp.mean(values * values, axis=-1, keepdims=True) + EPS) * gain


def snake_order(mesh):
    count = mesh.shape["fs"]
    axis = list(mesh.axis_names).index("fs")
    line = mesh.devices.take(0, axis=1 - axis).reshape(-1)
    where = [getattr(device, "coords", None) for device in line]
    if any(spot is None for spot in where):
        return list(range(count))
    at = {}
    for index, spot in enumerate(where):
        at[(spot[2], spot[1])] = index
    depth = 1 + max(z for z, _ in at)
    width = 1 + max(y for _, y in at)
    if depth * width != count or len(at) != count or width < 2 or depth % 2:
        return list(range(count))
    order = [at[(z, 0)] for z in range(depth)]
    for back, z in enumerate(reversed(range(depth))):
        columns = range(1, width)
        order += [at[(z, y)] for y in (columns if back % 2 == 0 else reversed(columns))]
    return order


class Ring:
    def __init__(self, order):
        self.n = len(order)
        self.order = order
        n = self.n
        self.pairs = {
            1: [(order[p], order[(p + 1) % n]) for p in range(n)],
            -1: [(order[p], order[(p - 1) % n]) for p in range(n)],
        }
        place = [0] * n
        for p, index in enumerate(order):
            place[index] = p
        self.order_row = jnp.array(order, jnp.int32)
        self.here = jnp.array(place, jnp.int32)[lax.axis_index("fs")]
        self.landed = {1: [], -1: []}

    def source(self, step):
        return self.order_row[lax.rem(self.here - step + self.n, self.n)]

    def send(self, value, way):
        landed = self.landed[way]
        if len(landed) >= FLIGHT:
            value = lax.optimization_barrier((value, landed[-FLIGHT]))[0]
        value = lax.ppermute(value, "fs", self.pairs[way])
        landed.append(value)
        return value

    def gather(self, shards, ties={}, paired=False, lead=1):
        n = self.n
        found = [[(self.source(0), shard)] for shard in shards]
        heads = [{1: shard, -1: shard} for shard in shards]
        for step in range(1, n // 2 + 1):
            for index in range(len(shards)):
                for way in (1, -1):
                    steps = n // 2 if (way == lead) == (index % 2 == 0 or paired) else n - 1 - n // 2
                    if step <= steps:
                        if step in ties:
                            heads[index][way] = lax.optimization_barrier((heads[index][way], ties[step]))[0]
                        heads[index][way] = self.send(heads[index][way], way)
                        found[index].append((self.source(way * step), heads[index][way]))
        return found


def stack_rows(blocks):
    height, width = blocks[0][1].shape
    total = jnp.zeros((height * len(blocks), width), blocks[0][1].dtype)
    for source, block in blocks:
        total = lax.dynamic_update_slice(total, block, (source * height, 0))
    return total


def stack_columns(blocks):
    height, width = blocks[0][1].shape
    total = jnp.zeros((height, width * len(blocks)), blocks[0][1].dtype)
    for source, block in blocks:
        total = lax.dynamic_update_slice(total, block, (0, source * width))
    return total


def swap_cores(value, count):
    return lax.ppermute(value, "tp", [(t, t ^ 1) for t in range(count)])


def from_chip(value, shift, count):
    return lax.ppermute(value, "tp", [(t, (t + CORES * shift) % count) for t in range(count)])


def chips_shares(value, count):
    chips = count // CORES
    chip = lax.axis_index("tp") // CORES
    found = [(chip, value)]
    for shift in range(1, chips):
        found.append((lax.rem(chip - shift + chips, chips), from_chip(value, shift, count)))
    return found


def gather_features(value, count):
    core = lax.rem(lax.axis_index("tp"), CORES)
    width = value.shape[1]
    total = jnp.zeros((value.shape[0], width * count), value.dtype)
    for chip, block in chips_shares(value, count):
        other = swap_cores(block, count)
        total = lax.dynamic_update_slice(total, block, (0, (chip * CORES + core) * width))
        total = lax.dynamic_update_slice(total, other, (0, (chip * CORES + 1 - core) * width))
    return total


def sum_all(value, count):
    core = lax.rem(lax.axis_index("tp"), CORES)
    half = value.shape[1] // CORES
    keep = lax.dynamic_slice_in_dim(value, core * half, half, 1)
    give = lax.dynamic_slice_in_dim(value, (1 - core) * half, half, 1)
    chip_sum = keep.astype(jnp.float32) + swap_cores(give, count).astype(jnp.float32)
    chip_sum = chip_sum.astype(jnp.bfloat16)
    total = 0.0
    for _, block in chips_shares(chip_sum, count):
        total = total + block.astype(jnp.float32)
    mine = total.astype(jnp.bfloat16)
    other = swap_cores(mine, count)
    low = jnp.where(core == 0, mine, other)
    high = jnp.where(core == 0, other, mine)
    return jnp.concatenate([low, high], axis=1)


def sum_own(value, count):
    rank = lax.axis_index("tp")
    core = lax.rem(rank, CORES)
    chip = rank // CORES
    chips = count // CORES
    length = value.shape[0]
    width = value.shape[1] // count

    def block(chip_at, core_at):
        at = (chip_at * CORES + core_at) * width
        return lax.dynamic_slice_in_dim(value, at, width, 1)

    total = 0.0
    for shift in list(range(1, chips)) + [0]:
        target = lax.rem(chip + shift, chips)
        part = block(target, core).astype(jnp.float32)
        part = part + swap_cores(block(target, 1 - core), count).astype(jnp.float32)
        if shift:
            part = from_chip(part.astype(jnp.bfloat16), shift, count).astype(jnp.float32)
        total = total + part
    return total


def minus_expm1(value):
    series = jnp.ones_like(value)
    for order in range(9, 1, -1):
        series = 1.0 + value * (1.0 / order) * series
    return jnp.where(value > -0.5, -value * series, 1.0 - jnp.exp(value))


def scan_block(decay, inflow, reverse):
    length = decay.shape[0]
    row = lax.broadcasted_iota(jnp.int32, decay.shape, 0)
    reach = 1
    while reach < length:
        if reverse:
            inside = row < length - reach
            turn = length - reach
        else:
            inside = row >= reach
            turn = reach
        before_inflow = jnp.where(inside, pltpu.roll(inflow, turn, 0), 0.0)
        inflow = inflow + decay * before_inflow
        if 2 * reach < length:
            decay = decay * jnp.where(inside, pltpu.roll(decay, turn, 0), 1.0)
        reach *= 2
    return inflow


def mixer_kernel(recur_ref, branch_ref, taps_ref, gate_ref, decay_ref, gain_ref, out_ref):
    recur = recur_ref[...].astype(jnp.float32)
    length, width = recur.shape
    row = lax.broadcasted_iota(jnp.int32, recur.shape, 0)
    taps = taps_ref[...]
    conv = taps[2:3] * recur
    for tap, shift in ((0, 2), (1, 1), (3, length - 1)):
        inside = row < length - 1 if tap == 3 else row >= shift
        conv = conv + taps[tap : tap + 1] * jnp.where(inside, pltpu.roll(recur, shift, 0), 0.0)
    first = conv.astype(jnp.bfloat16)
    rest = conv - first.astype(jnp.float32)
    second = rest.astype(jnp.bfloat16)
    third = (rest - second.astype(jnp.float32)).astype(jnp.bfloat16)
    total = None
    for direction in range(2):
        logits = []
        for kind in range(2):
            weight = gate_ref[0, :, pl.ds((direction * 2 + kind) * width, width)]
            logits.append(
                jnp.dot(third, weight, preferred_element_type=jnp.float32)
                + jnp.dot(second, weight, preferred_element_type=jnp.float32)
                + jnp.dot(first, weight, preferred_element_type=jnp.float32)
            )
        rate = 1.0 / (1.0 + jnp.exp(-logits[0]))
        inlet = 1.0 / (1.0 + jnp.exp(-logits[1]))
        log_decay = rate * decay_ref[direction : direction + 1, :]
        inflow = conv * inlet * jnp.sqrt(minus_expm1(2.0 * log_decay))
        state = scan_block(jnp.exp(log_decay), inflow, direction == 1)
        total = state if total is None else total + state
    branch = branch_ref[...].astype(jnp.float32)
    inner = 0.7978845608028654 * (branch + 0.044715 * (branch * branch * branch))
    gelu = branch * (0.5 * (1.0 + jnp.tanh(inner)))
    out_ref[...] = (total * gelu * gain_ref[...]).astype(jnp.bfloat16)


def mixer(both_x, taps, rate_own, inlet_own, decay_own, gain_own):
    length, channels = both_x.shape[0], both_x.shape[1] // 2
    group = rate_own.shape[-1]
    lanes = min(channels, 2 * group)
    blocks = channels // lanes
    per = lanes // group

    def dense(weight):
        spread = weight.reshape(2, blocks, per, group, 1, group) * jnp.eye(per, dtype=weight.dtype)[:, None, :, None]
        return spread.reshape(2, blocks, lanes, lanes)

    both = jnp.stack([dense(rate_own), dense(inlet_own)], axis=1)
    gates = both.transpose(2, 3, 0, 1, 4).reshape(blocks, lanes, 4 * lanes)
    slope = -SHRINK * jax.nn.softplus(-decay_own)
    column = lambda j: (0, j)
    return pl.pallas_call(
        mixer_kernel,
        grid=(blocks,),
        out_shape=jax.ShapeDtypeStruct((length, channels), jnp.bfloat16),
        in_specs=[
            pl.BlockSpec((length, lanes), column),
            pl.BlockSpec((length, lanes), lambda j: (0, blocks + j)),
            pl.BlockSpec((taps.shape[0], lanes), column),
            pl.BlockSpec((1, lanes, 4 * lanes), lambda j: (j, 0, 0)),
            pl.BlockSpec((2, lanes), column),
            pl.BlockSpec((1, lanes), column),
        ],
        out_specs=pl.BlockSpec((length, lanes), column),
        cost_estimate=pl.CostEstimate(flops=int(3e9), bytes_accessed=2**20, transcendentals=2**21),
        compiler_params=pltpu.CompilerParams(vmem_limit_bytes=24 * 2**20),
    )(both_x, both_x, taps, gates, slope, gain_own.reshape(1, channels))


def on_device(
    order,
    tp_count,
    tokens,
    mixer_gain,
    recur_in,
    branch_in,
    conv_taps,
    recur_gate,
    input_gate,
    decay_param,
    recur_gain,
    recur_out,
    mixer_post,
    channel_gain,
    hidden_gate,
    hidden_up,
    hidden_down,
    channel_post,
):
    rank_tp = lax.axis_index("tp")
    feature_width = tokens.shape[1]
    model_width = mixer_gain.shape[0]
    channel_width = recur_in.shape[1]
    group_count = channel_width // recur_gate.shape[-1]
    feature_start = rank_tp * feature_width
    channel_start = rank_tp * channel_width

    ring = Ring(order)
    packed = jnp.concatenate([recur_in, branch_in, recur_out.reshape(recur_in.shape)], axis=1)
    mix_blocks, gate_blocks = ring.gather([packed, hidden_gate])
    in_blocks = [(source, block[:, : 2 * channel_width]) for source, block in mix_blocks]
    out_blocks = [
        (source, block[:, 2 * channel_width :].reshape(recur_out.shape)) for source, block in mix_blocks
    ]

    gathered_in = gather_features(tokens, tp_count)
    gathered_float = gathered_in.astype(jnp.float32)
    normed_in = rms_scale(gathered_float, mixer_gain).astype(jnp.bfloat16)
    both_x = jnp.dot(normed_in, stack_rows(in_blocks), preferred_element_type=jnp.float32).astype(jnp.bfloat16)

    taps = lax.dynamic_slice_in_dim(conv_taps, channel_start, channel_width, 1).astype(jnp.float32)
    group_start = rank_tp * group_count
    rate_own = lax.dynamic_slice_in_dim(recur_gate, group_start, group_count, 1)
    inlet_own = lax.dynamic_slice_in_dim(input_gate, group_start, group_count, 1)
    decay_own = lax.dynamic_slice_in_dim(decay_param, channel_start, channel_width, 1)
    gain_own = lax.dynamic_slice_in_dim(recur_gain, channel_start, channel_width, 0)
    recur_y = mixer(both_x, taps, rate_own, inlet_own, decay_own, gain_own)

    (up_blocks,) = ring.gather([hidden_up], lead=-1)
    branch_part = jnp.dot(recur_y, stack_columns(out_blocks), preferred_element_type=jnp.float32)
    branch_sum = sum_all(branch_part.astype(jnp.bfloat16), tp_count).astype(jnp.float32)
    mid_full = (gathered_float + rms_scale(branch_sum, mixer_post)).astype(jnp.bfloat16)
    mid_own = lax.dynamic_slice_in_dim(mid_full, feature_start, feature_width, 1)
    channel_in = rms_scale(mid_full.astype(jnp.float32), channel_gain).astype(jnp.bfloat16)

    gate_total = jnp.dot(channel_in, stack_rows(gate_blocks), preferred_element_type=jnp.float32)
    up_total = jnp.dot(channel_in, stack_rows(up_blocks), preferred_element_type=jnp.float32)
    hidden = (jax.nn.silu(gate_total) * up_total).astype(jnp.bfloat16)

    cut = max(hidden_down.shape[0] // 256, 1) * 128
    low_blocks, high_blocks = ring.gather(
        [hidden_down[:cut], hidden_down[cut:]], {4: hidden}, True
    )
    part_blocks = []
    for (source, low), (_, high) in zip(low_blocks, high_blocks):
        part = jnp.dot(hidden[:, :cut], low, preferred_element_type=jnp.float32)
        part = part + jnp.dot(hidden[:, cut:], high, preferred_element_type=jnp.float32)
        part_blocks.append((source, part.astype(jnp.bfloat16)))
    hidden_part = stack_columns(part_blocks)
    hidden_own = sum_own(hidden_part, tp_count)
    energy_own = jnp.sum(hidden_own * hidden_own, axis=1).reshape(-1, 128)
    hidden_energy = lax.psum(energy_own, "tp").reshape(-1)
    close_own = lax.dynamic_slice_in_dim(channel_post, feature_start, feature_width, 0)
    return (
        mid_own.astype(jnp.float32)
        + hidden_own * lax.rsqrt(hidden_energy / model_width + EPS)[:, None] * close_own
    ).astype(jnp.bfloat16)


PLANES = 4
ROWS = 2
CHIPS = 2
MESH = pl.DeviceIdType.MESH
LANES = 128


def pooled_fits(mesh, args):
    if mesh.shape["fs"] != PLANES * ROWS or mesh.shape["tp"] != CHIPS * CORES:
        return False
    spots = [getattr(device, "coords", None) for device in mesh.devices.reshape(-1)]
    if all(spot is not None for spot in spots):
        if list(mesh.axis_names) != ["fs", "tp"]:
            return False
        at = mesh.devices
        for f in range(PLANES * ROWS):
            for t in range(CHIPS * CORES):
                if tuple(at[f, t].coords) != (t // CORES, f % ROWS, f // ROWS):
                    return False
    tokens, gate, down, recur_in, recur_out = args[0], args[12], args[14], args[2], args[9]
    half = gate.shape[1] // 2
    return (
        tokens.shape[1] % LANES == 0
        and tokens.shape[0] % 16 == 0
        and gate.shape[0] % 16 == 0
        and half % LANES == LANES // 2
        and down.shape[0] == gate.shape[1]
        and recur_in.shape[1] % LANES == 0
        and recur_out.shape[1] % LANES == 0
        and LANES % args[5].shape[-1] == 0
    )


class Wires:
    def __init__(self, sends, lands, nobody):
        self.sends = sends
        self.lands = lands
        self.nobody = nobody
        self.names = {}
        self.started = []

    def index(self, name):
        return self.names.setdefault(name, len(self.names))

    def send(self, name, source, target, to, land=None, only=None):
        copy = pltpu.make_async_remote_copy(
            src_ref=source,
            dst_ref=target,
            send_sem=self.sends.at[self.index(name)],
            recv_sem=self.lands.at[self.index(land or name)],
            device_id=to,
            device_id_type=MESH,
        )
        guarded(only, copy.start)
        self.started.append((only, copy))

    def wait(self, name, target):
        at = self.lands.at[self.index(name)]
        pltpu.make_async_remote_copy(
            src_ref=target,
            dst_ref=target,
            send_sem=at,
            recv_sem=at,
            device_id=self.nobody,
            device_id_type=MESH,
        ).wait_recv()

    def finish(self):
        for only, copy in self.started:
            guarded(only, copy.wait_send)


def guarded(only, action):
    if only is None:
        action()
    else:
        pl.when(only)(action)


def scan_pair(conv, logits, slope, reverse):
    rate = 1.0 / (1.0 + jnp.exp(-logits[0]))
    inlet = 1.0 / (1.0 + jnp.exp(-logits[1]))
    log_decay = rate * slope
    inflow = conv * inlet * jnp.sqrt(minus_expm1(2.0 * log_decay))
    return scan_block(jnp.exp(log_decay), inflow, reverse)


def log_one_plus(value):
    total = 1.0 + value
    exact = total == 1.0
    return jnp.where(exact, value, jnp.log(total) * (value / jnp.where(exact, 1.0, total - 1.0)))


def pooled_kernel(
    tokens,
    mixer_gain,
    recur_in,
    branch_in,
    conv_taps,
    recur_gate,
    input_gate,
    decay_param,
    recur_gain,
    recur_out,
    mixer_post,
    channel_gain,
    hidden_gate,
    hidden_up,
    hidden_down,
    channel_post,
    out,
    tok,
    normed,
    w_in,
    both_x,
    gates_raw,
    gates,
    recur_all,
    w_out,
    branch,
    mid,
    channel_in,
    edge,
    w_gate_up,
    other_gate_up,
    hidden,
    w_down,
    other_down,
    part,
    part_in,
    chip_send,
    chip_in,
    own_sum,
    plane_send,
    plane_in,
    energy,
    sends,
    lands,
    local,
):
    f = lax.axis_index("fs")
    t = lax.axis_index("tp")
    z, y = lax.div(f, ROWS), lax.rem(f, ROWS)
    x, c = lax.div(t, CORES), lax.rem(t, CORES)
    zi, zp = lax.rem(z, 2), lax.div(z, 2)
    planes = [z, z + 1 - 2 * zi, lax.rem(z + 2, PLANES), PLANES - 1 - z]
    is_mid = lax.div(lax.rem(z + 1, PLANES), 2) == 1
    is_end = lax.div(lax.rem(z + 1, PLANES), 2) == 0
    length, width = tokens.shape
    depth = recur_in.shape[0]
    channels = recur_in.shape[1]
    units = hidden_gate.shape[1]
    half = units // 2
    wide = half // LANES * LANES
    narrow = half - wide
    full = wide // LANES
    model = tok.shape[0] * width
    group = recur_gate.shape[-1]
    blocks = PLANES * ROWS

    def device(plane, row, chip, core):
        return {"fs": plane * ROWS + row, "tp": chip * CORES + core}

    def block(k, row):
        return planes[k] * ROWS + row

    near_y = device(z, 1 - y, x, c)
    near_x = device(z, y, 1 - x, c)
    far_x = device(z, y, 1 - x, 1 - c)
    near_c = device(z, y, x, 1 - c)
    plane_of = [None] + [device(planes[k], y, x, c) for k in (1, 2, 3)]
    t_c = x * CORES + 1 - c
    t_x = (1 - x) * CORES + c
    t_xc = (1 - x) * CORES + 1 - c
    wires = Wires(sends, lands, near_c)
    rows_of = lambda at, size: pl.ds(pl.multiple_of(at * size, size), size)

    moves = {}

    def move(name, source, target):
        copy = pltpu.make_async_copy(source, target, local.at[len(moves)])
        copy.start()
        moves[name] = copy

    def here(prefix):
        for name, copy in moves.items():
            if name.startswith(prefix):
                copy.wait()

    move("io0", recur_in, w_in.at[rows_of(f, depth), pl.ds(0, channels)])
    move("io1", branch_in, w_in.at[rows_of(f, depth), pl.ds(channels, channels)])
    move("io2", recur_out, w_out.at[f, rows_of(t, channels), :])
    move("tok", tokens, tok.at[t])
    columns = lambda at: pl.ds(pl.multiple_of(at, LANES), LANES)
    for side, target, row_at, parity in (("a", w_gate_up, f, zi), ("b", other_gate_up, 0, 1 - zi)):
        for n in range(full):
            start = parity * (units - wide) + n * LANES
            for m, weight in enumerate((hidden_gate, hidden_up)):
                move(
                    f"gu{side}{n}{m}",
                    weight.at[:, columns(start)],
                    target.at[rows_of(row_at, depth), pl.ds((2 * n + m) * LANES, LANES)],
                )
    move("gum0", hidden_gate.at[:, pl.ds(wide, LANES)], edge.at[0])
    move("gum1", hidden_up.at[:, pl.ds(wide, LANES)], edge.at[1])
    group_count = channels // group
    move("gate0", recur_gate.at[:, rows_of(t, group_count)], gates_raw.at[0])
    move("gate1", input_gate.at[:, rows_of(t, group_count)], gates_raw.at[1])
    for side, target, parity in (("a", w_down.at[f], zi), ("b", other_down, 1 - zi)):
        wide_at = pl.multiple_of(parity * (units - wide), 2 * narrow)
        narrow_at = pl.multiple_of(wide + parity * narrow, narrow)
        move(f"dn{side}0", hidden_down.at[pl.ds(wide_at, wide), :], target.at[pl.ds(0, wide), :])
        move(f"dn{side}1", hidden_down.at[pl.ds(narrow_at, narrow), :], target.at[pl.ds(wide, narrow), :])

    barrier = pltpu.get_barrier_semaphore()
    peers = [near_y, near_x, far_x, near_c] + plane_of[1:]
    for peer in peers:
        pl.semaphore_signal(barrier, inc=1, device_id=peer, device_id_type=MESH)
    pl.semaphore_wait(barrier, len(peers))

    def in_slot(k, row):
        return w_in.at[rows_of(block(k, row), depth), :]

    def out_slot(k, row):
        return w_out.at[block(k, row), rows_of(t, channels), :]

    part_rows = depth // 2

    def gate_slot(k, row, piece):
        at = pl.multiple_of(block(k, row) * depth + piece * part_rows, part_rows)
        return w_gate_up.at[pl.ds(at, part_rows), :]

    def other_slot(piece):
        return other_gate_up.at[pl.ds(piece * part_rows, part_rows), :]

    def down_slot(k, row):
        return w_down.at[block(k, row), pl.ds(0, half), :]

    down_other = other_down

    def mixer_to_y(k):
        wires.send(f"iy{k}", in_slot(k, y), in_slot(k, y), near_y)
        wires.send(f"oy{k}", out_slot(k, y), out_slot(k, y), near_y)

    def mixer_to_x(k, row, tag):
        wires.send(f"ox{tag}{k}", out_slot(k, row), out_slot(k, row), near_x)

    def mixer_to_z(name, k, to, land, only=None):
        wires.send("i" + name, in_slot(k, y), in_slot(k, y), to, f"iz{land}", only)
        wires.send("o" + name, out_slot(k, y), out_slot(k, y), to, f"oz{land}", only)

    def mixer_wait(k):
        wires.wait(f"iz{k}", in_slot(k, y))
        wires.wait(f"oz{k}", out_slot(k, y))

    def gate_own_to_z(piece, which, only):
        if which == 1:
            wires.send(f"g{piece}s1", gate_slot(0, y, piece), gate_slot(0, y, piece), plane_of[2], f"gz{piece}2", only)
        else:
            k = 1 if which == 2 else 3
            source = other_slot(piece)
            wires.send(f"g{piece}s{which}", source, gate_slot(0, y, piece), plane_of[k], f"gz{piece}{k}", only)

    def down_own_to_z(which, only):
        if which == 1:
            wires.send("ds1", down_slot(0, y), down_slot(0, y), plane_of[2], "dz2", only)
        else:
            k = 1 if which == 2 else 3
            wires.send(f"ds{which}", down_other, down_slot(0, y), plane_of[k], f"dz{k}", only)

    def gate_to_y(k, piece):
        wires.send(f"gy{piece}{k}", gate_slot(k, y, piece), gate_slot(k, y, piece), near_y)

    def down_to_y(k):
        wires.send(f"dy{k}", down_slot(k, y), down_slot(k, y), near_y)

    def gate_pass(k, piece):
        wires.wait(f"gz{piece}{k}", gate_slot(k, y, piece))
        if k == 1:
            wires.send(
                f"g{piece}r", gate_slot(1, y, piece), gate_slot(1, y, piece), plane_of[2], f"gz{piece}3", is_mid
            )
        gate_to_y(k, piece)

    def down_pass(k):
        wires.wait(f"dz{k}", down_slot(k, y))
        if k == 1:
            wires.send("dr", down_slot(1, y), down_slot(1, y), plane_of[2], "dz3", is_mid)
        down_to_y(k)

    here("io")
    mixer_to_y(0)
    mixer_to_z("z1", 0, plane_of[1], 1)
    mixer_to_z("z3", 0, plane_of[3], 3, is_mid)
    here("tok")
    wires.send("tc", tok.at[t], tok.at[t], near_c)
    wires.send("tx", tok.at[t], tok.at[t], near_x)
    mixer_to_x(0, y, "a")

    here("gum")
    lane = lax.broadcasted_iota(jnp.int32, edge.shape[1:], 1)
    edge_gate = edge[0].astype(jnp.float32)
    edge_up = edge[1].astype(jnp.float32)
    low = jnp.where(lane < narrow, edge_gate, pltpu.roll(edge_up, narrow, 1))
    high = jnp.where(lane < narrow, pltpu.roll(edge_gate, narrow, 1), edge_up)
    odd = zi == 1
    edge_at = pl.ds(2 * wide, LANES)
    w_gate_up[rows_of(f, depth), edge_at] = jnp.where(odd, high, low).astype(jnp.bfloat16)
    other_gate_up[:, edge_at] = jnp.where(odd, low, high).astype(jnp.bfloat16)
    w_down[:, pl.ds(half, LANES - narrow), :] = jnp.zeros((blocks, LANES - narrow, w_down.shape[2]), jnp.bfloat16)
    here("gua")
    here("gub")

    gate_to_y(0, 0)
    gate_own_to_z(0, 2, None)
    gate_own_to_z(0, 3, is_mid)
    gate_own_to_z(0, 1, is_end)

    here("gate")
    per = LANES // group
    runs = channels // LANES
    for j in range(runs):
        for direction in range(2):
            for kind in range(2):
                dense = None
                for a in range(per):
                    spread_row = lax.broadcasted_iota(jnp.int32, (group, LANES), 0)
                    spread_lane = lax.broadcasted_iota(jnp.int32, (group, LANES), 1)
                    spread = (spread_lane == spread_row + a * group).astype(jnp.bfloat16)
                    lift_row = lax.broadcasted_iota(jnp.int32, (LANES, group), 0)
                    lift_lane = lax.broadcasted_iota(jnp.int32, (LANES, group), 1)
                    lift = (lift_row == lift_lane + a * group).astype(jnp.bfloat16)
                    block_map = gates_raw[kind, direction, j * per + a]
                    block_map = jnp.dot(block_map, spread, preferred_element_type=jnp.float32).astype(jnp.bfloat16)
                    block_map = jnp.dot(lift, block_map, preferred_element_type=jnp.float32)
                    dense = block_map if dense is None else dense + block_map
                gates[j, :, pl.ds((direction * 2 + kind) * LANES, LANES)] = dense.astype(jnp.bfloat16)

    wires.wait("tx", tok.at[t_x])
    wires.send("txc", tok.at[t_x], tok.at[t_x], near_c)

    mixer_wait(1)
    mixer_to_z("r1", 1, plane_of[3], 2, is_mid)
    mixer_to_y(1)
    mixer_to_x(1, y, "a")

    wires.wait("tc", tok.at[t_c])
    wires.wait("txc", tok.at[t_xc])
    fine = 16

    @pl.loop(0, length // fine)
    def _(r):
        rows = rows_of(r, fine)
        values = jnp.concatenate([tok[i, rows, :] for i in range(tok.shape[0])], axis=1).astype(jnp.float32)
        normed[rows, :] = rms_scale(values, mixer_gain[...]).astype(jnp.bfloat16)

    def mid_three():
        wires.wait("iz3", in_slot(3, y))
        wires.wait("oz3", out_slot(3, y))

    def end_two():
        wires.wait("iz2", in_slot(2, y))
        wires.wait("oz2", out_slot(2, y))

    pl.when(is_mid)(mid_three)
    mixer_to_z("r3", 3, plane_of[1], 2, is_mid)
    gate_own_to_z(0, 1, is_mid)
    gate_own_to_z(1, 2, None)
    gate_own_to_z(1, 1, is_end)
    pl.when(is_end)(end_two)
    second = jnp.where(is_mid, planes[3], planes[2]) * ROWS + y
    third = jnp.where(is_mid, planes[2], planes[3]) * ROWS + y

    def mixer_late(at, tag):
        slot_in = w_in.at[rows_of(at, depth), :]
        slot_out = w_out.at[at, rows_of(t, channels), :]
        wires.send(f"iy{tag}", slot_in, slot_in, near_y)
        wires.send(f"oy{tag}", slot_out, slot_out, near_y)
        wires.send(f"oxa{tag}", slot_out, slot_out, near_x)

    def late_wait_y(at, tag):
        other = at - y + 1 - y
        wires.wait(f"iy{tag}", w_in.at[rows_of(other, depth), :])
        wires.wait(f"oy{tag}", w_out.at[other, rows_of(t, channels), :])
        slot = w_out.at[other, rows_of(t, channels), :]
        wires.send(f"oxb{tag}", slot, slot, near_x)

    mixer_late(second, "s")
    for k in (0, 1):
        wires.wait(f"iy{k}", in_slot(k, 1 - y))
        wires.wait(f"oy{k}", out_slot(k, 1 - y))
        mixer_to_x(k, 1 - y, "b")

    pl.when(is_mid)(end_two)
    mixer_to_z("r2", 2, plane_of[1], 3, is_mid)
    gate_own_to_z(1, 3, is_mid)
    gate_own_to_z(1, 1, is_mid)
    pl.when(is_end)(mid_three)
    mixer_late(third, "t")
    gate_to_y(0, 1)
    here("dn")
    gate_pass(1, 0)
    late_wait_y(second, "s")
    late_wait_y(third, "t")
    wires.send("oc1", w_out.at[:, rows_of(t, channels), :], w_out.at[:, rows_of(t, channels), :], near_c)

    @pl.loop(0, 2)
    def _(j):
        at = rows_of(j, channels)
        product = jnp.dot(normed[...], w_in[:, at], preferred_element_type=jnp.float32)
        both_x[:, at] = product.astype(jnp.bfloat16)

    gate_pass(2, 0)

    own_channels = pl.multiple_of(t * channels, LANES)

    @pl.loop(0, runs)
    def _(j):
        at = pl.ds(pl.multiple_of(j * LANES, LANES), LANES)
        gate_at = pl.ds(pl.multiple_of(channels + j * LANES, LANES), LANES)
        table_at = pl.ds(pl.multiple_of(own_channels + j * LANES, LANES), LANES)
        recur = both_x[:, at].astype(jnp.float32)
        row = lax.broadcasted_iota(jnp.int32, recur.shape, 0)
        taps = conv_taps[:, table_at].astype(jnp.float32)
        conv = taps[2:3] * recur
        for tap, shift in ((0, 2), (1, 1), (3, length - 1)):
            inside = row < length - 1 if tap == 3 else row >= shift
            conv = conv + taps[tap : tap + 1] * jnp.where(inside, pltpu.roll(recur, shift, 0), 0.0)
        first = conv.astype(jnp.bfloat16)
        rest = conv - first.astype(jnp.float32)
        second_part = rest.astype(jnp.bfloat16)
        third_part = (rest - second_part.astype(jnp.float32)).astype(jnp.bfloat16)
        decay = decay_param[:, table_at]
        slope = -SHRINK * (jnp.maximum(-decay, 0.0) + log_one_plus(jnp.exp(-jnp.abs(decay))))
        total = None
        for direction in range(2):
            logits = []
            for kind in range(2):
                weight = gates[j, :, pl.ds((direction * 2 + kind) * LANES, LANES)]
                logits.append(
                    jnp.dot(third_part, weight, preferred_element_type=jnp.float32)
                    + jnp.dot(second_part, weight, preferred_element_type=jnp.float32)
                    + jnp.dot(first, weight, preferred_element_type=jnp.float32)
                )
            state = scan_pair(conv, logits, slope[direction : direction + 1], direction == 1)
            total = state if total is None else total + state
        value = both_x[:, gate_at].astype(jnp.float32)
        inner = 0.7978845608028654 * (value + 0.044715 * (value * value * value))
        gelu = value * (0.5 * (1.0 + jnp.tanh(inner)))
        recur_all[:, table_at] = (total * gelu * recur_gain[:, table_at]).astype(jnp.bfloat16)

    mine = recur_all.at[:, rows_of(t, channels)]
    wires.send("rx", mine, mine, near_x)
    wires.send("rc", mine, mine, near_c)
    gate_pass(3, 0)
    for k, tag in ((0, "b0"), (1, "b1"), (0, "a0"), (1, "a1")):
        slot = w_out.at[block(k, y if tag[0] == "a" else 1 - y), rows_of(t_x, channels), :]
        wires.wait("ox" + tag, slot)
    for tag, at in (("s", second), ("t", third)):
        wires.wait("oxa" + tag, w_out.at[at, rows_of(t_x, channels), :])
        wires.wait("oxb" + tag, w_out.at[at + 1 - 2 * y, rows_of(t_x, channels), :])
    wires.send("oc2", w_out.at[:, rows_of(t_x, channels), :], w_out.at[:, rows_of(t_x, channels), :], near_c)
    theirs = recur_all.at[:, rows_of(t_x, channels)]
    wires.wait("rx", theirs)
    wires.send("rxc", theirs, theirs, near_c)
    gate_pass(1, 1)
    wires.wait("oc1", w_out.at[:, rows_of(t_c, channels), :])
    wires.wait("oc2", w_out.at[:, rows_of(t_xc, channels), :])
    wires.wait("rc", recur_all.at[:, rows_of(t_c, channels)])
    wires.wait("rxc", recur_all.at[:, rows_of(t_xc, channels)])

    @pl.loop(0, blocks)
    def _(b):
        branch[:, rows_of(b, depth)] = jnp.dot(recur_all[...], w_out[b], preferred_element_type=jnp.float32)

    @pl.loop(0, length // fine)
    def _(r):
        rows = rows_of(r, fine)
        values = jnp.concatenate([tok[i, rows, :] for i in range(tok.shape[0])], axis=1).astype(jnp.float32)
        middle = (values + rms_scale(branch[rows, :], mixer_post[...])).astype(jnp.bfloat16)
        mid[rows, :] = middle
        channel_in[0, rows, :] = rms_scale(middle.astype(jnp.float32), channel_gain[...]).astype(jnp.bfloat16)

    def quarter(s, at):
        return channel_in.at[s, :, rows_of(at, width)]

    wires.send("cz", quarter(0, t), quarter(1, t), plane_of[1])
    gate_pass(2, 1)
    gate_pass(3, 1)
    down_to_y(0)
    down_own_to_z(2, None)
    down_own_to_z(3, is_mid)
    down_own_to_z(1, None)
    wires.wait("cz", quarter(1, t))
    wires.send("cx", quarter(1, t), quarter(1, t), near_x)
    wires.send("cc1", quarter(1, t), quarter(1, t), near_c)
    down_pass(1)
    wires.wait("cx", quarter(1, t_x))
    wires.send("cc2", quarter(1, t_x), quarter(1, t_x), near_c)
    down_pass(2)
    wires.wait("cc1", quarter(1, t_c))
    wires.wait("cc2", quarter(1, t_xc))
    for k in range(PLANES):
        for piece in range(2):
            wires.wait(f"gy{piece}{k}", gate_slot(k, 1 - y, piece))

    @pl.loop(0, full)
    def _(n):
        at = pl.ds(pl.multiple_of(n * 2 * LANES, 2 * LANES), 2 * LANES)
        store = pl.ds(pl.multiple_of(n * LANES, LANES), LANES)
        for s in range(2):
            product = jnp.dot(channel_in[s], w_gate_up[:, at], preferred_element_type=jnp.float32)
            gate_value, up_value = product[:, :LANES], product[:, LANES:]
            hidden[s, :, store] = (jax.nn.silu(gate_value) * up_value).astype(jnp.bfloat16)

    lane_tail = lax.broadcasted_iota(jnp.int32, (length, LANES), 1)
    for s in range(2):
        product = jnp.dot(channel_in[s], w_gate_up[:, edge_at], preferred_element_type=jnp.float32)
        value = jax.nn.silu(product) * pltpu.roll(product, narrow, 1)
        hidden[s, :, pl.ds(wide, LANES)] = jnp.where(lane_tail < narrow, value, 0.0).astype(jnp.bfloat16)

    down_pass(3)

    def products(k):
        for row in range(ROWS):
            at = pl.ds(row * depth, depth)
            for s in range(2):
                value = jnp.dot(hidden[s], w_down[planes[k] * ROWS + row], preferred_element_type=jnp.float32)
                part[k, s, :, at] = value.astype(jnp.bfloat16)

    def give(k):
        wires.send(f"pc{k}", part.at[k], part_in.at[k // 2], near_c, f"pc{k // 2}", lax.rem(zi + c, 2) != k % 2)

    keeps = lambda k: lax.rem(zi + c, 2) == k % 2
    owns = lambda k: lax.rem(zp + x, 2) == k // 2
    both = lambda k: jnp.logical_and(keeps(k), owns(k))
    passes = lambda k: jnp.logical_and(keeps(k), jnp.logical_not(owns(k)))

    def chip_sum(k):
        def run():
            wires.wait(f"pc{k // 2}", part_in.at[k // 2])
            for s in range(2):
                chip_send[s] = (part[k, s].astype(jnp.float32) + part_in[k // 2, s].astype(jnp.float32)).astype(
                    jnp.bfloat16
                )

        pl.when(passes(k))(run)
        wires.send(f"px{k}", chip_send, chip_in, near_x, "px", passes(k))

    def all_sum(k):
        def run():
            wires.wait(f"pc{k // 2}", part_in.at[k // 2])
            wires.wait("px", chip_in)
            sums = [
                part[k, s].astype(jnp.float32)
                + part_in[k // 2, s].astype(jnp.float32)
                + chip_in[s].astype(jnp.float32)
                for s in range(2)
            ]
            own_sum[...] = sums[0]
            plane_send[...] = sums[1].astype(jnp.bfloat16)

        pl.when(both(k))(run)
        wires.send(f"pz{k}", plane_send, plane_in, plane_of[1], "pz", both(k))

    for k in range(PLANES):
        wires.wait(f"dy{k}", down_slot(k, 1 - y))
        products(k)
        give(k)
        if k > 0:
            chip_sum(k - 1)
        if k > 1:
            all_sum(k - 2)
    chip_sum(PLANES - 1)
    all_sum(PLANES - 2)
    all_sum(PLANES - 1)

    wires.wait("pz", plane_in)
    total = own_sum[...] + plane_in[...].astype(jnp.float32)
    own_sum[...] = total
    square = total * total
    folded = square[:, :LANES]
    for n in range(1, width // LANES):
        folded = folded + square[:, n * LANES : (n + 1) * LANES]
    line = jnp.sum(folded.T, axis=0, keepdims=True)
    energy[t] = jnp.broadcast_to(line, energy.shape[1:])
    wires.send("ex", energy.at[t], energy.at[t], near_x)
    wires.send("exc", energy.at[t], energy.at[t], far_x)
    wires.send("ec", energy.at[t], energy.at[t], near_c)
    wires.wait("ex", energy.at[t_x])
    wires.wait("exc", energy.at[t_xc])
    wires.wait("ec", energy.at[t_c])
    line = energy[0, 0:1, :]
    for i in range(1, energy.shape[0]):
        line = line + energy[i, 0:1, :]
    scale = jnp.broadcast_to(lax.rsqrt(line / model + EPS), (LANES, length)).T
    close = channel_post[:, rows_of(t, width)]
    kept = mid[:, rows_of(t, width)].astype(jnp.float32)
    for n in range(width // LANES):
        at = pl.ds(n * LANES, LANES)
        value = kept[:, n * LANES : (n + 1) * LANES] + own_sum[:, at] * scale * close[:, n * LANES : (n + 1) * LANES]
        out[:, at] = value.astype(jnp.bfloat16)
    wires.finish()


def pooled(*args):
    tokens, mixer_gain, recur_in, recur_gate, recur_out = args[0], args[1], args[2], args[5], args[9]
    hidden_gate, hidden_down = args[12], args[14]
    length, width = tokens.shape
    depth, channels = recur_in.shape
    model = mixer_gain.shape[0]
    units = hidden_gate.shape[1]
    half = units // 2
    padded = half // LANES * LANES + LANES
    blocks = PLANES * ROWS
    shares = CHIPS * CORES
    group = recur_gate.shape[-1]
    runs = channels // LANES
    bf16, f32 = jnp.bfloat16, jnp.float32
    anywhere = pl.BlockSpec(memory_space=pl.ANY)
    vmem = pl.BlockSpec(memory_space=pltpu.VMEM)
    small = (1, 4, 7, 8, 10, 11, 15)
    args = [arg.reshape(1, -1) if arg.ndim == 1 else arg for arg in args]
    scratch = [
        pltpu.VMEM((shares, length, width), bf16),
        pltpu.VMEM((length, model), bf16),
        pltpu.VMEM((model, 2 * channels), bf16),
        pltpu.VMEM((length, 2 * channels), bf16),
        pltpu.VMEM((2, 2, channels // group, group, group), bf16),
        pltpu.VMEM((runs, LANES, 4 * LANES), bf16),
        pltpu.VMEM((length, shares * channels), bf16),
        pltpu.VMEM((blocks, shares * channels, recur_out.shape[1]), bf16),
        pltpu.VMEM((length, model), f32),
        pltpu.VMEM((length, model), bf16),
        pltpu.VMEM((2, length, model), bf16),
        pltpu.VMEM((2, depth, LANES), bf16),
        pltpu.VMEM((model, units), bf16),
        pltpu.VMEM((depth, units), bf16),
        pltpu.VMEM((2, length, padded), bf16),
        pltpu.VMEM((blocks, padded, hidden_down.shape[1]), bf16),
        pltpu.VMEM((half, hidden_down.shape[1]), bf16),
        pltpu.VMEM((PLANES, 2, length, width), bf16),
        pltpu.VMEM((2, 2, length, width), bf16),
        pltpu.VMEM((2, length, width), bf16),
        pltpu.VMEM((2, length, width), bf16),
        pltpu.VMEM((length, width), f32),
        pltpu.VMEM((length, width), bf16),
        pltpu.VMEM((length, width), bf16),
        pltpu.VMEM((shares, 8, length), f32),
        pltpu.SemaphoreType.DMA((128,)),
        pltpu.SemaphoreType.DMA((128,)),
        pltpu.SemaphoreType.DMA((40,)),
    ]
    return pl.pallas_call(
        pooled_kernel,
        out_shape=jax.ShapeDtypeStruct((length, width), bf16),
        in_specs=[vmem if index in small else anywhere for index in range(len(args))],
        out_specs=vmem,
        scratch_shapes=scratch,
        compiler_params=pltpu.CompilerParams(
            collective_id=0, has_side_effects=True, vmem_limit_bytes=63 * 2**20
        ),
    )(*args)


def solution(mesh):
    in_specs = (
        P("fs", "tp"),
        P(),
        P("fs", "tp"),
        P("fs", "tp"),
        P(),
        P(),
        P(),
        P(),
        P(),
        P("tp", "fs"),
        P(),
        P(),
        P("fs", "tp"),
        P("fs", "tp"),
        P("tp", "fs"),
        P(),
    )
    out_specs = P("fs", "tp")

    def body(*args):
        if pooled_fits(mesh, args):
            return pooled(*args)
        return on_device(snake_order(mesh), mesh.shape["tp"], *args)

    return jax.shard_map(body, mesh=mesh, in_specs=in_specs, out_specs=out_specs, check_vma=False)
```

```python
import functools

import jax
import jax.numpy as jnp
from jax import lax
from jax.experimental import pallas as pl
from jax.experimental.pallas import tpu as pltpu
from jax.sharding import PartitionSpec as P

EPS = 1e-06
SHRINK = 8.0
CORES = 2
FLIGHT = 5


def rms_scale(values, gain):
    return values * lax.rsqrt(jnp.mean(values * values, axis=-1, keepdims=True) + EPS) * gain


def snake_order(mesh):
    count = mesh.shape["fs"]
    axis = list(mesh.axis_names).index("fs")
    line = mesh.devices.take(0, axis=1 - axis).reshape(-1)
    where = [getattr(device, "coords", None) for device in line]
    if any(spot is None for spot in where):
        return list(range(count))
    at = {}
    for index, spot in enumerate(where):
        at[(spot[2], spot[1])] = index
    depth = 1 + max(z for z, _ in at)
    width = 1 + max(y for _, y in at)
    if depth * width != count or len(at) != count or width < 2 or depth % 2:
        return list(range(count))
    order = [at[(z, 0)] for z in range(depth)]
    for back, z in enumerate(reversed(range(depth))):
        columns = range(1, width)
        order += [at[(z, y)] for y in (columns if back % 2 == 0 else reversed(columns))]
    return order


class Ring:
    def __init__(self, order):
        self.n = len(order)
        self.order = order
        n = self.n
        self.pairs = {
            1: [(order[p], order[(p + 1) % n]) for p in range(n)],
            -1: [(order[p], order[(p - 1) % n]) for p in range(n)],
        }
        place = [0] * n
        for p, index in enumerate(order):
            place[index] = p
        self.order_row = jnp.array(order, jnp.int32)
        self.here = jnp.array(place, jnp.int32)[lax.axis_index("fs")]
        self.landed = {1: [], -1: []}

    def source(self, step):
        return self.order_row[lax.rem(self.here - step + self.n, self.n)]

    def send(self, value, way):
        landed = self.landed[way]
        if len(landed) >= FLIGHT:
            value = lax.optimization_barrier((value, landed[-FLIGHT]))[0]
        value = lax.ppermute(value, "fs", self.pairs[way])
        landed.append(value)
        return value

    def gather(self, shards, ties={}, paired=False, lead=1):
        n = self.n
        found = [[(self.source(0), shard)] for shard in shards]
        heads = [{1: shard, -1: shard} for shard in shards]
        for step in range(1, n // 2 + 1):
            for index in range(len(shards)):
                for way in (1, -1):
                    steps = n // 2 if (way == lead) == (index % 2 == 0 or paired) else n - 1 - n // 2
                    if step <= steps:
                        if step in ties:
                            heads[index][way] = lax.optimization_barrier((heads[index][way], ties[step]))[0]
                        heads[index][way] = self.send(heads[index][way], way)
                        found[index].append((self.source(way * step), heads[index][way]))
        return found


def stack_rows(blocks):
    height, width = blocks[0][1].shape
    total = jnp.zeros((height * len(blocks), width), blocks[0][1].dtype)
    for source, block in blocks:
        total = lax.dynamic_update_slice(total, block, (source * height, 0))
    return total


def stack_columns(blocks):
    height, width = blocks[0][1].shape
    total = jnp.zeros((height, width * len(blocks)), blocks[0][1].dtype)
    for source, block in blocks:
        total = lax.dynamic_update_slice(total, block, (0, source * width))
    return total


def swap_cores(value, count):
    return lax.ppermute(value, "tp", [(t, t ^ 1) for t in range(count)])


def from_chip(value, shift, count):
    return lax.ppermute(value, "tp", [(t, (t + CORES * shift) % count) for t in range(count)])


def chips_shares(value, count):
    chips = count // CORES
    chip = lax.axis_index("tp") // CORES
    found = [(chip, value)]
    for shift in range(1, chips):
        found.append((lax.rem(chip - shift + chips, chips), from_chip(value, shift, count)))
    return found


def gather_features(value, count):
    core = lax.rem(lax.axis_index("tp"), CORES)
    width = value.shape[1]
    total = jnp.zeros((value.shape[0], width * count), value.dtype)
    for chip, block in chips_shares(value, count):
        other = swap_cores(block, count)
        total = lax.dynamic_update_slice(total, block, (0, (chip * CORES + core) * width))
        total = lax.dynamic_update_slice(total, other, (0, (chip * CORES + 1 - core) * width))
    return total


def sum_all(value, count):
    core = lax.rem(lax.axis_index("tp"), CORES)
    half = value.shape[1] // CORES
    keep = lax.dynamic_slice_in_dim(value, core * half, half, 1)
    give = lax.dynamic_slice_in_dim(value, (1 - core) * half, half, 1)
    chip_sum = keep.astype(jnp.float32) + swap_cores(give, count).astype(jnp.float32)
    chip_sum = chip_sum.astype(jnp.bfloat16)
    total = 0.0
    for _, block in chips_shares(chip_sum, count):
        total = total + block.astype(jnp.float32)
    mine = total.astype(jnp.bfloat16)
    other = swap_cores(mine, count)
    low = jnp.where(core == 0, mine, other)
    high = jnp.where(core == 0, other, mine)
    return jnp.concatenate([low, high], axis=1)


def sum_own(value, count):
    rank = lax.axis_index("tp")
    core = lax.rem(rank, CORES)
    chip = rank // CORES
    chips = count // CORES
    length = value.shape[0]
    width = value.shape[1] // count

    def block(chip_at, core_at):
        at = (chip_at * CORES + core_at) * width
        return lax.dynamic_slice_in_dim(value, at, width, 1)

    total = 0.0
    for shift in list(range(1, chips)) + [0]:
        target = lax.rem(chip + shift, chips)
        part = block(target, core).astype(jnp.float32)
        part = part + swap_cores(block(target, 1 - core), count).astype(jnp.float32)
        if shift:
            part = from_chip(part.astype(jnp.bfloat16), shift, count).astype(jnp.float32)
        total = total + part
    return total


def minus_expm1(value):
    series = jnp.ones_like(value)
    for order in range(9, 1, -1):
        series = 1.0 + value * (1.0 / order) * series
    return jnp.where(value > -0.5, -value * series, 1.0 - jnp.exp(value))


def scan_block(decay, inflow, reverse):
    length = decay.shape[0]
    row = lax.broadcasted_iota(jnp.int32, decay.shape, 0)
    reach = 1
    while reach < length:
        if reverse:
            inside = row < length - reach
            turn = length - reach
        else:
            inside = row >= reach
            turn = reach
        before_inflow = jnp.where(inside, pltpu.roll(inflow, turn, 0), 0.0)
        inflow = inflow + decay * before_inflow
        if 2 * reach < length:
            decay = decay * jnp.where(inside, pltpu.roll(decay, turn, 0), 1.0)
        reach *= 2
    return inflow


def mixer_kernel(recur_ref, branch_ref, taps_ref, gate_ref, decay_ref, gain_ref, out_ref):
    recur = recur_ref[...].astype(jnp.float32)
    length, width = recur.shape
    row = lax.broadcasted_iota(jnp.int32, recur.shape, 0)
    taps = taps_ref[...]
    conv = taps[2:3] * recur
    for tap, shift in ((0, 2), (1, 1), (3, length - 1)):
        inside = row < length - 1 if tap == 3 else row >= shift
        conv = conv + taps[tap : tap + 1] * jnp.where(inside, pltpu.roll(recur, shift, 0), 0.0)
    first = conv.astype(jnp.bfloat16)
    rest = conv - first.astype(jnp.float32)
    second = rest.astype(jnp.bfloat16)
    third = (rest - second.astype(jnp.float32)).astype(jnp.bfloat16)
    total = None
    for direction in range(2):
        logits = []
        for kind in range(2):
            weight = gate_ref[0, :, pl.ds((direction * 2 + kind) * width, width)]
            logits.append(
                jnp.dot(third, weight, preferred_element_type=jnp.float32)
                + jnp.dot(second, weight, preferred_element_type=jnp.float32)
                + jnp.dot(first, weight, preferred_element_type=jnp.float32)
            )
        rate = 1.0 / (1.0 + jnp.exp(-logits[0]))
        inlet = 1.0 / (1.0 + jnp.exp(-logits[1]))
        log_decay = rate * decay_ref[direction : direction + 1, :]
        inflow = conv * inlet * jnp.sqrt(minus_expm1(2.0 * log_decay))
        state = scan_block(jnp.exp(log_decay), inflow, direction == 1)
        total = state if total is None else total + state
    branch = branch_ref[...].astype(jnp.float32)
    inner = 0.7978845608028654 * (branch + 0.044715 * (branch * branch * branch))
    gelu = branch * (0.5 * (1.0 + jnp.tanh(inner)))
    out_ref[...] = (total * gelu * gain_ref[...]).astype(jnp.bfloat16)


def mixer(both_x, taps, rate_own, inlet_own, decay_own, gain_own):
    length, channels = both_x.shape[0], both_x.shape[1] // 2
    group = rate_own.shape[-1]
    lanes = min(channels, 2 * group)
    blocks = channels // lanes
    per = lanes // group

    def dense(weight):
        spread = weight.reshape(2, blocks, per, group, 1, group) * jnp.eye(per, dtype=weight.dtype)[:, None, :, None]
        return spread.reshape(2, blocks, lanes, lanes)

    both = jnp.stack([dense(rate_own), dense(inlet_own)], axis=1)
    gates = both.transpose(2, 3, 0, 1, 4).reshape(blocks, lanes, 4 * lanes)
    slope = -SHRINK * jax.nn.softplus(-decay_own)
    column = lambda j: (0, j)
    return pl.pallas_call(
        mixer_kernel,
        grid=(blocks,),
        out_shape=jax.ShapeDtypeStruct((length, channels), jnp.bfloat16),
        in_specs=[
            pl.BlockSpec((length, lanes), column),
            pl.BlockSpec((length, lanes), lambda j: (0, blocks + j)),
            pl.BlockSpec((taps.shape[0], lanes), column),
            pl.BlockSpec((1, lanes, 4 * lanes), lambda j: (j, 0, 0)),
            pl.BlockSpec((2, lanes), column),
            pl.BlockSpec((1, lanes), column),
        ],
        out_specs=pl.BlockSpec((length, lanes), column),
        cost_estimate=pl.CostEstimate(flops=int(3e9), bytes_accessed=2**20, transcendentals=2**21),
        compiler_params=pltpu.CompilerParams(vmem_limit_bytes=24 * 2**20),
    )(both_x, both_x, taps, gates, slope, gain_own.reshape(1, channels))


def on_device(
    order,
    tp_count,
    tokens,
    mixer_gain,
    recur_in,
    branch_in,
    conv_taps,
    recur_gate,
    input_gate,
    decay_param,
    recur_gain,
    recur_out,
    mixer_post,
    channel_gain,
    hidden_gate,
    hidden_up,
    hidden_down,
    channel_post,
):
    rank_tp = lax.axis_index("tp")
    feature_width = tokens.shape[1]
    model_width = mixer_gain.shape[0]
    channel_width = recur_in.shape[1]
    group_count = channel_width // recur_gate.shape[-1]
    feature_start = rank_tp * feature_width
    channel_start = rank_tp * channel_width

    ring = Ring(order)
    packed = jnp.concatenate([recur_in, branch_in, recur_out.reshape(recur_in.shape)], axis=1)
    mix_blocks, gate_blocks = ring.gather([packed, hidden_gate])
    in_blocks = [(source, block[:, : 2 * channel_width]) for source, block in mix_blocks]
    out_blocks = [
        (source, block[:, 2 * channel_width :].reshape(recur_out.shape)) for source, block in mix_blocks
    ]

    gathered_in = gather_features(tokens, tp_count)
    gathered_float = gathered_in.astype(jnp.float32)
    normed_in = rms_scale(gathered_float, mixer_gain).astype(jnp.bfloat16)
    both_x = jnp.dot(normed_in, stack_rows(in_blocks), preferred_element_type=jnp.float32).astype(jnp.bfloat16)

    taps = lax.dynamic_slice_in_dim(conv_taps, channel_start, channel_width, 1).astype(jnp.float32)
    group_start = rank_tp * group_count
    rate_own = lax.dynamic_slice_in_dim(recur_gate, group_start, group_count, 1)
    inlet_own = lax.dynamic_slice_in_dim(input_gate, group_start, group_count, 1)
    decay_own = lax.dynamic_slice_in_dim(decay_param, channel_start, channel_width, 1)
    gain_own = lax.dynamic_slice_in_dim(recur_gain, channel_start, channel_width, 0)
    recur_y = mixer(both_x, taps, rate_own, inlet_own, decay_own, gain_own)

    (up_blocks,) = ring.gather([hidden_up], lead=-1)
    branch_part = jnp.dot(recur_y, stack_columns(out_blocks), preferred_element_type=jnp.float32)
    branch_sum = sum_all(branch_part.astype(jnp.bfloat16), tp_count).astype(jnp.float32)
    mid_full = (gathered_float + rms_scale(branch_sum, mixer_post)).astype(jnp.bfloat16)
    mid_own = lax.dynamic_slice_in_dim(mid_full, feature_start, feature_width, 1)
    channel_in = rms_scale(mid_full.astype(jnp.float32), channel_gain).astype(jnp.bfloat16)

    gate_total = jnp.dot(channel_in, stack_rows(gate_blocks), preferred_element_type=jnp.float32)
    up_total = jnp.dot(channel_in, stack_rows(up_blocks), preferred_element_type=jnp.float32)
    hidden = (jax.nn.silu(gate_total) * up_total).astype(jnp.bfloat16)

    cut = max(hidden_down.shape[0] // 256, 1) * 128
    low_blocks, high_blocks = ring.gather(
        [hidden_down[:cut], hidden_down[cut:]], {4: hidden}, True
    )
    part_blocks = []
    for (source, low), (_, high) in zip(low_blocks, high_blocks):
        part = jnp.dot(hidden[:, :cut], low, preferred_element_type=jnp.float32)
        part = part + jnp.dot(hidden[:, cut:], high, preferred_element_type=jnp.float32)
        part_blocks.append((source, part.astype(jnp.bfloat16)))
    hidden_part = stack_columns(part_blocks)
    hidden_own = sum_own(hidden_part, tp_count)
    energy_own = jnp.sum(hidden_own * hidden_own, axis=1).reshape(-1, 128)
    hidden_energy = lax.psum(energy_own, "tp").reshape(-1)
    close_own = lax.dynamic_slice_in_dim(channel_post, feature_start, feature_width, 0)
    return (
        mid_own.astype(jnp.float32)
        + hidden_own * lax.rsqrt(hidden_energy / model_width + EPS)[:, None] * close_own
    ).astype(jnp.bfloat16)


PLANES = 4
ROWS = 2
CHIPS = 2
MESH = pl.DeviceIdType.MESH
LANES = 128


def pooled_fits(mesh, args):
    if mesh.shape["fs"] != PLANES * ROWS or mesh.shape["tp"] != CHIPS * CORES:
        return False
    spots = [getattr(device, "coords", None) for device in mesh.devices.reshape(-1)]
    if all(spot is not None for spot in spots):
        if list(mesh.axis_names) != ["fs", "tp"]:
            return False
        at = mesh.devices
        for f in range(PLANES * ROWS):
            for t in range(CHIPS * CORES):
                if tuple(at[f, t].coords) != (t // CORES, f % ROWS, f // ROWS):
                    return False
    tokens, gate, down, recur_in, recur_out = args[0], args[12], args[14], args[2], args[9]
    half = gate.shape[1] // 2
    return (
        tokens.shape[1] % LANES == 0
        and tokens.shape[0] % 16 == 0
        and gate.shape[0] % 16 == 0
        and half % LANES == LANES // 2
        and down.shape[0] == gate.shape[1]
        and recur_in.shape[1] % LANES == 0
        and recur_out.shape[1] % LANES == 0
        and LANES % args[5].shape[-1] == 0
    )


class Wires:
    def __init__(self, sends, lands, nobody):
        self.sends = sends
        self.lands = lands
        self.nobody = nobody
        self.names = {}
        self.started = []

    def index(self, name):
        return self.names.setdefault(name, len(self.names))

    def send(self, name, source, target, to, land=None, only=None):
        copy = pltpu.make_async_remote_copy(
            src_ref=source,
            dst_ref=target,
            send_sem=self.sends.at[self.index(name)],
            recv_sem=self.lands.at[self.index(land or name)],
            device_id=to,
            device_id_type=MESH,
        )
        guarded(only, copy.start)
        self.started.append((only, copy))

    def wait(self, name, target):
        at = self.lands.at[self.index(name)]
        with jax.named_scope("wait_" + name):
            pltpu.make_async_remote_copy(
                src_ref=target,
                dst_ref=target,
                send_sem=at,
                recv_sem=at,
                device_id=self.nobody,
                device_id_type=MESH,
            ).wait_recv()

    def finish(self):
        with jax.named_scope("finish"):
            for only, copy in self.started:
                guarded(only, copy.wait_send)


def guarded(only, action):
    if only is None:
        action()
    else:
        pl.when(only)(action)


def scan_pair(conv, logits, slope, reverse):
    rate = 1.0 / (1.0 + jnp.exp(-logits[0]))
    inlet = 1.0 / (1.0 + jnp.exp(-logits[1]))
    log_decay = rate * slope
    inflow = conv * inlet * jnp.sqrt(minus_expm1(2.0 * log_decay))
    return scan_block(jnp.exp(log_decay), inflow, reverse)


def log_one_plus(value):
    total = 1.0 + value
    exact = total == 1.0
    return jnp.where(exact, value, jnp.log(total) * (value / jnp.where(exact, 1.0, total - 1.0)))


def pooled_kernel(
    tokens,
    mixer_gain,
    recur_in,
    branch_in,
    conv_taps,
    recur_gate,
    input_gate,
    decay_param,
    recur_gain,
    recur_out,
    mixer_post,
    channel_gain,
    hidden_gate,
    hidden_up,
    hidden_down,
    channel_post,
    out,
    tok,
    normed,
    w_in,
    both_x,
    gates_raw,
    gates,
    recur_all,
    w_out,
    branch,
    mid,
    channel_in,
    edge,
    w_gate_up,
    other_gate_up,
    hidden,
    w_down,
    other_down,
    part,
    part_in,
    chip_send,
    chip_in,
    own_sum,
    plane_send,
    plane_in,
    early_send,
    early_in,
    energy,
    sends,
    lands,
    local,
):
    f = lax.axis_index("fs")
    t = lax.axis_index("tp")
    z, y = lax.div(f, ROWS), lax.rem(f, ROWS)
    x, c = lax.div(t, CORES), lax.rem(t, CORES)
    zi, zp = lax.rem(z, 2), lax.div(z, 2)
    planes = [z, z + 1 - 2 * zi, lax.rem(z + 2, PLANES), PLANES - 1 - z]
    is_mid = lax.div(lax.rem(z + 1, PLANES), 2) == 1
    is_end = lax.div(lax.rem(z + 1, PLANES), 2) == 0
    length, width = tokens.shape
    depth = recur_in.shape[0]
    channels = recur_in.shape[1]
    units = hidden_gate.shape[1]
    half = units // 2
    wide = half // LANES * LANES
    narrow = half - wide
    full = wide // LANES
    model = tok.shape[0] * width
    group = recur_gate.shape[-1]
    blocks = PLANES * ROWS

    def device(plane, row, chip, core):
        return {"fs": plane * ROWS + row, "tp": chip * CORES + core}

    def block(k, row):
        return planes[k] * ROWS + row

    near_y = device(z, 1 - y, x, c)
    near_x = device(z, y, 1 - x, c)
    far_x = device(z, y, 1 - x, 1 - c)
    near_c = device(z, y, x, 1 - c)
    plane_of = [None] + [device(planes[k], y, x, c) for k in (1, 2, 3)]
    t_c = x * CORES + 1 - c
    t_x = (1 - x) * CORES + c
    t_xc = (1 - x) * CORES + 1 - c
    wires = Wires(sends, lands, near_c)
    rows_of = lambda at, size: pl.ds(pl.multiple_of(at * size, size), size)

    moves = {}

    def move(name, source, target):
        copy = pltpu.make_async_copy(source, target, local.at[len(moves)])
        copy.start()
        moves[name] = copy

    def here(prefix):
        for name, copy in moves.items():
            if name.startswith(prefix):
                copy.wait()

    move("io0", recur_in, w_in.at[rows_of(f, depth), pl.ds(0, channels)])
    move("io1", branch_in, w_in.at[rows_of(f, depth), pl.ds(channels, channels)])
    move("io2", recur_out, w_out.at[f, rows_of(t, channels), :])
    move("tok", tokens, tok.at[t])
    columns = lambda at: pl.ds(pl.multiple_of(at, LANES), LANES)
    for side, target, row_at, parity in (("a", w_gate_up, f, zi), ("b", other_gate_up, 0, 1 - zi)):
        for n in range(full):
            start = parity * (units - wide) + n * LANES
            for m, weight in enumerate((hidden_gate, hidden_up)):
                move(
                    f"gu{side}{n}{m}",
                    weight.at[:, columns(start)],
                    target.at[rows_of(row_at, depth), pl.ds((2 * n + m) * LANES, LANES)],
                )
    move("gum0", hidden_gate.at[:, pl.ds(wide, LANES)], edge.at[0])
    move("gum1", hidden_up.at[:, pl.ds(wide, LANES)], edge.at[1])
    group_count = channels // group
    move("gate0", recur_gate.at[:, rows_of(t, group_count)], gates_raw.at[0])
    move("gate1", input_gate.at[:, rows_of(t, group_count)], gates_raw.at[1])
    for side, target, parity in (("a", w_down.at[f], zi), ("b", other_down, 1 - zi)):
        wide_at = pl.multiple_of(parity * (units - wide), 2 * narrow)
        narrow_at = pl.multiple_of(wide + parity * narrow, narrow)
        move(f"dn{side}0", hidden_down.at[pl.ds(wide_at, wide), :], target.at[pl.ds(0, wide), :])
        move(f"dn{side}1", hidden_down.at[pl.ds(narrow_at, narrow), :], target.at[pl.ds(wide, narrow), :])

    barrier = pltpu.get_barrier_semaphore()
    peers = [near_y, near_x, far_x, near_c] + plane_of[1:]
    for peer in peers:
        pl.semaphore_signal(barrier, inc=1, device_id=peer, device_id_type=MESH)
    with jax.named_scope("barrier"):
        pl.semaphore_wait(barrier, len(peers))

    def in_slot(k, row):
        return w_in.at[rows_of(block(k, row), depth), :]

    def out_slot(k, row):
        return w_out.at[block(k, row), rows_of(t, channels), :]

    part_rows = depth // 2

    def gate_slot(k, row, piece):
        at = pl.multiple_of(block(k, row) * depth + piece * part_rows, part_rows)
        return w_gate_up.at[pl.ds(at, part_rows), :]

    def other_slot(piece):
        return other_gate_up.at[pl.ds(piece * part_rows, part_rows), :]

    def down_slot(k, row):
        return w_down.at[block(k, row), pl.ds(0, half), :]

    down_other = other_down

    slots = {"i": in_slot, "o": out_slot}

    def mixer_to_y(kind, k):
        slot = slots[kind](k, y)
        wires.send(f"{kind}y{k}", slot, slot, near_y)

    def mixer_to_x(k, row, tag):
        wires.send(f"ox{tag}{k}", out_slot(k, row), out_slot(k, row), near_x)

    def mixer_to_z(kind, name, k, to, land, only=None):
        slot = slots[kind](k, y)
        wires.send(kind + name, slot, slot, to, f"{kind}z{land}", only)

    def mixer_wait(kind, k, only=None):
        guarded(only, lambda: wires.wait(f"{kind}z{k}", slots[kind](k, y)))

    late_at = {
        "s": jnp.where(is_mid, planes[3], planes[2]) * ROWS,
        "t": jnp.where(is_mid, planes[2], planes[3]) * ROWS,
    }

    def late_slot(kind, tag, row):
        at = late_at[tag] + row
        if kind == "i":
            return w_in.at[rows_of(at, depth), :]
        return w_out.at[at, rows_of(t, channels), :]

    def late_to_y(kind, tag):
        slot = late_slot(kind, tag, y)
        wires.send(f"{kind}y{tag}", slot, slot, near_y)

    def late_to_x(tag, row, side):
        slot = late_slot("o", tag, row)
        wires.send(f"ox{side}{tag}", slot, slot, near_x)

    def gate_own_to_z(piece, which, only):
        if which == 1:
            wires.send(f"g{piece}s1", gate_slot(0, y, piece), gate_slot(0, y, piece), plane_of[2], f"gz{piece}2", only)
        else:
            k = 1 if which == 2 else 3
            source = other_slot(piece)
            wires.send(f"g{piece}s{which}", source, gate_slot(0, y, piece), plane_of[k], f"gz{piece}{k}", only)

    def down_own_to_z(which, only):
        if which == 1:
            wires.send("ds1", down_slot(0, y), down_slot(0, y), plane_of[2], "dz2", only)
        else:
            k = 1 if which == 2 else 3
            wires.send(f"ds{which}", down_other, down_slot(0, y), plane_of[k], f"dz{k}", only)

    def gate_to_y(k, piece):
        wires.send(f"gy{piece}{k}", gate_slot(k, y, piece), gate_slot(k, y, piece), near_y)

    def down_to_y(k):
        wires.send(f"dy{k}", down_slot(k, y), down_slot(k, y), near_y)

    def gate_pass(k, piece, only=None):
        guarded(only, lambda: wires.wait(f"gz{piece}{k}", gate_slot(k, y, piece)))
        if k == 1:
            passing = is_mid if only is None else only
            if passing is is_mid:
                slot = gate_slot(1, y, piece)
                wires.send(f"g{piece}r", slot, slot, plane_of[2], f"gz{piece}3", is_mid)
        slot = gate_slot(k, y, piece)
        wires.send(f"gy{piece}{k}", slot, slot, near_y, only=only)

    fine_width = depth // 2
    halves = ((0, fine_width), (fine_width, fine_width))
    whole = ((0, depth),)

    def down_piece(k, row, at, size):
        return w_down.at[block(k, row), pl.ds(0, half), pl.ds(at, size)]

    def down_pass(k, only=None):
        guarded(only, lambda: wires.wait(f"dz{k}", down_slot(k, y)))
        if k == 1:
            passing = is_mid if only is None else only
            if passing is is_mid:
                wires.send("dr", down_slot(1, y), down_slot(1, y), plane_of[2], "dz3", is_mid)
        for at, size in halves if k == 1 else whole:
            slot = down_piece(k, y, at, size)
            wires.send(f"dy{k}{at}", slot, slot, near_y, only=only)

    here("io0")
    here("io1")
    mixer_to_y("i", 0)
    mixer_to_z("i", "z1", 0, plane_of[1], 1)
    mixer_to_z("i", "z3", 0, plane_of[3], 3, is_mid)
    here("tok")
    wires.send("tc", tok.at[t], tok.at[t], near_c)
    wires.send("tx", tok.at[t], tok.at[t], near_x)
    here("io2")
    mixer_to_y("o", 0)
    mixer_to_z("o", "z1", 0, plane_of[1], 1)
    mixer_to_z("o", "z3", 0, plane_of[3], 3, is_mid)

    here("gum")
    lane = lax.broadcasted_iota(jnp.int32, edge.shape[1:], 1)
    edge_gate = edge[0].astype(jnp.float32)
    edge_up = edge[1].astype(jnp.float32)
    low = jnp.where(lane < narrow, edge_gate, pltpu.roll(edge_up, narrow, 1))
    high = jnp.where(lane < narrow, pltpu.roll(edge_gate, narrow, 1), edge_up)
    odd = zi == 1
    edge_at = pl.ds(2 * wide, LANES)
    w_gate_up[rows_of(f, depth), edge_at] = jnp.where(odd, high, low).astype(jnp.bfloat16)
    other_gate_up[:, edge_at] = jnp.where(odd, low, high).astype(jnp.bfloat16)
    w_down[:, pl.ds(half, LANES - narrow), :] = jnp.zeros((blocks, LANES - narrow, w_down.shape[2]), jnp.bfloat16)
    here("gua")
    here("gub")

    gate_own_to_z(0, 2, is_end)
    gate_own_to_z(1, 2, is_end)

    mixer_wait("i", 1)
    mixer_to_z("i", "r1", 1, plane_of[3], 2, is_mid)
    mixer_to_y("i", 1)
    gate_to_y(0, 0)
    mixer_wait("i", 3, is_mid)
    mixer_to_z("i", "r3", 3, plane_of[1], 2, is_mid)

    wires.wait("tx", tok.at[t_x])
    wires.send("txc", tok.at[t_x], tok.at[t_x], near_c)

    mixer_wait("o", 1)
    mixer_to_z("o", "r1", 1, plane_of[3], 2, is_mid)
    gate_own_to_z(0, 3, is_mid)
    mixer_wait("i", 2)
    late_to_y("i", "s")
    mixer_to_z("i", "r2", 2, plane_of[1], 3, is_mid)
    mixer_wait("o", 3, is_mid)
    mixer_to_z("o", "r3", 3, plane_of[1], 2, is_mid)
    mixer_to_x(0, y, "a")
    here("gate")
    per = LANES // group
    runs = channels // LANES
    for j in range(runs):
        for direction in range(2):
            for kind in range(2):
                dense = None
                for a in range(per):
                    spread_row = lax.broadcasted_iota(jnp.int32, (group, LANES), 0)
                    spread_lane = lax.broadcasted_iota(jnp.int32, (group, LANES), 1)
                    spread = (spread_lane == spread_row + a * group).astype(jnp.bfloat16)
                    lift_row = lax.broadcasted_iota(jnp.int32, (LANES, group), 0)
                    lift_lane = lax.broadcasted_iota(jnp.int32, (LANES, group), 1)
                    lift = (lift_row == lift_lane + a * group).astype(jnp.bfloat16)
                    block_map = gates_raw[kind, direction, j * per + a]
                    block_map = jnp.dot(block_map, spread, preferred_element_type=jnp.float32).astype(jnp.bfloat16)
                    block_map = jnp.dot(lift, block_map, preferred_element_type=jnp.float32)
                    dense = block_map if dense is None else dense + block_map
                gates[j, :, pl.ds((direction * 2 + kind) * LANES, LANES)] = dense.astype(jnp.bfloat16)

    mixer_wait("i", 3, is_end)
    late_to_y("i", "t")
    mixer_to_y("o", 1)
    mixer_wait("o", 2)
    late_to_y("o", "s")
    mixer_to_z("o", "r2", 2, plane_of[1], 3, is_mid)
    gate_own_to_z(0, 2, is_mid)
    gate_own_to_z(0, 1, None)
    gate_pass(1, 0, is_mid)
    wires.wait("tc", tok.at[t_c])
    wires.wait("txc", tok.at[t_xc])
    fine = 16

    with jax.named_scope("norm"):

        @pl.loop(0, length // fine, unroll=2)
        def _(r):
            rows = rows_of(r, fine)
            values = jnp.concatenate([tok[i, rows, :] for i in range(tok.shape[0])], axis=1).astype(jnp.float32)
            normed[rows, :] = rms_scale(values, mixer_gain[...]).astype(jnp.bfloat16)

    mixer_wait("o", 3, is_end)
    late_to_y("o", "t")
    gate_to_y(0, 1)
    gate_own_to_z(1, 2, is_mid)
    gate_own_to_z(1, 3, is_mid)
    gate_own_to_z(1, 1, None)
    here("dn")
    down_own_to_z(2, is_end)
    gate_pass(1, 1, is_mid)
    wires.wait("oy0", out_slot(0, 1 - y))
    mixer_to_x(0, 1 - y, "b")
    mixer_to_x(1, y, "a")
    for k in (0, 1):
        wires.wait(f"iy{k}", in_slot(k, 1 - y))
    for tag in ("s", "t"):
        wires.wait(f"iy{tag}", late_slot("i", tag, 1 - y))

    with jax.named_scope("in_proj"):

        @pl.loop(0, 2)
        def _(j):
            at = rows_of(j, channels)
            product = jnp.dot(normed[...], w_in[:, at], preferred_element_type=jnp.float32)
            both_x[:, at] = product.astype(jnp.bfloat16)


    own_channels = pl.multiple_of(t * channels, LANES)

    with jax.named_scope("scan"):

        @pl.loop(0, runs)
        def _(j):
            at = pl.ds(pl.multiple_of(j * LANES, LANES), LANES)
            gate_at = pl.ds(pl.multiple_of(channels + j * LANES, LANES), LANES)
            table_at = pl.ds(pl.multiple_of(own_channels + j * LANES, LANES), LANES)
            recur = both_x[:, at].astype(jnp.float32)
            row = lax.broadcasted_iota(jnp.int32, recur.shape, 0)
            taps = conv_taps[:, table_at].astype(jnp.float32)
            conv = taps[2:3] * recur
            for tap, shift in ((0, 2), (1, 1), (3, length - 1)):
                inside = row < length - 1 if tap == 3 else row >= shift
                conv = conv + taps[tap : tap + 1] * jnp.where(inside, pltpu.roll(recur, shift, 0), 0.0)
            first = conv.astype(jnp.bfloat16)
            rest = conv - first.astype(jnp.float32)
            second_part = rest.astype(jnp.bfloat16)
            third_part = (rest - second_part.astype(jnp.float32)).astype(jnp.bfloat16)
            decay = decay_param[:, table_at]
            slope = -SHRINK * (jnp.maximum(-decay, 0.0) + log_one_plus(jnp.exp(-jnp.abs(decay))))
            total = None
            for direction in range(2):
                logits = []
                for kind in range(2):
                    weight = gates[j, :, pl.ds((direction * 2 + kind) * LANES, LANES)]
                    logits.append(
                        jnp.dot(third_part, weight, preferred_element_type=jnp.float32)
                        + jnp.dot(second_part, weight, preferred_element_type=jnp.float32)
                        + jnp.dot(first, weight, preferred_element_type=jnp.float32)
                    )
                state = scan_pair(conv, logits, slope[direction : direction + 1], direction == 1)
                total = state if total is None else total + state
            value = both_x[:, gate_at].astype(jnp.float32)
            inner = 0.7978845608028654 * (value + 0.044715 * (value * value * value))
            gelu = value * (0.5 * (1.0 + jnp.tanh(inner)))
            recur_all[:, table_at] = (total * gelu * recur_gain[:, table_at]).astype(jnp.bfloat16)

    mine = recur_all.at[:, rows_of(t, channels)]
    wires.send("rx", mine, mine, near_x)
    wires.send("rc", mine, mine, near_c)
    wires.wait("oy1", out_slot(1, 1 - y))
    mixer_to_x(1, 1 - y, "b")
    late_to_x("s", y, "a")
    late_to_x("t", y, "a")
    gate_pass(1, 0, is_end)
    wires.send("dy00", down_slot(0, y), down_slot(0, y), near_y, only=is_end)
    gate_pass(3, 0, is_mid)
    for tag in ("s", "t"):
        wires.wait(f"oy{tag}", late_slot("o", tag, 1 - y))
        late_to_x(tag, 1 - y, "b")
    wires.send("oc1", w_out.at[:, rows_of(t, channels), :], w_out.at[:, rows_of(t, channels), :], near_c)
    for k in (0, 1):
        for side, row in (("a", y), ("b", 1 - y)):
            wires.wait(f"ox{side}{k}", w_out.at[block(k, row), rows_of(t_x, channels), :])
    for tag in ("s", "t"):
        for side, row in (("a", y), ("b", 1 - y)):
            wires.wait(f"ox{side}{tag}", w_out.at[late_at[tag] + row, rows_of(t_x, channels), :])
    wires.send("oc2", w_out.at[:, rows_of(t_x, channels), :], w_out.at[:, rows_of(t_x, channels), :], near_c)
    theirs = recur_all.at[:, rows_of(t_x, channels)]
    wires.wait("rx", theirs)
    wires.send("rxc", theirs, theirs, near_c)
    wires.wait("oc1", w_out.at[:, rows_of(t_c, channels), :])
    wires.wait("oc2", w_out.at[:, rows_of(t_xc, channels), :])
    wires.wait("rc", recur_all.at[:, rows_of(t_c, channels)])
    wires.wait("rxc", recur_all.at[:, rows_of(t_xc, channels)])

    gate_pass(2, 0, is_end)
    with jax.named_scope("branch_dot"):

        @pl.loop(0, blocks)
        def _(b):
            branch[:, rows_of(b, depth)] = jnp.dot(recur_all[...], w_out[b], preferred_element_type=jnp.float32)

    def quarter(s, at, piece):
        return channel_in.at[s, pl.ds(piece * (length // 2), length // 2), rows_of(at, width)]

    for piece in range(2):
        with jax.named_scope(f"branch_norm{piece}"):

            @pl.loop(piece * length // 2 // fine, (piece + 1) * length // 2 // fine, unroll=2)
            def _(r):
                rows = rows_of(r, fine)
                values = jnp.concatenate([tok[i, rows, :] for i in range(tok.shape[0])], axis=1).astype(jnp.float32)
                middle = (values + rms_scale(branch[rows, :], mixer_post[...])).astype(jnp.bfloat16)
                mid[rows, :] = middle
                channel_in[0, rows, :] = rms_scale(middle.astype(jnp.float32), channel_gain[...]).astype(jnp.bfloat16)

        wires.send(f"cz{piece}", quarter(0, t, piece), quarter(1, t, piece), plane_of[1])

    down_own_to_z(2, is_mid)
    gate_pass(2, 0, is_mid)
    gate_pass(1, 1, is_end)
    gate_pass(3, 1, is_mid)
    gate_pass(3, 0, is_end)
    down_own_to_z(3, is_mid)
    down_own_to_z(1, is_end)
    wires.wait("cz0", quarter(1, t, 0))
    wires.send("cx0", quarter(1, t, 0), quarter(1, t, 0), near_x)
    wires.send("cca0", quarter(1, t, 0), quarter(1, t, 0), near_c)
    gate_pass(2, 1)
    wires.wait("cz1", quarter(1, t, 1))
    wires.send("cx1", quarter(1, t, 1), quarter(1, t, 1), near_x)
    wires.send("cca1", quarter(1, t, 1), quarter(1, t, 1), near_c)
    gate_pass(3, 1, is_end)
    wires.send("dy00", down_slot(0, y), down_slot(0, y), near_y, only=is_mid)
    for piece in range(2):
        wires.wait(f"cx{piece}", quarter(1, t_x, piece))
        wires.send(f"ccb{piece}", quarter(1, t_x, piece), quarter(1, t_x, piece), near_c)
    for piece in range(2):
        wires.wait(f"cca{piece}", quarter(1, t_c, piece))
        wires.wait(f"ccb{piece}", quarter(1, t_xc, piece))
    down_pass(3, is_mid)
    down_own_to_z(1, is_mid)
    down_pass(1, is_mid)
    down_pass(2, is_mid)
    down_pass(2, is_end)
    for k in range(PLANES):
        for piece in range(2):
            wires.wait(f"gy{piece}{k}", gate_slot(k, 1 - y, piece))

    with jax.named_scope("gate_up"):

        @pl.loop(0, full)
        def _(n):
            at = pl.ds(pl.multiple_of(n * 2 * LANES, 2 * LANES), 2 * LANES)
            store = pl.ds(pl.multiple_of(n * LANES, LANES), LANES)
            for s in range(2):
                product = jnp.dot(channel_in[s], w_gate_up[:, at], preferred_element_type=jnp.float32)
                gate_value, up_value = product[:, :LANES], product[:, LANES:]
                hidden[s, :, store] = (jax.nn.silu(gate_value) * up_value).astype(jnp.bfloat16)

    lane_tail = lax.broadcasted_iota(jnp.int32, (length, LANES), 1)
    for s in range(2):
        product = jnp.dot(channel_in[s], w_gate_up[:, edge_at], preferred_element_type=jnp.float32)
        value = jax.nn.silu(product) * pltpu.roll(product, narrow, 1)
        hidden[s, :, pl.ds(wide, LANES)] = jnp.where(lane_tail < narrow, value, 0.0).astype(jnp.bfloat16)

    mine_odd = lax.rem(zi + c, 2)
    mine_late = lax.rem(zp + x, 2)

    def pieces(kk, late):
        return halves if kk == 0 and late else whole

    def products(k, late, at, size):
        row = 1 - y if late else y
        with jax.named_scope(f"products{k}{late}"):
            for s in range(2):
                weight = w_down[block(k, row), :, pl.ds(at, size)]
                value = jnp.dot(hidden[s], weight, preferred_element_type=jnp.float32)
                part[k, late, s, :, pl.ds(at, size)] = value.astype(jnp.bfloat16)
        kk = k // 2
        for start, share in pieces(kk, late):
            if at <= start < at + size:
                columns = pl.ds(start, share)
                wires.send(
                    f"pc{k}{late}{start}",
                    part.at[k, late, :, :, columns],
                    part_in.at[kk, late, :, :, columns],
                    near_c,
                    f"pc{kk}{late}{start}",
                    mine_odd != k % 2,
                )

    def chip_sum(kk, late, at, size, only=None):
        columns = pl.ds(at, size)

        def run():
            wires.wait(f"pc{kk}{late}{at}", part_in.at[kk, late, :, :, columns])
            with jax.named_scope(f"chip_sum{kk}{late}"):
                kept = 2 * kk + mine_odd
                give = part[kept, late, 1, :, columns].astype(jnp.float32)
                give = give + part_in[kk, late, 1, :, columns].astype(jnp.float32)
                plane_send[kk, late, :, columns] = give.astype(jnp.bfloat16)

        guarded(only, run)
        tag = "" if only is None else "e" if only is even else "o"
        wires.send(
            f"pz{kk}{late}{at}{tag}",
            plane_send.at[kk, late, :, columns],
            plane_in.at[kk, late, :, columns],
            plane_of[1],
            f"pz{kk}{late}{at}",
            only,
        )

    def plane_sum(kk, late, at, size):
        columns = pl.ds(at, size)
        wires.wait(f"pz{kk}{late}{at}", plane_in.at[kk, late, :, columns])
        kept = 2 * kk + mine_odd
        with jax.named_scope(f"plane_sum{kk}{late}"):
            value = part[kept, late, 0, :, columns].astype(jnp.float32)
            value = value + part_in[kk, late, 0, :, columns].astype(jnp.float32)
            value = value + plane_in[kk, late, :, columns].astype(jnp.float32)

            def keep():
                own_sum[late, :, columns] = value

            def hand():
                chip_send[late, :, columns] = value.astype(jnp.bfloat16)

            pl.when(mine_late == kk)(keep)
            pl.when(mine_late != kk)(hand)
        for start, share in halves if late else whole:
            if at <= start < at + size:
                share_at = pl.ds(start, share)
                wires.send(
                    f"px{kk}{late}{start}",
                    chip_send.at[late, :, share_at],
                    chip_in.at[late, :, share_at],
                    near_x,
                    f"px{late}{start}",
                    mine_late != kk,
                )

    def pair_sum(kk, s):
        kept = 2 * kk + mine_odd
        return part[kept, 0, s].astype(jnp.float32) + part_in[kk, 0, s].astype(jnp.float32)

    def chip_give(kk):
        def run():
            wires.wait(f"pc{kk}00", part_in.at[kk, 0])
            with jax.named_scope(f"chip_give{kk}"):
                for s in range(2):
                    early_send[s] = pair_sum(kk, s).astype(jnp.bfloat16)

        passing = mine_late != kk
        pl.when(passing)(run)
        wires.send(f"px{kk}0", early_send, early_in, near_x, "px00", passing)

    def chip_take(kk):
        def run():
            wires.wait(f"pc{kk}00", part_in.at[kk, 0])
            wires.wait("px00", early_in)
            with jax.named_scope(f"chip_take{kk}"):
                own_sum[0] = pair_sum(kk, 0) + early_in[0].astype(jnp.float32)
                plane_send[1 - kk, 0] = (pair_sum(kk, 1) + early_in[1].astype(jnp.float32)).astype(jnp.bfloat16)

        taking = mine_late == kk
        pl.when(taking)(run)
        wires.send(f"pz{kk}0", plane_send.at[1 - kk, 0], plane_in.at[0, 0], plane_of[1], "pz00", taking)

    def down_wait(k):
        for at, size in halves if k == 1 else whole:
            wires.wait(f"dy{k}{at}", down_piece(k, 1 - y, at, size))

    even = mine_odd == 0
    uneven = mine_odd == 1
    all_of = (0, depth)
    products(0, 0, *all_of)
    down_pass(3, is_end)
    products(2, 0, *all_of)
    products(3, 0, *all_of)
    down_pass(1, is_end)
    chip_give(1)
    products(1, 0, *all_of)
    chip_give(0)
    down_wait(0)
    products(0, 1, *all_of)
    for at, size in halves:
        chip_sum(0, 1, at, size, even)
    down_wait(2)
    products(2, 1, *all_of)
    chip_take(1)
    down_wait(3)
    products(3, 1, *all_of)
    chip_sum(1, 1, *all_of)
    chip_take(0)
    for at, size in halves:
        wires.wait(f"dy1{at}", down_piece(1, 1 - y, at, size))
        products(1, 1, at, size)
        chip_sum(0, 1, at, size, uneven)
    plane_sum(1, 1, *all_of)
    for at, size in halves:
        plane_sum(0, 1, at, size)

    line = None
    for late, (start, share) in [(0, whole[0]), (1, halves[0]), (1, halves[1])]:
        columns = pl.ds(start, share)
        if late:
            arrived = chip_in.at[late, :, columns]
            wires.wait(f"px{late}{start}", arrived)
        else:
            arrived = plane_in.at[0, 0]
            wires.wait("pz00", arrived)
        with jax.named_scope(f"own_sum{late}"):
            total = own_sum[late, :, columns] + arrived[...].astype(jnp.float32)
            own_sum[late, :, columns] = total
            square = total * total
            folded = square[:, :LANES]
            for n in range(1, share // LANES):
                folded = folded + square[:, n * LANES : (n + 1) * LANES]
            found = jnp.sum(folded.T, axis=0, keepdims=True)
            line = found if line is None else line + found
    energy[t] = jnp.broadcast_to(line, energy.shape[1:])
    wires.send("ex", energy.at[t], energy.at[t], near_x)
    wires.send("exc", energy.at[t], energy.at[t], far_x)
    wires.send("ec", energy.at[t], energy.at[t], near_c)
    wires.wait("ex", energy.at[t_x])
    wires.wait("exc", energy.at[t_xc])
    wires.wait("ec", energy.at[t_c])
    line = energy[0, 0:1, :]
    for i in range(1, energy.shape[0]):
        line = line + energy[i, 0:1, :]
    with jax.named_scope("last"):
        scale = jnp.broadcast_to(lax.rsqrt(line / model + EPS), (LANES, length)).T
        for late, row in ((0, y), (1, 1 - y)):
            for n in range(depth // LANES):
                at = pl.ds(pl.multiple_of(row * depth + n * LANES, LANES), LANES)
                wide_at = pl.ds(pl.multiple_of(t * width + row * depth + n * LANES, LANES), LANES)
                value = own_sum[late, :, pl.ds(n * LANES, LANES)] * scale * channel_post[:, wide_at]
                out[:, at] = (mid[:, wide_at].astype(jnp.float32) + value).astype(jnp.bfloat16)
    wires.finish()


def pooled(*args):
    tokens, mixer_gain, recur_in, recur_gate, recur_out = args[0], args[1], args[2], args[5], args[9]
    hidden_gate, hidden_down = args[12], args[14]
    length, width = tokens.shape
    depth, channels = recur_in.shape
    model = mixer_gain.shape[0]
    units = hidden_gate.shape[1]
    half = units // 2
    padded = half // LANES * LANES + LANES
    blocks = PLANES * ROWS
    shares = CHIPS * CORES
    group = recur_gate.shape[-1]
    runs = channels // LANES
    bf16, f32 = jnp.bfloat16, jnp.float32
    anywhere = pl.BlockSpec(memory_space=pl.ANY)
    vmem = pl.BlockSpec(memory_space=pltpu.VMEM)
    small = (1, 4, 7, 8, 10, 11, 15)
    args = [arg.reshape(1, -1) if arg.ndim == 1 else arg for arg in args]
    scratch = [
        pltpu.VMEM((shares, length, width), bf16),
        pltpu.VMEM((length, model), bf16),
        pltpu.VMEM((model, 2 * channels), bf16),
        pltpu.VMEM((length, 2 * channels), bf16),
        pltpu.VMEM((2, 2, channels // group, group, group), bf16),
        pltpu.VMEM((runs, LANES, 4 * LANES), bf16),
        pltpu.VMEM((length, shares * channels), bf16),
        pltpu.VMEM((blocks, shares * channels, recur_out.shape[1]), bf16),
        pltpu.VMEM((length, model), f32),
        pltpu.VMEM((length, model), bf16),
        pltpu.VMEM((2, length, model), bf16),
        pltpu.VMEM((2, depth, LANES), bf16),
        pltpu.VMEM((model, units), bf16),
        pltpu.VMEM((depth, units), bf16),
        pltpu.VMEM((2, length, padded), bf16),
        pltpu.VMEM((blocks, padded, hidden_down.shape[1]), bf16),
        pltpu.VMEM((half, hidden_down.shape[1]), bf16),
        pltpu.VMEM((PLANES, 2, 2, length, depth), bf16),
        pltpu.VMEM((2, 2, 2, length, depth), bf16),
        pltpu.VMEM((2, length, depth), bf16),
        pltpu.VMEM((2, length, depth), bf16),
        pltpu.VMEM((2, length, depth), f32),
        pltpu.VMEM((2, 2, length, depth), bf16),
        pltpu.VMEM((2, 2, length, depth), bf16),
        pltpu.VMEM((2, length, depth), bf16),
        pltpu.VMEM((2, length, depth), bf16),
        pltpu.VMEM((shares, 8, length), f32),
        pltpu.SemaphoreType.DMA((128,)),
        pltpu.SemaphoreType.DMA((128,)),
        pltpu.SemaphoreType.DMA((40,)),
    ]
    return pl.pallas_call(
        pooled_kernel,
        out_shape=jax.ShapeDtypeStruct((length, width), bf16),
        in_specs=[vmem if index in small else anywhere for index in range(len(args))],
        out_specs=vmem,
        scratch_shapes=scratch,
        compiler_params=pltpu.CompilerParams(
            collective_id=0, has_side_effects=True, vmem_limit_bytes=63 * 2**20
        ),
    )(*args)


def solution(mesh):
    in_specs = (
        P("fs", "tp"),
        P(),
        P("fs", "tp"),
        P("fs", "tp"),
        P(),
        P(),
        P(),
        P(),
        P(),
        P("tp", "fs"),
        P(),
        P(),
        P("fs", "tp"),
        P("fs", "tp"),
        P("tp", "fs"),
        P(),
    )
    out_specs = P("fs", "tp")

    def body(*args):
        if pooled_fits(mesh, args):
            return pooled(*args)
        return on_device(snake_order(mesh), mesh.shape["tp"], *args)

    return jax.shard_map(body, mesh=mesh, in_specs=in_specs, out_specs=out_specs, check_vma=False)
```

```python
import functools

import jax
import jax.numpy as jnp
from jax import lax
from jax.experimental import pallas as pl
from jax.experimental.pallas import tpu as pltpu
from jax.sharding import PartitionSpec as P

EPS = 1e-06
SHRINK = 8.0
CORES = 2
FLIGHT = 5


def rms_scale(values, gain):
    return values * lax.rsqrt(jnp.mean(values * values, axis=-1, keepdims=True) + EPS) * gain


def snake_order(mesh):
    count = mesh.shape["fs"]
    axis = list(mesh.axis_names).index("fs")
    line = mesh.devices.take(0, axis=1 - axis).reshape(-1)
    where = [getattr(device, "coords", None) for device in line]
    if any(spot is None for spot in where):
        return list(range(count))
    at = {}
    for index, spot in enumerate(where):
        at[(spot[2], spot[1])] = index
    depth = 1 + max(z for z, _ in at)
    width = 1 + max(y for _, y in at)
    if depth * width != count or len(at) != count or width < 2 or depth % 2:
        return list(range(count))
    order = [at[(z, 0)] for z in range(depth)]
    for back, z in enumerate(reversed(range(depth))):
        columns = range(1, width)
        order += [at[(z, y)] for y in (columns if back % 2 == 0 else reversed(columns))]
    return order


class Ring:
    def __init__(self, order):
        self.n = len(order)
        self.order = order
        n = self.n
        self.pairs = {
            1: [(order[p], order[(p + 1) % n]) for p in range(n)],
            -1: [(order[p], order[(p - 1) % n]) for p in range(n)],
        }
        place = [0] * n
        for p, index in enumerate(order):
            place[index] = p
        self.order_row = jnp.array(order, jnp.int32)
        self.here = jnp.array(place, jnp.int32)[lax.axis_index("fs")]
        self.landed = {1: [], -1: []}

    def source(self, step):
        return self.order_row[lax.rem(self.here - step + self.n, self.n)]

    def send(self, value, way):
        landed = self.landed[way]
        if len(landed) >= FLIGHT:
            value = lax.optimization_barrier((value, landed[-FLIGHT]))[0]
        value = lax.ppermute(value, "fs", self.pairs[way])
        landed.append(value)
        return value

    def gather(self, shards, ties={}, paired=False, lead=1):
        n = self.n
        found = [[(self.source(0), shard)] for shard in shards]
        heads = [{1: shard, -1: shard} for shard in shards]
        for step in range(1, n // 2 + 1):
            for index in range(len(shards)):
                for way in (1, -1):
                    steps = n // 2 if (way == lead) == (index % 2 == 0 or paired) else n - 1 - n // 2
                    if step <= steps:
                        if step in ties:
                            heads[index][way] = lax.optimization_barrier((heads[index][way], ties[step]))[0]
                        heads[index][way] = self.send(heads[index][way], way)
                        found[index].append((self.source(way * step), heads[index][way]))
        return found


def stack_rows(blocks):
    height, width = blocks[0][1].shape
    total = jnp.zeros((height * len(blocks), width), blocks[0][1].dtype)
    for source, block in blocks:
        total = lax.dynamic_update_slice(total, block, (source * height, 0))
    return total


def stack_columns(blocks):
    height, width = blocks[0][1].shape
    total = jnp.zeros((height, width * len(blocks)), blocks[0][1].dtype)
    for source, block in blocks:
        total = lax.dynamic_update_slice(total, block, (0, source * width))
    return total


def swap_cores(value, count):
    return lax.ppermute(value, "tp", [(t, t ^ 1) for t in range(count)])


def from_chip(value, shift, count):
    return lax.ppermute(value, "tp", [(t, (t + CORES * shift) % count) for t in range(count)])


def chips_shares(value, count):
    chips = count // CORES
    chip = lax.axis_index("tp") // CORES
    found = [(chip, value)]
    for shift in range(1, chips):
        found.append((lax.rem(chip - shift + chips, chips), from_chip(value, shift, count)))
    return found


def gather_features(value, count):
    core = lax.rem(lax.axis_index("tp"), CORES)
    width = value.shape[1]
    total = jnp.zeros((value.shape[0], width * count), value.dtype)
    for chip, block in chips_shares(value, count):
        other = swap_cores(block, count)
        total = lax.dynamic_update_slice(total, block, (0, (chip * CORES + core) * width))
        total = lax.dynamic_update_slice(total, other, (0, (chip * CORES + 1 - core) * width))
    return total


def sum_all(value, count):
    core = lax.rem(lax.axis_index("tp"), CORES)
    half = value.shape[1] // CORES
    keep = lax.dynamic_slice_in_dim(value, core * half, half, 1)
    give = lax.dynamic_slice_in_dim(value, (1 - core) * half, half, 1)
    chip_sum = keep.astype(jnp.float32) + swap_cores(give, count).astype(jnp.float32)
    chip_sum = chip_sum.astype(jnp.bfloat16)
    total = 0.0
    for _, block in chips_shares(chip_sum, count):
        total = total + block.astype(jnp.float32)
    mine = total.astype(jnp.bfloat16)
    other = swap_cores(mine, count)
    low = jnp.where(core == 0, mine, other)
    high = jnp.where(core == 0, other, mine)
    return jnp.concatenate([low, high], axis=1)


def sum_own(value, count):
    rank = lax.axis_index("tp")
    core = lax.rem(rank, CORES)
    chip = rank // CORES
    chips = count // CORES
    length = value.shape[0]
    width = value.shape[1] // count

    def block(chip_at, core_at):
        at = (chip_at * CORES + core_at) * width
        return lax.dynamic_slice_in_dim(value, at, width, 1)

    total = 0.0
    for shift in list(range(1, chips)) + [0]:
        target = lax.rem(chip + shift, chips)
        part = block(target, core).astype(jnp.float32)
        part = part + swap_cores(block(target, 1 - core), count).astype(jnp.float32)
        if shift:
            part = from_chip(part.astype(jnp.bfloat16), shift, count).astype(jnp.float32)
        total = total + part
    return total


def minus_expm1(value):
    series = jnp.ones_like(value)
    for order in range(9, 1, -1):
        series = 1.0 + value * (1.0 / order) * series
    return jnp.where(value > -0.5, -value * series, 1.0 - jnp.exp(value))


def scan_block(decay, inflow, reverse):
    length = decay.shape[0]
    row = lax.broadcasted_iota(jnp.int32, decay.shape, 0)
    reach = 1
    while reach < length:
        if reverse:
            inside = row < length - reach
            turn = length - reach
        else:
            inside = row >= reach
            turn = reach
        before_inflow = jnp.where(inside, pltpu.roll(inflow, turn, 0), 0.0)
        inflow = inflow + decay * before_inflow
        if 2 * reach < length:
            decay = decay * jnp.where(inside, pltpu.roll(decay, turn, 0), 1.0)
        reach *= 2
    return inflow


def mixer_kernel(recur_ref, branch_ref, taps_ref, gate_ref, decay_ref, gain_ref, out_ref):
    recur = recur_ref[...].astype(jnp.float32)
    length, width = recur.shape
    row = lax.broadcasted_iota(jnp.int32, recur.shape, 0)
    taps = taps_ref[...]
    conv = taps[2:3] * recur
    for tap, shift in ((0, 2), (1, 1), (3, length - 1)):
        inside = row < length - 1 if tap == 3 else row >= shift
        conv = conv + taps[tap : tap + 1] * jnp.where(inside, pltpu.roll(recur, shift, 0), 0.0)
    first = conv.astype(jnp.bfloat16)
    rest = conv - first.astype(jnp.float32)
    second = rest.astype(jnp.bfloat16)
    third = (rest - second.astype(jnp.float32)).astype(jnp.bfloat16)
    total = None
    for direction in range(2):
        logits = []
        for kind in range(2):
            weight = gate_ref[0, :, pl.ds((direction * 2 + kind) * width, width)]
            logits.append(
                jnp.dot(third, weight, preferred_element_type=jnp.float32)
                + jnp.dot(second, weight, preferred_element_type=jnp.float32)
                + jnp.dot(first, weight, preferred_element_type=jnp.float32)
            )
        rate = 1.0 / (1.0 + jnp.exp(-logits[0]))
        inlet = 1.0 / (1.0 + jnp.exp(-logits[1]))
        log_decay = rate * decay_ref[direction : direction + 1, :]
        inflow = conv * inlet * jnp.sqrt(minus_expm1(2.0 * log_decay))
        state = scan_block(jnp.exp(log_decay), inflow, direction == 1)
        total = state if total is None else total + state
    branch = branch_ref[...].astype(jnp.float32)
    inner = 0.7978845608028654 * (branch + 0.044715 * (branch * branch * branch))
    gelu = branch * (0.5 * (1.0 + jnp.tanh(inner)))
    out_ref[...] = (total * gelu * gain_ref[...]).astype(jnp.bfloat16)


def mixer(both_x, taps, rate_own, inlet_own, decay_own, gain_own):
    length, channels = both_x.shape[0], both_x.shape[1] // 2
    group = rate_own.shape[-1]
    lanes = min(channels, 2 * group)
    blocks = channels // lanes
    per = lanes // group

    def dense(weight):
        spread = weight.reshape(2, blocks, per, group, 1, group) * jnp.eye(per, dtype=weight.dtype)[:, None, :, None]
        return spread.reshape(2, blocks, lanes, lanes)

    both = jnp.stack([dense(rate_own), dense(inlet_own)], axis=1)
    gates = both.transpose(2, 3, 0, 1, 4).reshape(blocks, lanes, 4 * lanes)
    slope = -SHRINK * jax.nn.softplus(-decay_own)
    column = lambda j: (0, j)
    return pl.pallas_call(
        mixer_kernel,
        grid=(blocks,),
        out_shape=jax.ShapeDtypeStruct((length, channels), jnp.bfloat16),
        in_specs=[
            pl.BlockSpec((length, lanes), column),
            pl.BlockSpec((length, lanes), lambda j: (0, blocks + j)),
            pl.BlockSpec((taps.shape[0], lanes), column),
            pl.BlockSpec((1, lanes, 4 * lanes), lambda j: (j, 0, 0)),
            pl.BlockSpec((2, lanes), column),
            pl.BlockSpec((1, lanes), column),
        ],
        out_specs=pl.BlockSpec((length, lanes), column),
        cost_estimate=pl.CostEstimate(flops=int(3e9), bytes_accessed=2**20, transcendentals=2**21),
        compiler_params=pltpu.CompilerParams(vmem_limit_bytes=24 * 2**20),
    )(both_x, both_x, taps, gates, slope, gain_own.reshape(1, channels))


def on_device(
    order,
    tp_count,
    tokens,
    mixer_gain,
    recur_in,
    branch_in,
    conv_taps,
    recur_gate,
    input_gate,
    decay_param,
    recur_gain,
    recur_out,
    mixer_post,
    channel_gain,
    hidden_gate,
    hidden_up,
    hidden_down,
    channel_post,
):
    rank_tp = lax.axis_index("tp")
    feature_width = tokens.shape[1]
    model_width = mixer_gain.shape[0]
    channel_width = recur_in.shape[1]
    group_count = channel_width // recur_gate.shape[-1]
    feature_start = rank_tp * feature_width
    channel_start = rank_tp * channel_width

    ring = Ring(order)
    packed = jnp.concatenate([recur_in, branch_in, recur_out.reshape(recur_in.shape)], axis=1)
    mix_blocks, gate_blocks = ring.gather([packed, hidden_gate])
    in_blocks = [(source, block[:, : 2 * channel_width]) for source, block in mix_blocks]
    out_blocks = [
        (source, block[:, 2 * channel_width :].reshape(recur_out.shape)) for source, block in mix_blocks
    ]

    gathered_in = gather_features(tokens, tp_count)
    gathered_float = gathered_in.astype(jnp.float32)
    normed_in = rms_scale(gathered_float, mixer_gain).astype(jnp.bfloat16)
    both_x = jnp.dot(normed_in, stack_rows(in_blocks), preferred_element_type=jnp.float32).astype(jnp.bfloat16)

    taps = lax.dynamic_slice_in_dim(conv_taps, channel_start, channel_width, 1).astype(jnp.float32)
    group_start = rank_tp * group_count
    rate_own = lax.dynamic_slice_in_dim(recur_gate, group_start, group_count, 1)
    inlet_own = lax.dynamic_slice_in_dim(input_gate, group_start, group_count, 1)
    decay_own = lax.dynamic_slice_in_dim(decay_param, channel_start, channel_width, 1)
    gain_own = lax.dynamic_slice_in_dim(recur_gain, channel_start, channel_width, 0)
    recur_y = mixer(both_x, taps, rate_own, inlet_own, decay_own, gain_own)

    (up_blocks,) = ring.gather([hidden_up], lead=-1)
    branch_part = jnp.dot(recur_y, stack_columns(out_blocks), preferred_element_type=jnp.float32)
    branch_sum = sum_all(branch_part.astype(jnp.bfloat16), tp_count).astype(jnp.float32)
    mid_full = (gathered_float + rms_scale(branch_sum, mixer_post)).astype(jnp.bfloat16)
    mid_own = lax.dynamic_slice_in_dim(mid_full, feature_start, feature_width, 1)
    channel_in = rms_scale(mid_full.astype(jnp.float32), channel_gain).astype(jnp.bfloat16)

    gate_total = jnp.dot(channel_in, stack_rows(gate_blocks), preferred_element_type=jnp.float32)
    up_total = jnp.dot(channel_in, stack_rows(up_blocks), preferred_element_type=jnp.float32)
    hidden = (jax.nn.silu(gate_total) * up_total).astype(jnp.bfloat16)

    cut = max(hidden_down.shape[0] // 256, 1) * 128
    low_blocks, high_blocks = ring.gather(
        [hidden_down[:cut], hidden_down[cut:]], {4: hidden}, True
    )
    part_blocks = []
    for (source, low), (_, high) in zip(low_blocks, high_blocks):
        part = jnp.dot(hidden[:, :cut], low, preferred_element_type=jnp.float32)
        part = part + jnp.dot(hidden[:, cut:], high, preferred_element_type=jnp.float32)
        part_blocks.append((source, part.astype(jnp.bfloat16)))
    hidden_part = stack_columns(part_blocks)
    hidden_own = sum_own(hidden_part, tp_count)
    energy_own = jnp.sum(hidden_own * hidden_own, axis=1).reshape(-1, 128)
    hidden_energy = lax.psum(energy_own, "tp").reshape(-1)
    close_own = lax.dynamic_slice_in_dim(channel_post, feature_start, feature_width, 0)
    return (
        mid_own.astype(jnp.float32)
        + hidden_own * lax.rsqrt(hidden_energy / model_width + EPS)[:, None] * close_own
    ).astype(jnp.bfloat16)


PLANES = 4
ROWS = 2
CHIPS = 2
MESH = pl.DeviceIdType.MESH
LANES = 128


def pooled_fits(mesh, args):
    if mesh.shape["fs"] != PLANES * ROWS or mesh.shape["tp"] != CHIPS * CORES:
        return False
    spots = [getattr(device, "coords", None) for device in mesh.devices.reshape(-1)]
    if all(spot is not None for spot in spots):
        if list(mesh.axis_names) != ["fs", "tp"]:
            return False
        at = mesh.devices
        for f in range(PLANES * ROWS):
            for t in range(CHIPS * CORES):
                if tuple(at[f, t].coords) != (t // CORES, f % ROWS, f // ROWS):
                    return False
    tokens, gate, down, recur_in, recur_out = args[0], args[12], args[14], args[2], args[9]
    half = gate.shape[1] // 2
    return (
        tokens.shape[1] % LANES == 0
        and tokens.shape[0] % 16 == 0
        and gate.shape[0] % 16 == 0
        and half % LANES == LANES // 2
        and down.shape[0] == gate.shape[1]
        and recur_in.shape[1] % LANES == 0
        and recur_out.shape[1] % LANES == 0
        and LANES % args[5].shape[-1] == 0
    )


class Wires:
    def __init__(self, sends, lands, nobody):
        self.sends = sends
        self.lands = lands
        self.nobody = nobody
        self.names = {}
        self.started = []

    def index(self, name):
        return self.names.setdefault(name, len(self.names))

    def send(self, name, source, target, to, land=None, only=None):
        copy = pltpu.make_async_remote_copy(
            src_ref=source,
            dst_ref=target,
            send_sem=self.sends.at[self.index(name)],
            recv_sem=self.lands.at[self.index(land or name)],
            device_id=to,
            device_id_type=MESH,
        )
        guarded(only, copy.start)
        self.started.append((only, copy))

    def wait(self, name, target):
        at = self.lands.at[self.index(name)]
        with jax.named_scope("wait_" + name):
            pltpu.make_async_remote_copy(
                src_ref=target,
                dst_ref=target,
                send_sem=at,
                recv_sem=at,
                device_id=self.nobody,
                device_id_type=MESH,
            ).wait_recv()

    def finish(self):
        with jax.named_scope("finish"):
            for only, copy in self.started:
                guarded(only, copy.wait_send)


def guarded(only, action):
    if only is None:
        action()
    else:
        pl.when(only)(action)


def scan_pair(conv, logits, slope, reverse):
    rate = 1.0 / (1.0 + jnp.exp(-logits[0]))
    inlet = 1.0 / (1.0 + jnp.exp(-logits[1]))
    log_decay = rate * slope
    inflow = conv * inlet * jnp.sqrt(minus_expm1(2.0 * log_decay))
    return scan_block(jnp.exp(log_decay), inflow, reverse)


def log_one_plus(value):
    total = 1.0 + value
    exact = total == 1.0
    return jnp.where(exact, value, jnp.log(total) * (value / jnp.where(exact, 1.0, total - 1.0)))


def pooled_kernel(
    tokens,
    mixer_gain,
    recur_in,
    branch_in,
    conv_taps,
    recur_gate,
    input_gate,
    decay_param,
    recur_gain,
    recur_out,
    mixer_post,
    channel_gain,
    hidden_gate,
    hidden_up,
    hidden_down,
    channel_post,
    out,
    tok,
    normed,
    w_in,
    both_x,
    gates_raw,
    gates,
    recur_all,
    w_out,
    branch,
    mid,
    channel_in,
    edge,
    w_gate_up,
    other_gate_up,
    hidden,
    w_down,
    other_down,
    part,
    part_in,
    chip_send,
    chip_in,
    own_sum,
    plane_send,
    plane_in,
    early_send,
    early_in,
    energy,
    sends,
    lands,
    local,
):
    f = lax.axis_index("fs")
    t = lax.axis_index("tp")
    z, y = lax.div(f, ROWS), lax.rem(f, ROWS)
    x, c = lax.div(t, CORES), lax.rem(t, CORES)
    zi, zp = lax.rem(z, 2), lax.div(z, 2)
    planes = [z, z + 1 - 2 * zi, lax.rem(z + 2, PLANES), PLANES - 1 - z]
    is_mid = lax.div(lax.rem(z + 1, PLANES), 2) == 1
    is_end = lax.div(lax.rem(z + 1, PLANES), 2) == 0
    length, width = tokens.shape
    depth = recur_in.shape[0]
    channels = recur_in.shape[1]
    units = hidden_gate.shape[1]
    half = units // 2
    wide = half // LANES * LANES
    narrow = half - wide
    full = wide // LANES
    model = tok.shape[0] * width
    group = recur_gate.shape[-1]
    blocks = PLANES * ROWS

    def device(plane, row, chip, core):
        return {"fs": plane * ROWS + row, "tp": chip * CORES + core}

    def block(k, row):
        return planes[k] * ROWS + row

    near_y = device(z, 1 - y, x, c)
    near_x = device(z, y, 1 - x, c)
    far_x = device(z, y, 1 - x, 1 - c)
    near_c = device(z, y, x, 1 - c)
    plane_of = [None] + [device(planes[k], y, x, c) for k in (1, 2, 3)]
    t_c = x * CORES + 1 - c
    t_x = (1 - x) * CORES + c
    t_xc = (1 - x) * CORES + 1 - c
    wires = Wires(sends, lands, near_c)
    rows_of = lambda at, size: pl.ds(pl.multiple_of(at * size, size), size)

    moves = {}

    def move(name, source, target):
        copy = pltpu.make_async_copy(source, target, local.at[len(moves)])
        copy.start()
        moves[name] = copy

    def here(prefix):
        for name, copy in moves.items():
            if name.startswith(prefix):
                copy.wait()

    move("io0", recur_in, w_in.at[rows_of(f, depth), pl.ds(0, channels)])
    move("io1", branch_in, w_in.at[rows_of(f, depth), pl.ds(channels, channels)])
    move("io2", recur_out, w_out.at[f, rows_of(t, channels), :])
    move("tok", tokens, tok.at[t])
    columns = lambda at: pl.ds(pl.multiple_of(at, LANES), LANES)
    for side, target, row_at, parity in (("a", w_gate_up, f, zi), ("b", other_gate_up, 0, 1 - zi)):
        for n in range(full):
            start = parity * (units - wide) + n * LANES
            for m, weight in enumerate((hidden_gate, hidden_up)):
                move(
                    f"gu{side}{n}{m}",
                    weight.at[:, columns(start)],
                    target.at[rows_of(row_at, depth), pl.ds((2 * n + m) * LANES, LANES)],
                )
    move("gum0", hidden_gate.at[:, pl.ds(wide, LANES)], edge.at[0])
    move("gum1", hidden_up.at[:, pl.ds(wide, LANES)], edge.at[1])
    group_count = channels // group
    move("gate0", recur_gate.at[:, rows_of(t, group_count)], gates_raw.at[0])
    move("gate1", input_gate.at[:, rows_of(t, group_count)], gates_raw.at[1])
    for side, target, parity in (("a", w_down.at[f], zi), ("b", other_down, 1 - zi)):
        wide_at = pl.multiple_of(parity * (units - wide), 2 * narrow)
        narrow_at = pl.multiple_of(wide + parity * narrow, narrow)
        move(f"dn{side}0", hidden_down.at[pl.ds(wide_at, wide), :], target.at[pl.ds(0, wide), :])
        move(f"dn{side}1", hidden_down.at[pl.ds(narrow_at, narrow), :], target.at[pl.ds(wide, narrow), :])

    barrier = pltpu.get_barrier_semaphore()
    peers = [near_y, near_x, far_x, near_c] + plane_of[1:]
    for peer in peers:
        pl.semaphore_signal(barrier, inc=1, device_id=peer, device_id_type=MESH)
    with jax.named_scope("barrier"):
        pl.semaphore_wait(barrier, len(peers))

    def in_slot(k, row):
        return w_in.at[rows_of(block(k, row), depth), :]

    def out_slot(k, row):
        return w_out.at[block(k, row), rows_of(t, channels), :]

    part_rows = depth // 2

    def gate_slot(k, row, piece):
        at = pl.multiple_of(block(k, row) * depth + piece * part_rows, part_rows)
        return w_gate_up.at[pl.ds(at, part_rows), :]

    def other_slot(piece):
        return other_gate_up.at[pl.ds(piece * part_rows, part_rows), :]

    def down_slot(k, row):
        return w_down.at[block(k, row), pl.ds(0, half), :]

    down_other = other_down

    slots = {"i": in_slot, "o": out_slot}

    def mixer_to_y(kind, k):
        slot = slots[kind](k, y)
        wires.send(f"{kind}y{k}", slot, slot, near_y)

    def mixer_to_x(k, row, tag):
        wires.send(f"ox{tag}{k}", out_slot(k, row), out_slot(k, row), near_x)

    def mixer_to_z(kind, name, k, to, land, only=None):
        slot = slots[kind](k, y)
        wires.send(kind + name, slot, slot, to, f"{kind}z{land}", only)

    def mixer_wait(kind, k, only=None):
        guarded(only, lambda: wires.wait(f"{kind}z{k}", slots[kind](k, y)))

    late_at = {
        "s": jnp.where(is_mid, planes[3], planes[2]) * ROWS,
        "t": jnp.where(is_mid, planes[2], planes[3]) * ROWS,
    }

    def late_slot(kind, tag, row):
        at = late_at[tag] + row
        if kind == "i":
            return w_in.at[rows_of(at, depth), :]
        return w_out.at[at, rows_of(t, channels), :]

    def late_to_y(kind, tag):
        slot = late_slot(kind, tag, y)
        wires.send(f"{kind}y{tag}", slot, slot, near_y)

    def late_to_x(tag, row, side):
        slot = late_slot("o", tag, row)
        wires.send(f"ox{side}{tag}", slot, slot, near_x)

    def gate_own_to_z(piece, which, only):
        if which == 1:
            wires.send(f"g{piece}s1", gate_slot(0, y, piece), gate_slot(0, y, piece), plane_of[2], f"gz{piece}2", only)
        else:
            k = 1 if which == 2 else 3
            source = other_slot(piece)
            wires.send(f"g{piece}s{which}", source, gate_slot(0, y, piece), plane_of[k], f"gz{piece}{k}", only)

    def down_own_to_z(which, only):
        if which == 1:
            wires.send("ds1", down_slot(0, y), down_slot(0, y), plane_of[2], "dz2", only)
        else:
            k = 1 if which == 2 else 3
            wires.send(f"ds{which}", down_other, down_slot(0, y), plane_of[k], f"dz{k}", only)

    def gate_to_y(k, piece):
        wires.send(f"gy{piece}{k}", gate_slot(k, y, piece), gate_slot(k, y, piece), near_y)

    def down_to_y(k):
        wires.send(f"dy{k}", down_slot(k, y), down_slot(k, y), near_y)

    def gate_pass(k, piece, only=None):
        guarded(only, lambda: wires.wait(f"gz{piece}{k}", gate_slot(k, y, piece)))
        if k == 1:
            passing = is_mid if only is None else only
            if passing is is_mid:
                slot = gate_slot(1, y, piece)
                wires.send(f"g{piece}r", slot, slot, plane_of[2], f"gz{piece}3", is_mid)
        slot = gate_slot(k, y, piece)
        wires.send(f"gy{piece}{k}", slot, slot, near_y, only=only)

    fine_width = depth // 2
    halves = ((0, fine_width), (fine_width, fine_width))
    whole = ((0, depth),)

    def down_piece(k, row, at, size):
        return w_down.at[block(k, row), pl.ds(0, half), pl.ds(at, size)]

    def down_come(k, only=None):
        guarded(only, lambda: wires.wait(f"dz{k}", down_slot(k, y)))

    def down_on(k, only=None):
        for at, size in halves if k == 1 else whole:
            slot = down_piece(k, y, at, size)
            wires.send(f"dy{k}{at}", slot, slot, near_y, only=only)

    def down_pass(k, only=None):
        down_come(k, only)
        down_on(k, only)

    here("io0")
    here("io1")
    mixer_to_y("i", 0)
    mixer_to_z("i", "z1", 0, plane_of[1], 1)
    mixer_to_z("i", "z3", 0, plane_of[3], 3, is_mid)
    here("tok")
    wires.send("tc", tok.at[t], tok.at[t], near_c)
    wires.send("tx", tok.at[t], tok.at[t], near_x)
    here("io2")
    mixer_to_y("o", 0)
    mixer_to_z("o", "z1", 0, plane_of[1], 1)
    mixer_to_z("o", "z3", 0, plane_of[3], 3, is_mid)

    here("gum")
    lane = lax.broadcasted_iota(jnp.int32, edge.shape[1:], 1)
    edge_gate = edge[0].astype(jnp.float32)
    edge_up = edge[1].astype(jnp.float32)
    low = jnp.where(lane < narrow, edge_gate, pltpu.roll(edge_up, narrow, 1))
    high = jnp.where(lane < narrow, pltpu.roll(edge_gate, narrow, 1), edge_up)
    odd = zi == 1
    edge_at = pl.ds(2 * wide, LANES)
    w_gate_up[rows_of(f, depth), edge_at] = jnp.where(odd, high, low).astype(jnp.bfloat16)
    other_gate_up[:, edge_at] = jnp.where(odd, low, high).astype(jnp.bfloat16)
    w_down[:, pl.ds(half, LANES - narrow), :] = jnp.zeros((blocks, LANES - narrow, w_down.shape[2]), jnp.bfloat16)
    here("gua")
    here("gub")

    gate_own_to_z(0, 2, is_end)
    gate_own_to_z(1, 2, is_end)

    mixer_wait("i", 1)
    mixer_to_z("i", "r1", 1, plane_of[3], 2, is_mid)
    mixer_to_y("i", 1)
    gate_to_y(0, 0)
    mixer_wait("i", 3, is_mid)
    mixer_to_z("i", "r3", 3, plane_of[1], 2, is_mid)

    wires.wait("tx", tok.at[t_x])
    wires.send("txc", tok.at[t_x], tok.at[t_x], near_c)

    mixer_wait("o", 1)
    mixer_to_z("o", "r1", 1, plane_of[3], 2, is_mid)
    gate_own_to_z(0, 3, is_mid)
    mixer_wait("i", 2)
    late_to_y("i", "s")
    mixer_to_z("i", "r2", 2, plane_of[1], 3, is_mid)
    mixer_wait("o", 3, is_mid)
    mixer_to_z("o", "r3", 3, plane_of[1], 2, is_mid)
    mixer_to_x(0, y, "a")
    here("gate")
    per = LANES // group
    runs = channels // LANES
    for j in range(runs):
        for direction in range(2):
            for kind in range(2):
                dense = None
                for a in range(per):
                    spread_row = lax.broadcasted_iota(jnp.int32, (group, LANES), 0)
                    spread_lane = lax.broadcasted_iota(jnp.int32, (group, LANES), 1)
                    spread = (spread_lane == spread_row + a * group).astype(jnp.bfloat16)
                    lift_row = lax.broadcasted_iota(jnp.int32, (LANES, group), 0)
                    lift_lane = lax.broadcasted_iota(jnp.int32, (LANES, group), 1)
                    lift = (lift_row == lift_lane + a * group).astype(jnp.bfloat16)
                    block_map = gates_raw[kind, direction, j * per + a]
                    block_map = jnp.dot(block_map, spread, preferred_element_type=jnp.float32).astype(jnp.bfloat16)
                    block_map = jnp.dot(lift, block_map, preferred_element_type=jnp.float32)
                    dense = block_map if dense is None else dense + block_map
                gates[j, :, pl.ds((direction * 2 + kind) * LANES, LANES)] = dense.astype(jnp.bfloat16)

    mixer_wait("i", 3, is_end)
    late_to_y("i", "t")
    mixer_to_y("o", 1)
    mixer_wait("o", 2)
    late_to_y("o", "s")
    mixer_to_z("o", "r2", 2, plane_of[1], 3, is_mid)
    gate_own_to_z(0, 2, is_mid)
    gate_own_to_z(0, 1, None)
    gate_pass(1, 0, is_mid)
    wires.wait("tc", tok.at[t_c])
    wires.wait("txc", tok.at[t_xc])
    fine = 16

    with jax.named_scope("norm"):

        @pl.loop(0, length // fine, unroll=2)
        def _(r):
            rows = rows_of(r, fine)
            values = jnp.concatenate([tok[i, rows, :] for i in range(tok.shape[0])], axis=1).astype(jnp.float32)
            normed[rows, :] = rms_scale(values, mixer_gain[...]).astype(jnp.bfloat16)

    mixer_wait("o", 3, is_end)
    late_to_y("o", "t")
    gate_to_y(0, 1)
    gate_own_to_z(1, 2, is_mid)
    gate_own_to_z(1, 3, is_mid)
    gate_own_to_z(1, 1, None)
    here("dn")
    down_own_to_z(2, is_end)
    gate_pass(1, 1, is_mid)
    wires.wait("oy0", out_slot(0, 1 - y))
    mixer_to_x(0, 1 - y, "b")
    mixer_to_x(1, y, "a")
    for k in (0, 1):
        wires.wait(f"iy{k}", in_slot(k, 1 - y))
    for tag in ("s", "t"):
        wires.wait(f"iy{tag}", late_slot("i", tag, 1 - y))

    with jax.named_scope("in_proj"):

        @pl.loop(0, 2)
        def _(j):
            at = rows_of(j, channels)
            product = jnp.dot(normed[...], w_in[:, at], preferred_element_type=jnp.float32)
            both_x[:, at] = product.astype(jnp.bfloat16)


    own_channels = pl.multiple_of(t * channels, LANES)

    with jax.named_scope("scan"):

        @pl.loop(0, runs)
        def _(j):
            at = pl.ds(pl.multiple_of(j * LANES, LANES), LANES)
            gate_at = pl.ds(pl.multiple_of(channels + j * LANES, LANES), LANES)
            table_at = pl.ds(pl.multiple_of(own_channels + j * LANES, LANES), LANES)
            recur = both_x[:, at].astype(jnp.float32)
            row = lax.broadcasted_iota(jnp.int32, recur.shape, 0)
            taps = conv_taps[:, table_at].astype(jnp.float32)
            conv = taps[2:3] * recur
            for tap, shift in ((0, 2), (1, 1), (3, length - 1)):
                inside = row < length - 1 if tap == 3 else row >= shift
                conv = conv + taps[tap : tap + 1] * jnp.where(inside, pltpu.roll(recur, shift, 0), 0.0)
            first = conv.astype(jnp.bfloat16)
            rest = conv - first.astype(jnp.float32)
            second_part = rest.astype(jnp.bfloat16)
            third_part = (rest - second_part.astype(jnp.float32)).astype(jnp.bfloat16)
            decay = decay_param[:, table_at]
            slope = -SHRINK * (jnp.maximum(-decay, 0.0) + log_one_plus(jnp.exp(-jnp.abs(decay))))
            total = None
            for direction in range(2):
                logits = []
                for kind in range(2):
                    weight = gates[j, :, pl.ds((direction * 2 + kind) * LANES, LANES)]
                    logits.append(
                        jnp.dot(third_part, weight, preferred_element_type=jnp.float32)
                        + jnp.dot(second_part, weight, preferred_element_type=jnp.float32)
                        + jnp.dot(first, weight, preferred_element_type=jnp.float32)
                    )
                state = scan_pair(conv, logits, slope[direction : direction + 1], direction == 1)
                total = state if total is None else total + state
            value = both_x[:, gate_at].astype(jnp.float32)
            inner = 0.7978845608028654 * (value + 0.044715 * (value * value * value))
            gelu = value * (0.5 * (1.0 + jnp.tanh(inner)))
            recur_all[:, table_at] = (total * gelu * recur_gain[:, table_at]).astype(jnp.bfloat16)

    mine = recur_all.at[:, rows_of(t, channels)]
    wires.send("rx", mine, mine, near_x)
    wires.send("rc", mine, mine, near_c)
    wires.wait("oy1", out_slot(1, 1 - y))
    mixer_to_x(1, 1 - y, "b")
    late_to_x("s", y, "a")
    late_to_x("t", y, "a")
    gate_pass(1, 0, is_end)
    wires.send("dy00", down_slot(0, y), down_slot(0, y), near_y, only=is_end)
    gate_pass(3, 0, is_mid)
    for tag in ("s", "t"):
        wires.wait(f"oy{tag}", late_slot("o", tag, 1 - y))
        late_to_x(tag, 1 - y, "b")
    wires.send("oc1", w_out.at[:, rows_of(t, channels), :], w_out.at[:, rows_of(t, channels), :], near_c)
    for k in (0, 1):
        for side, row in (("a", y), ("b", 1 - y)):
            wires.wait(f"ox{side}{k}", w_out.at[block(k, row), rows_of(t_x, channels), :])
    for tag in ("s", "t"):
        for side, row in (("a", y), ("b", 1 - y)):
            wires.wait(f"ox{side}{tag}", w_out.at[late_at[tag] + row, rows_of(t_x, channels), :])
    wires.send("oc2", w_out.at[:, rows_of(t_x, channels), :], w_out.at[:, rows_of(t_x, channels), :], near_c)
    theirs = recur_all.at[:, rows_of(t_x, channels)]
    wires.wait("rx", theirs)
    wires.send("rxc", theirs, theirs, near_c)
    wires.wait("oc1", w_out.at[:, rows_of(t_c, channels), :])
    wires.wait("oc2", w_out.at[:, rows_of(t_xc, channels), :])
    wires.wait("rc", recur_all.at[:, rows_of(t_c, channels)])
    wires.wait("rxc", recur_all.at[:, rows_of(t_xc, channels)])

    gate_pass(2, 0, is_end)
    with jax.named_scope("branch_dot"):

        @pl.loop(0, blocks)
        def _(b):
            branch[:, rows_of(b, depth)] = jnp.dot(recur_all[...], w_out[b], preferred_element_type=jnp.float32)

    def quarter(s, at, piece):
        return channel_in.at[s, pl.ds(piece * (length // 2), length // 2), rows_of(at, width)]

    for piece in range(2):
        with jax.named_scope(f"branch_norm{piece}"):

            @pl.loop(piece * length // 2 // fine, (piece + 1) * length // 2 // fine, unroll=2)
            def _(r):
                rows = rows_of(r, fine)
                values = jnp.concatenate([tok[i, rows, :] for i in range(tok.shape[0])], axis=1).astype(jnp.float32)
                middle = (values + rms_scale(branch[rows, :], mixer_post[...])).astype(jnp.bfloat16)
                mid[rows, :] = middle
                channel_in[0, rows, :] = rms_scale(middle.astype(jnp.float32), channel_gain[...]).astype(jnp.bfloat16)

        wires.send(f"cz{piece}", quarter(0, t, piece), quarter(1, t, piece), plane_of[1])

    down_own_to_z(2, is_mid)
    gate_pass(2, 0, is_mid)
    gate_pass(1, 1, is_end)
    gate_pass(3, 1, is_mid)
    gate_pass(3, 0, is_end)
    down_own_to_z(3, is_mid)
    down_own_to_z(1, is_end)
    wires.wait("cz0", quarter(1, t, 0))
    wires.send("cx0", quarter(1, t, 0), quarter(1, t, 0), near_x)
    wires.send("cca0", quarter(1, t, 0), quarter(1, t, 0), near_c)
    gate_pass(2, 1)
    wires.wait("cz1", quarter(1, t, 1))
    wires.send("cx1", quarter(1, t, 1), quarter(1, t, 1), near_x)
    wires.send("cca1", quarter(1, t, 1), quarter(1, t, 1), near_c)
    gate_pass(3, 1, is_end)
    wires.send("dy00", down_slot(0, y), down_slot(0, y), near_y, only=is_mid)
    for piece in range(2):
        wires.wait(f"cx{piece}", quarter(1, t_x, piece))
        wires.send(f"ccb{piece}", quarter(1, t_x, piece), quarter(1, t_x, piece), near_c)
    for piece in range(2):
        wires.wait(f"cca{piece}", quarter(1, t_c, piece))
        wires.wait(f"ccb{piece}", quarter(1, t_xc, piece))
    down_own_to_z(1, is_mid)
    down_come(1, is_mid)
    wires.send("dr", down_slot(1, y), down_slot(1, y), plane_of[2], "dz3", is_mid)
    down_come(3, is_mid)
    down_pass(2, is_mid)
    down_on(3, is_mid)
    down_on(1, is_mid)
    down_pass(2, is_end)
    for k in range(PLANES):
        for piece in range(2):
            wires.wait(f"gy{piece}{k}", gate_slot(k, 1 - y, piece))

    def gate_up(first, last):
        with jax.named_scope(f"gate_up{first}"):

            @pl.loop(first, last)
            def _(n):
                at = pl.ds(pl.multiple_of(n * 2 * LANES, 2 * LANES), 2 * LANES)
                store = pl.ds(pl.multiple_of(n * LANES, LANES), LANES)
                for s in range(2):
                    product = jnp.dot(channel_in[s], w_gate_up[:, at], preferred_element_type=jnp.float32)
                    gate_value, up_value = product[:, :LANES], product[:, LANES:]
                    hidden[s, :, store] = (jax.nn.silu(gate_value) * up_value).astype(jnp.bfloat16)

    gate_up(0, full // 2 + 1)
    down_pass(3, is_end)
    gate_up(full // 2 + 1, full)

    lane_tail = lax.broadcasted_iota(jnp.int32, (length, LANES), 1)
    for s in range(2):
        product = jnp.dot(channel_in[s], w_gate_up[:, edge_at], preferred_element_type=jnp.float32)
        value = jax.nn.silu(product) * pltpu.roll(product, narrow, 1)
        hidden[s, :, pl.ds(wide, LANES)] = jnp.where(lane_tail < narrow, value, 0.0).astype(jnp.bfloat16)

    mine_odd = lax.rem(zi + c, 2)
    mine_late = lax.rem(zp + x, 2)

    def pieces(kk, late):
        return halves if kk == 0 and late else whole

    def products(k, late, at, size):
        row = 1 - y if late else y
        with jax.named_scope(f"products{k}{late}"):
            for s in range(2):
                weight = w_down[block(k, row), :, pl.ds(at, size)]
                value = jnp.dot(hidden[s], weight, preferred_element_type=jnp.float32)
                part[k, late, s, :, pl.ds(at, size)] = value.astype(jnp.bfloat16)
        kk = k // 2
        for start, share in pieces(kk, late):
            if at <= start < at + size:
                columns = pl.ds(start, share)
                wires.send(
                    f"pc{k}{late}{start}",
                    part.at[k, late, :, :, columns],
                    part_in.at[kk, late, :, :, columns],
                    near_c,
                    f"pc{kk}{late}{start}",
                    mine_odd != k % 2,
                )

    def chip_sum(kk, late, at, size, only=None):
        columns = pl.ds(at, size)

        def run():
            wires.wait(f"pc{kk}{late}{at}", part_in.at[kk, late, :, :, columns])
            with jax.named_scope(f"chip_sum{kk}{late}"):
                kept = 2 * kk + mine_odd
                give = part[kept, late, 1, :, columns].astype(jnp.float32)
                give = give + part_in[kk, late, 1, :, columns].astype(jnp.float32)
                plane_send[kk, late, :, columns] = give.astype(jnp.bfloat16)

        guarded(only, run)
        tag = "" if only is None else "e" if only is even else "o"
        wires.send(
            f"pz{kk}{late}{at}{tag}",
            plane_send.at[kk, late, :, columns],
            plane_in.at[kk, late, :, columns],
            plane_of[1],
            f"pz{kk}{late}{at}",
            only,
        )

    def plane_sum(kk, late, at, size):
        columns = pl.ds(at, size)
        wires.wait(f"pz{kk}{late}{at}", plane_in.at[kk, late, :, columns])
        kept = 2 * kk + mine_odd
        with jax.named_scope(f"plane_sum{kk}{late}"):
            value = part[kept, late, 0, :, columns].astype(jnp.float32)
            value = value + part_in[kk, late, 0, :, columns].astype(jnp.float32)
            value = value + plane_in[kk, late, :, columns].astype(jnp.float32)

            def keep():
                own_sum[late, :, columns] = value

            def hand():
                chip_send[late, :, columns] = value.astype(jnp.bfloat16)

            pl.when(mine_late == kk)(keep)
            pl.when(mine_late != kk)(hand)
        for start, share in halves if late else whole:
            if at <= start < at + size:
                share_at = pl.ds(start, share)
                wires.send(
                    f"px{kk}{late}{start}",
                    chip_send.at[late, :, share_at],
                    chip_in.at[late, :, share_at],
                    near_x,
                    f"px{late}{start}",
                    mine_late != kk,
                )

    def pair_sum(kk, s):
        kept = 2 * kk + mine_odd
        return part[kept, 0, s].astype(jnp.float32) + part_in[kk, 0, s].astype(jnp.float32)

    def chip_give(kk):
        def run():
            wires.wait(f"pc{kk}00", part_in.at[kk, 0])
            with jax.named_scope(f"chip_give{kk}"):
                for s in range(2):
                    early_send[s] = pair_sum(kk, s).astype(jnp.bfloat16)

        passing = mine_late != kk
        pl.when(passing)(run)
        wires.send(f"px{kk}0", early_send, early_in, near_x, "px00", passing)

    def chip_take(kk):
        def run():
            wires.wait(f"pc{kk}00", part_in.at[kk, 0])
            wires.wait("px00", early_in)
            with jax.named_scope(f"chip_take{kk}"):
                own_sum[0] = pair_sum(kk, 0) + early_in[0].astype(jnp.float32)
                plane_send[1 - kk, 0] = (pair_sum(kk, 1) + early_in[1].astype(jnp.float32)).astype(jnp.bfloat16)

        taking = mine_late == kk
        pl.when(taking)(run)
        wires.send(f"pz{kk}0", plane_send.at[1 - kk, 0], plane_in.at[0, 0], plane_of[1], "pz00", taking)

    def down_wait(k):
        for at, size in halves if k == 1 else whole:
            wires.wait(f"dy{k}{at}", down_piece(k, 1 - y, at, size))

    even = mine_odd == 0
    uneven = mine_odd == 1
    all_of = (0, depth)
    products(0, 0, *all_of)
    products(2, 0, *all_of)
    products(3, 0, *all_of)
    down_pass(1, is_end)
    chip_give(1)
    products(1, 0, *all_of)
    chip_give(0)
    down_wait(0)
    products(0, 1, *all_of)
    for at, size in halves:
        chip_sum(0, 1, at, size, even)
    down_wait(2)
    products(2, 1, *all_of)
    down_wait(3)
    products(3, 1, *all_of)
    chip_sum(1, 1, *all_of)
    for at, size in halves:
        wires.wait(f"dy1{at}", down_piece(1, 1 - y, at, size))
        products(1, 1, at, size)
        chip_sum(0, 1, at, size, uneven)
    chip_take(1)
    chip_take(0)
    plane_sum(1, 1, *all_of)
    for at, size in halves:
        plane_sum(0, 1, at, size)

    line = None
    for late, (start, share) in [(0, whole[0]), (1, halves[0]), (1, halves[1])]:
        columns = pl.ds(start, share)
        if late:
            arrived = chip_in.at[late, :, columns]
            wires.wait(f"px{late}{start}", arrived)
        else:
            arrived = plane_in.at[0, 0]
            wires.wait("pz00", arrived)
        with jax.named_scope(f"own_sum{late}"):
            total = own_sum[late, :, columns] + arrived[...].astype(jnp.float32)
            own_sum[late, :, columns] = total
            square = total * total
            folded = square[:, :LANES]
            for n in range(1, share // LANES):
                folded = folded + square[:, n * LANES : (n + 1) * LANES]
            found = jnp.sum(folded.T, axis=0, keepdims=True)
            line = found if line is None else line + found
    energy[t] = jnp.broadcast_to(line, energy.shape[1:])
    wires.send("ex", energy.at[t], energy.at[t], near_x)
    wires.send("exc", energy.at[t], energy.at[t], far_x)
    wires.send("ec", energy.at[t], energy.at[t], near_c)
    wires.wait("ex", energy.at[t_x])
    wires.wait("exc", energy.at[t_xc])
    wires.wait("ec", energy.at[t_c])
    line = energy[0, 0:1, :]
    for i in range(1, energy.shape[0]):
        line = line + energy[i, 0:1, :]
    with jax.named_scope("last"):
        scale = jnp.broadcast_to(lax.rsqrt(line / model + EPS), (LANES, length)).T
        for late, row in ((0, y), (1, 1 - y)):
            for n in range(depth // LANES):
                at = pl.ds(pl.multiple_of(row * depth + n * LANES, LANES), LANES)
                wide_at = pl.ds(pl.multiple_of(t * width + row * depth + n * LANES, LANES), LANES)
                value = own_sum[late, :, pl.ds(n * LANES, LANES)] * scale * channel_post[:, wide_at]
                out[:, at] = (mid[:, wide_at].astype(jnp.float32) + value).astype(jnp.bfloat16)
    wires.finish()


def pooled(*args):
    tokens, mixer_gain, recur_in, recur_gate, recur_out = args[0], args[1], args[2], args[5], args[9]
    hidden_gate, hidden_down = args[12], args[14]
    length, width = tokens.shape
    depth, channels = recur_in.shape
    model = mixer_gain.shape[0]
    units = hidden_gate.shape[1]
    half = units // 2
    padded = half // LANES * LANES + LANES
    blocks = PLANES * ROWS
    shares = CHIPS * CORES
    group = recur_gate.shape[-1]
    runs = channels // LANES
    bf16, f32 = jnp.bfloat16, jnp.float32
    anywhere = pl.BlockSpec(memory_space=pl.ANY)
    vmem = pl.BlockSpec(memory_space=pltpu.VMEM)
    small = (1, 4, 7, 8, 10, 11, 15)
    args = [arg.reshape(1, -1) if arg.ndim == 1 else arg for arg in args]
    scratch = [
        pltpu.VMEM((shares, length, width), bf16),
        pltpu.VMEM((length, model), bf16),
        pltpu.VMEM((model, 2 * channels), bf16),
        pltpu.VMEM((length, 2 * channels), bf16),
        pltpu.VMEM((2, 2, channels // group, group, group), bf16),
        pltpu.VMEM((runs, LANES, 4 * LANES), bf16),
        pltpu.VMEM((length, shares * channels), bf16),
        pltpu.VMEM((blocks, shares * channels, recur_out.shape[1]), bf16),
        pltpu.VMEM((length, model), f32),
        pltpu.VMEM((length, model), bf16),
        pltpu.VMEM((2, length, model), bf16),
        pltpu.VMEM((2, depth, LANES), bf16),
        pltpu.VMEM((model, units), bf16),
        pltpu.VMEM((depth, units), bf16),
        pltpu.VMEM((2, length, padded), bf16),
        pltpu.VMEM((blocks, padded, hidden_down.shape[1]), bf16),
        pltpu.VMEM((half, hidden_down.shape[1]), bf16),
        pltpu.VMEM((PLANES, 2, 2, length, depth), bf16),
        pltpu.VMEM((2, 2, 2, length, depth), bf16),
        pltpu.VMEM((2, length, depth), bf16),
        pltpu.VMEM((2, length, depth), bf16),
        pltpu.VMEM((2, length, depth), f32),
        pltpu.VMEM((2, 2, length, depth), bf16),
        pltpu.VMEM((2, 2, length, depth), bf16),
        pltpu.VMEM((2, length, depth), bf16),
        pltpu.VMEM((2, length, depth), bf16),
        pltpu.VMEM((shares, 8, length), f32),
        pltpu.SemaphoreType.DMA((128,)),
        pltpu.SemaphoreType.DMA((128,)),
        pltpu.SemaphoreType.DMA((40,)),
    ]
    return pl.pallas_call(
        pooled_kernel,
        out_shape=jax.ShapeDtypeStruct((length, width), bf16),
        in_specs=[vmem if index in small else anywhere for index in range(len(args))],
        out_specs=vmem,
        scratch_shapes=scratch,
        compiler_params=pltpu.CompilerParams(
            collective_id=0, has_side_effects=True, vmem_limit_bytes=63 * 2**20
        ),
    )(*args)


def solution(mesh):
    in_specs = (
        P("fs", "tp"),
        P(),
        P("fs", "tp"),
        P("fs", "tp"),
        P(),
        P(),
        P(),
        P(),
        P(),
        P("tp", "fs"),
        P(),
        P(),
        P("fs", "tp"),
        P("fs", "tp"),
        P("tp", "fs"),
        P(),
    )
    out_specs = P("fs", "tp")

    def body(*args):
        if pooled_fits(mesh, args):
            return pooled(*args)
        return on_device(snake_order(mesh), mesh.shape["tp"], *args)

    return jax.shard_map(body, mesh=mesh, in_specs=in_specs, out_specs=out_specs, check_vma=False)
```

```python
import functools

import jax
import jax.numpy as jnp
from jax import lax
from jax.experimental import pallas as pl
from jax.experimental.pallas import tpu as pltpu
from jax.sharding import PartitionSpec as P

EPS = 1e-06
SHRINK = 8.0
CORES = 2
FLIGHT = 5


def rms_scale(values, gain):
    return values * lax.rsqrt(jnp.mean(values * values, axis=-1, keepdims=True) + EPS) * gain


def snake_order(mesh):
    count = mesh.shape["fs"]
    axis = list(mesh.axis_names).index("fs")
    line = mesh.devices.take(0, axis=1 - axis).reshape(-1)
    where = [getattr(device, "coords", None) for device in line]
    if any(spot is None for spot in where):
        return list(range(count))
    at = {}
    for index, spot in enumerate(where):
        at[(spot[2], spot[1])] = index
    depth = 1 + max(z for z, _ in at)
    width = 1 + max(y for _, y in at)
    if depth * width != count or len(at) != count or width < 2 or depth % 2:
        return list(range(count))
    order = [at[(z, 0)] for z in range(depth)]
    for back, z in enumerate(reversed(range(depth))):
        columns = range(1, width)
        order += [at[(z, y)] for y in (columns if back % 2 == 0 else reversed(columns))]
    return order


class Ring:
    def __init__(self, order):
        self.n = len(order)
        self.order = order
        n = self.n
        self.pairs = {
            1: [(order[p], order[(p + 1) % n]) for p in range(n)],
            -1: [(order[p], order[(p - 1) % n]) for p in range(n)],
        }
        place = [0] * n
        for p, index in enumerate(order):
            place[index] = p
        self.order_row = jnp.array(order, jnp.int32)
        self.here = jnp.array(place, jnp.int32)[lax.axis_index("fs")]
        self.landed = {1: [], -1: []}

    def source(self, step):
        return self.order_row[lax.rem(self.here - step + self.n, self.n)]

    def send(self, value, way):
        landed = self.landed[way]
        if len(landed) >= FLIGHT:
            value = lax.optimization_barrier((value, landed[-FLIGHT]))[0]
        value = lax.ppermute(value, "fs", self.pairs[way])
        landed.append(value)
        return value

    def gather(self, shards, ties={}, paired=False, lead=1):
        n = self.n
        found = [[(self.source(0), shard)] for shard in shards]
        heads = [{1: shard, -1: shard} for shard in shards]
        for step in range(1, n // 2 + 1):
            for index in range(len(shards)):
                for way in (1, -1):
                    steps = n // 2 if (way == lead) == (index % 2 == 0 or paired) else n - 1 - n // 2
                    if step <= steps:
                        if step in ties:
                            heads[index][way] = lax.optimization_barrier((heads[index][way], ties[step]))[0]
                        heads[index][way] = self.send(heads[index][way], way)
                        found[index].append((self.source(way * step), heads[index][way]))
        return found


def stack_rows(blocks):
    height, width = blocks[0][1].shape
    total = jnp.zeros((height * len(blocks), width), blocks[0][1].dtype)
    for source, block in blocks:
        total = lax.dynamic_update_slice(total, block, (source * height, 0))
    return total


def stack_columns(blocks):
    height, width = blocks[0][1].shape
    total = jnp.zeros((height, width * len(blocks)), blocks[0][1].dtype)
    for source, block in blocks:
        total = lax.dynamic_update_slice(total, block, (0, source * width))
    return total


def swap_cores(value, count):
    return lax.ppermute(value, "tp", [(t, t ^ 1) for t in range(count)])


def from_chip(value, shift, count):
    return lax.ppermute(value, "tp", [(t, (t + CORES * shift) % count) for t in range(count)])


def chips_shares(value, count):
    chips = count // CORES
    chip = lax.axis_index("tp") // CORES
    found = [(chip, value)]
    for shift in range(1, chips):
        found.append((lax.rem(chip - shift + chips, chips), from_chip(value, shift, count)))
    return found


def gather_features(value, count):
    core = lax.rem(lax.axis_index("tp"), CORES)
    width = value.shape[1]
    total = jnp.zeros((value.shape[0], width * count), value.dtype)
    for chip, block in chips_shares(value, count):
        other = swap_cores(block, count)
        total = lax.dynamic_update_slice(total, block, (0, (chip * CORES + core) * width))
        total = lax.dynamic_update_slice(total, other, (0, (chip * CORES + 1 - core) * width))
    return total


def sum_all(value, count):
    core = lax.rem(lax.axis_index("tp"), CORES)
    half = value.shape[1] // CORES
    keep = lax.dynamic_slice_in_dim(value, core * half, half, 1)
    give = lax.dynamic_slice_in_dim(value, (1 - core) * half, half, 1)
    chip_sum = keep.astype(jnp.float32) + swap_cores(give, count).astype(jnp.float32)
    chip_sum = chip_sum.astype(jnp.bfloat16)
    total = 0.0
    for _, block in chips_shares(chip_sum, count):
        total = total + block.astype(jnp.float32)
    mine = total.astype(jnp.bfloat16)
    other = swap_cores(mine, count)
    low = jnp.where(core == 0, mine, other)
    high = jnp.where(core == 0, other, mine)
    return jnp.concatenate([low, high], axis=1)


def sum_own(value, count):
    rank = lax.axis_index("tp")
    core = lax.rem(rank, CORES)
    chip = rank // CORES
    chips = count // CORES
    length = value.shape[0]
    width = value.shape[1] // count

    def block(chip_at, core_at):
        at = (chip_at * CORES + core_at) * width
        return lax.dynamic_slice_in_dim(value, at, width, 1)

    total = 0.0
    for shift in list(range(1, chips)) + [0]:
        target = lax.rem(chip + shift, chips)
        part = block(target, core).astype(jnp.float32)
        part = part + swap_cores(block(target, 1 - core), count).astype(jnp.float32)
        if shift:
            part = from_chip(part.astype(jnp.bfloat16), shift, count).astype(jnp.float32)
        total = total + part
    return total


def minus_expm1(value):
    series = jnp.ones_like(value)
    for order in range(9, 1, -1):
        series = 1.0 + value * (1.0 / order) * series
    return jnp.where(value > -0.5, -value * series, 1.0 - jnp.exp(value))


def scan_block(decay, inflow, reverse):
    length = decay.shape[0]
    row = lax.broadcasted_iota(jnp.int32, decay.shape, 0)
    reach = 1
    while reach < length:
        if reverse:
            inside = row < length - reach
            turn = length - reach
        else:
            inside = row >= reach
            turn = reach
        before_inflow = jnp.where(inside, pltpu.roll(inflow, turn, 0), 0.0)
        inflow = inflow + decay * before_inflow
        if 2 * reach < length:
            decay = decay * jnp.where(inside, pltpu.roll(decay, turn, 0), 1.0)
        reach *= 2
    return inflow


def mixer_kernel(recur_ref, branch_ref, taps_ref, gate_ref, decay_ref, gain_ref, out_ref):
    recur = recur_ref[...].astype(jnp.float32)
    length, width = recur.shape
    row = lax.broadcasted_iota(jnp.int32, recur.shape, 0)
    taps = taps_ref[...]
    conv = taps[2:3] * recur
    for tap, shift in ((0, 2), (1, 1), (3, length - 1)):
        inside = row < length - 1 if tap == 3 else row >= shift
        conv = conv + taps[tap : tap + 1] * jnp.where(inside, pltpu.roll(recur, shift, 0), 0.0)
    first = conv.astype(jnp.bfloat16)
    rest = conv - first.astype(jnp.float32)
    second = rest.astype(jnp.bfloat16)
    third = (rest - second.astype(jnp.float32)).astype(jnp.bfloat16)
    total = None
    for direction in range(2):
        logits = []
        for kind in range(2):
            weight = gate_ref[0, :, pl.ds((direction * 2 + kind) * width, width)]
            logits.append(
                jnp.dot(third, weight, preferred_element_type=jnp.float32)
                + jnp.dot(second, weight, preferred_element_type=jnp.float32)
                + jnp.dot(first, weight, preferred_element_type=jnp.float32)
            )
        rate = 1.0 / (1.0 + jnp.exp(-logits[0]))
        inlet = 1.0 / (1.0 + jnp.exp(-logits[1]))
        log_decay = rate * decay_ref[direction : direction + 1, :]
        inflow = conv * inlet * jnp.sqrt(minus_expm1(2.0 * log_decay))
        state = scan_block(jnp.exp(log_decay), inflow, direction == 1)
        total = state if total is None else total + state
    branch = branch_ref[...].astype(jnp.float32)
    inner = 0.7978845608028654 * (branch + 0.044715 * (branch * branch * branch))
    gelu = branch * (0.5 * (1.0 + jnp.tanh(inner)))
    out_ref[...] = (total * gelu * gain_ref[...]).astype(jnp.bfloat16)


def mixer(both_x, taps, rate_own, inlet_own, decay_own, gain_own):
    length, channels = both_x.shape[0], both_x.shape[1] // 2
    group = rate_own.shape[-1]
    lanes = min(channels, 2 * group)
    blocks = channels // lanes
    per = lanes // group

    def dense(weight):
        spread = weight.reshape(2, blocks, per, group, 1, group) * jnp.eye(per, dtype=weight.dtype)[:, None, :, None]
        return spread.reshape(2, blocks, lanes, lanes)

    both = jnp.stack([dense(rate_own), dense(inlet_own)], axis=1)
    gates = both.transpose(2, 3, 0, 1, 4).reshape(blocks, lanes, 4 * lanes)
    slope = -SHRINK * jax.nn.softplus(-decay_own)
    column = lambda j: (0, j)
    return pl.pallas_call(
        mixer_kernel,
        grid=(blocks,),
        out_shape=jax.ShapeDtypeStruct((length, channels), jnp.bfloat16),
        in_specs=[
            pl.BlockSpec((length, lanes), column),
            pl.BlockSpec((length, lanes), lambda j: (0, blocks + j)),
            pl.BlockSpec((taps.shape[0], lanes), column),
            pl.BlockSpec((1, lanes, 4 * lanes), lambda j: (j, 0, 0)),
            pl.BlockSpec((2, lanes), column),
            pl.BlockSpec((1, lanes), column),
        ],
        out_specs=pl.BlockSpec((length, lanes), column),
        cost_estimate=pl.CostEstimate(flops=int(3e9), bytes_accessed=2**20, transcendentals=2**21),
        compiler_params=pltpu.CompilerParams(vmem_limit_bytes=24 * 2**20),
    )(both_x, both_x, taps, gates, slope, gain_own.reshape(1, channels))


def on_device(
    order,
    tp_count,
    tokens,
    mixer_gain,
    recur_in,
    branch_in,
    conv_taps,
    recur_gate,
    input_gate,
    decay_param,
    recur_gain,
    recur_out,
    mixer_post,
    channel_gain,
    hidden_gate,
    hidden_up,
    hidden_down,
    channel_post,
):
    rank_tp = lax.axis_index("tp")
    feature_width = tokens.shape[1]
    model_width = mixer_gain.shape[0]
    channel_width = recur_in.shape[1]
    group_count = channel_width // recur_gate.shape[-1]
    feature_start = rank_tp * feature_width
    channel_start = rank_tp * channel_width

    ring = Ring(order)
    packed = jnp.concatenate([recur_in, branch_in, recur_out.reshape(recur_in.shape)], axis=1)
    mix_blocks, gate_blocks = ring.gather([packed, hidden_gate])
    in_blocks = [(source, block[:, : 2 * channel_width]) for source, block in mix_blocks]
    out_blocks = [
        (source, block[:, 2 * channel_width :].reshape(recur_out.shape)) for source, block in mix_blocks
    ]

    gathered_in = gather_features(tokens, tp_count)
    gathered_float = gathered_in.astype(jnp.float32)
    normed_in = rms_scale(gathered_float, mixer_gain).astype(jnp.bfloat16)
    both_x = jnp.dot(normed_in, stack_rows(in_blocks), preferred_element_type=jnp.float32).astype(jnp.bfloat16)

    taps = lax.dynamic_slice_in_dim(conv_taps, channel_start, channel_width, 1).astype(jnp.float32)
    group_start = rank_tp * group_count
    rate_own = lax.dynamic_slice_in_dim(recur_gate, group_start, group_count, 1)
    inlet_own = lax.dynamic_slice_in_dim(input_gate, group_start, group_count, 1)
    decay_own = lax.dynamic_slice_in_dim(decay_param, channel_start, channel_width, 1)
    gain_own = lax.dynamic_slice_in_dim(recur_gain, channel_start, channel_width, 0)
    recur_y = mixer(both_x, taps, rate_own, inlet_own, decay_own, gain_own)

    (up_blocks,) = ring.gather([hidden_up], lead=-1)
    branch_part = jnp.dot(recur_y, stack_columns(out_blocks), preferred_element_type=jnp.float32)
    branch_sum = sum_all(branch_part.astype(jnp.bfloat16), tp_count).astype(jnp.float32)
    mid_full = (gathered_float + rms_scale(branch_sum, mixer_post)).astype(jnp.bfloat16)
    mid_own = lax.dynamic_slice_in_dim(mid_full, feature_start, feature_width, 1)
    channel_in = rms_scale(mid_full.astype(jnp.float32), channel_gain).astype(jnp.bfloat16)

    gate_total = jnp.dot(channel_in, stack_rows(gate_blocks), preferred_element_type=jnp.float32)
    up_total = jnp.dot(channel_in, stack_rows(up_blocks), preferred_element_type=jnp.float32)
    hidden = (jax.nn.silu(gate_total) * up_total).astype(jnp.bfloat16)

    cut = max(hidden_down.shape[0] // 256, 1) * 128
    low_blocks, high_blocks = ring.gather(
        [hidden_down[:cut], hidden_down[cut:]], {4: hidden}, True
    )
    part_blocks = []
    for (source, low), (_, high) in zip(low_blocks, high_blocks):
        part = jnp.dot(hidden[:, :cut], low, preferred_element_type=jnp.float32)
        part = part + jnp.dot(hidden[:, cut:], high, preferred_element_type=jnp.float32)
        part_blocks.append((source, part.astype(jnp.bfloat16)))
    hidden_part = stack_columns(part_blocks)
    hidden_own = sum_own(hidden_part, tp_count)
    energy_own = jnp.sum(hidden_own * hidden_own, axis=1).reshape(-1, 128)
    hidden_energy = lax.psum(energy_own, "tp").reshape(-1)
    close_own = lax.dynamic_slice_in_dim(channel_post, feature_start, feature_width, 0)
    return (
        mid_own.astype(jnp.float32)
        + hidden_own * lax.rsqrt(hidden_energy / model_width + EPS)[:, None] * close_own
    ).astype(jnp.bfloat16)


PLANES = 4
ROWS = 2
CHIPS = 2
MESH = pl.DeviceIdType.MESH
LANES = 128


def pooled_fits(mesh, args):
    if mesh.shape["fs"] != PLANES * ROWS or mesh.shape["tp"] != CHIPS * CORES:
        return False
    spots = [getattr(device, "coords", None) for device in mesh.devices.reshape(-1)]
    if all(spot is not None for spot in spots):
        if list(mesh.axis_names) != ["fs", "tp"]:
            return False
        at = mesh.devices
        for f in range(PLANES * ROWS):
            for t in range(CHIPS * CORES):
                if tuple(at[f, t].coords) != (t // CORES, f % ROWS, f // ROWS):
                    return False
    tokens, gate, down, recur_in, recur_out = args[0], args[12], args[14], args[2], args[9]
    half = gate.shape[1] // 2
    return (
        tokens.shape[1] % LANES == 0
        and tokens.shape[0] % 16 == 0
        and gate.shape[0] % 16 == 0
        and half % LANES == LANES // 2
        and down.shape[0] == gate.shape[1]
        and recur_in.shape[1] % LANES == 0
        and recur_out.shape[1] % LANES == 0
        and LANES % args[5].shape[-1] == 0
    )


class Wires:
    def __init__(self, sends, lands, nobody):
        self.sends = sends
        self.lands = lands
        self.nobody = nobody
        self.names = {}
        self.started = []

    def index(self, name):
        return self.names.setdefault(name, len(self.names))

    def send(self, name, source, target, to, land=None, only=None):
        copy = pltpu.make_async_remote_copy(
            src_ref=source,
            dst_ref=target,
            send_sem=self.sends.at[self.index(name)],
            recv_sem=self.lands.at[self.index(land or name)],
            device_id=to,
            device_id_type=MESH,
        )
        guarded(only, copy.start)
        self.started.append((only, copy))

    def wait(self, name, target):
        at = self.lands.at[self.index(name)]
        with jax.named_scope("wait_" + name):
            pltpu.make_async_remote_copy(
                src_ref=target,
                dst_ref=target,
                send_sem=at,
                recv_sem=at,
                device_id=self.nobody,
                device_id_type=MESH,
            ).wait_recv()

    def finish(self):
        with jax.named_scope("finish"):
            for only, copy in self.started:
                guarded(only, copy.wait_send)


def guarded(only, action):
    if only is None:
        action()
    else:
        pl.when(only)(action)


def scan_pair(conv, logits, slope, reverse):
    rate = 1.0 / (1.0 + jnp.exp(-logits[0]))
    inlet = 1.0 / (1.0 + jnp.exp(-logits[1]))
    log_decay = rate * slope
    inflow = conv * inlet * jnp.sqrt(minus_expm1(2.0 * log_decay))
    return scan_block(jnp.exp(log_decay), inflow, reverse)


def log_one_plus(value):
    total = 1.0 + value
    exact = total == 1.0
    return jnp.where(exact, value, jnp.log(total) * (value / jnp.where(exact, 1.0, total - 1.0)))


def pooled_kernel(
    tokens,
    mixer_gain,
    recur_in,
    branch_in,
    conv_taps,
    recur_gate,
    input_gate,
    decay_param,
    recur_gain,
    recur_out,
    mixer_post,
    channel_gain,
    hidden_gate,
    hidden_up,
    hidden_down,
    channel_post,
    out,
    tok,
    normed,
    w_in,
    both_x,
    gates_raw,
    gates,
    recur_all,
    w_out,
    branch,
    mid,
    channel_in,
    edge,
    w_gate_up,
    other_gate_up,
    hidden,
    w_down,
    other_down,
    part,
    part_in,
    chip_send,
    chip_in,
    own_sum,
    plane_send,
    plane_in,
    early_send,
    early_in,
    energy,
    sends,
    lands,
    local,
):
    f = lax.axis_index("fs")
    t = lax.axis_index("tp")
    z, y = lax.div(f, ROWS), lax.rem(f, ROWS)
    x, c = lax.div(t, CORES), lax.rem(t, CORES)
    zi, zp = lax.rem(z, 2), lax.div(z, 2)
    planes = [z, z + 1 - 2 * zi, lax.rem(z + 2, PLANES), PLANES - 1 - z]
    is_mid = lax.div(lax.rem(z + 1, PLANES), 2) == 1
    is_end = lax.div(lax.rem(z + 1, PLANES), 2) == 0
    length, width = tokens.shape
    depth = recur_in.shape[0]
    channels = recur_in.shape[1]
    units = hidden_gate.shape[1]
    half = units // 2
    wide = half // LANES * LANES
    narrow = half - wide
    full = wide // LANES
    model = tok.shape[0] * width
    group = recur_gate.shape[-1]
    blocks = PLANES * ROWS

    def device(plane, row, chip, core):
        return {"fs": plane * ROWS + row, "tp": chip * CORES + core}

    def block(k, row):
        return planes[k] * ROWS + row

    near_y = device(z, 1 - y, x, c)
    near_x = device(z, y, 1 - x, c)
    far_x = device(z, y, 1 - x, 1 - c)
    near_c = device(z, y, x, 1 - c)
    plane_of = [None] + [device(planes[k], y, x, c) for k in (1, 2, 3)]
    t_c = x * CORES + 1 - c
    t_x = (1 - x) * CORES + c
    t_xc = (1 - x) * CORES + 1 - c
    wires = Wires(sends, lands, near_c)
    rows_of = lambda at, size: pl.ds(pl.multiple_of(at * size, size), size)

    moves = {}

    def move(name, source, target):
        copy = pltpu.make_async_copy(source, target, local.at[len(moves)])
        copy.start()
        moves[name] = copy

    def here(prefix):
        for name, copy in moves.items():
            if name.startswith(prefix):
                copy.wait()

    move("io0", recur_in, w_in.at[rows_of(f, depth), pl.ds(0, channels)])
    move("io1", branch_in, w_in.at[rows_of(f, depth), pl.ds(channels, channels)])
    move("io2", recur_out, w_out.at[f, rows_of(t, channels), :])
    move("tok", tokens, tok.at[t])
    columns = lambda at: pl.ds(pl.multiple_of(at, LANES), LANES)
    for side, target, row_at, parity in (("a", w_gate_up, f, zi), ("b", other_gate_up, 0, 1 - zi)):
        for n in range(full):
            start = parity * (units - wide) + n * LANES
            for m, weight in enumerate((hidden_gate, hidden_up)):
                move(
                    f"gu{side}{n}{m}",
                    weight.at[:, columns(start)],
                    target.at[rows_of(row_at, depth), pl.ds((2 * n + m) * LANES, LANES)],
                )
    move("gum0", hidden_gate.at[:, pl.ds(wide, LANES)], edge.at[0])
    move("gum1", hidden_up.at[:, pl.ds(wide, LANES)], edge.at[1])
    group_count = channels // group
    move("gate0", recur_gate.at[:, rows_of(t, group_count)], gates_raw.at[0])
    move("gate1", input_gate.at[:, rows_of(t, group_count)], gates_raw.at[1])
    for side, target, parity in (("a", w_down.at[f], zi), ("b", other_down, 1 - zi)):
        wide_at = pl.multiple_of(parity * (units - wide), 2 * narrow)
        narrow_at = pl.multiple_of(wide + parity * narrow, narrow)
        move(f"dn{side}0", hidden_down.at[pl.ds(wide_at, wide), :], target.at[pl.ds(0, wide), :])
        move(f"dn{side}1", hidden_down.at[pl.ds(narrow_at, narrow), :], target.at[pl.ds(wide, narrow), :])

    barrier = pltpu.get_barrier_semaphore()
    peers = [near_y, near_x, far_x, near_c] + plane_of[1:]
    for peer in peers:
        pl.semaphore_signal(barrier, inc=1, device_id=peer, device_id_type=MESH)
    with jax.named_scope("barrier"):
        pl.semaphore_wait(barrier, len(peers))

    def in_slot(k, row):
        return w_in.at[rows_of(block(k, row), depth), :]

    def out_slot(k, row):
        return w_out.at[block(k, row), rows_of(t, channels), :]

    part_rows = depth // 2

    def gate_slot(k, row, piece):
        at = pl.multiple_of(block(k, row) * depth + piece * part_rows, part_rows)
        return w_gate_up.at[pl.ds(at, part_rows), :]

    def other_slot(piece):
        return other_gate_up.at[pl.ds(piece * part_rows, part_rows), :]

    def down_slot(k, row):
        return w_down.at[block(k, row), pl.ds(0, half), :]

    down_other = other_down

    slots = {"i": in_slot, "o": out_slot}

    def mixer_to_y(kind, k):
        slot = slots[kind](k, y)
        wires.send(f"{kind}y{k}", slot, slot, near_y)

    def mixer_to_x(k, row, tag):
        wires.send(f"ox{tag}{k}", out_slot(k, row), out_slot(k, row), near_x)

    def mixer_to_z(kind, name, k, to, land, only=None):
        slot = slots[kind](k, y)
        wires.send(kind + name, slot, slot, to, f"{kind}z{land}", only)

    def mixer_wait(kind, k, only=None):
        guarded(only, lambda: wires.wait(f"{kind}z{k}", slots[kind](k, y)))

    late_at = {
        "s": jnp.where(is_mid, planes[3], planes[2]) * ROWS,
        "t": jnp.where(is_mid, planes[2], planes[3]) * ROWS,
    }

    def late_slot(kind, tag, row):
        at = late_at[tag] + row
        if kind == "i":
            return w_in.at[rows_of(at, depth), :]
        return w_out.at[at, rows_of(t, channels), :]

    def late_to_y(kind, tag):
        slot = late_slot(kind, tag, y)
        wires.send(f"{kind}y{tag}", slot, slot, near_y)

    def late_to_x(tag, row, side):
        slot = late_slot("o", tag, row)
        wires.send(f"ox{side}{tag}", slot, slot, near_x)

    def gate_own_to_z(piece, which, only):
        if which == 1:
            wires.send(f"g{piece}s1", gate_slot(0, y, piece), gate_slot(0, y, piece), plane_of[2], f"gz{piece}2", only)
        else:
            k = 1 if which == 2 else 3
            source = other_slot(piece)
            wires.send(f"g{piece}s{which}", source, gate_slot(0, y, piece), plane_of[k], f"gz{piece}{k}", only)

    def down_own_to_z(which, only):
        if which == 1:
            wires.send("ds1", down_slot(0, y), down_slot(0, y), plane_of[2], "dz2", only)
        else:
            k = 1 if which == 2 else 3
            wires.send(f"ds{which}", down_other, down_slot(0, y), plane_of[k], f"dz{k}", only)

    def gate_to_y(k, piece):
        wires.send(f"gy{piece}{k}", gate_slot(k, y, piece), gate_slot(k, y, piece), near_y)

    def down_to_y(k):
        wires.send(f"dy{k}", down_slot(k, y), down_slot(k, y), near_y)

    def gate_pass(k, piece, only=None):
        guarded(only, lambda: wires.wait(f"gz{piece}{k}", gate_slot(k, y, piece)))
        if k == 1:
            passing = is_mid if only is None else only
            if passing is is_mid:
                slot = gate_slot(1, y, piece)
                wires.send(f"g{piece}r", slot, slot, plane_of[2], f"gz{piece}3", is_mid)
        slot = gate_slot(k, y, piece)
        wires.send(f"gy{piece}{k}", slot, slot, near_y, only=only)

    fine_width = depth // 2
    halves = ((0, fine_width), (fine_width, fine_width))
    whole = ((0, depth),)

    def down_piece(k, row, at, size):
        return w_down.at[block(k, row), pl.ds(0, half), pl.ds(at, size)]

    def down_come(k, only=None):
        guarded(only, lambda: wires.wait(f"dz{k}", down_slot(k, y)))

    def down_on(k, only=None):
        for at, size in halves if k == 1 else whole:
            slot = down_piece(k, y, at, size)
            wires.send(f"dy{k}{at}", slot, slot, near_y, only=only)

    def down_pass(k, only=None):
        down_come(k, only)
        down_on(k, only)

    here("io0")
    here("io1")
    mixer_to_y("i", 0)
    mixer_to_z("i", "z1", 0, plane_of[1], 1)
    mixer_to_z("i", "z3", 0, plane_of[3], 3, is_mid)
    here("tok")
    wires.send("tc", tok.at[t], tok.at[t], near_c)
    wires.send("tx", tok.at[t], tok.at[t], near_x)
    here("io2")
    mixer_to_y("o", 0)
    mixer_to_z("o", "z1", 0, plane_of[1], 1)
    mixer_to_z("o", "z3", 0, plane_of[3], 3, is_mid)

    here("gum")
    lane = lax.broadcasted_iota(jnp.int32, edge.shape[1:], 1)
    edge_gate = edge[0].astype(jnp.float32)
    edge_up = edge[1].astype(jnp.float32)
    low = jnp.where(lane < narrow, edge_gate, pltpu.roll(edge_up, narrow, 1))
    high = jnp.where(lane < narrow, pltpu.roll(edge_gate, narrow, 1), edge_up)
    odd = zi == 1
    edge_at = pl.ds(2 * wide, LANES)
    w_gate_up[rows_of(f, depth), edge_at] = jnp.where(odd, high, low).astype(jnp.bfloat16)
    other_gate_up[:, edge_at] = jnp.where(odd, low, high).astype(jnp.bfloat16)
    w_down[:, pl.ds(half, LANES - narrow), :] = jnp.zeros((blocks, LANES - narrow, w_down.shape[2]), jnp.bfloat16)
    here("gua")
    here("gub")

    gate_own_to_z(0, 2, is_end)
    gate_own_to_z(1, 2, is_end)

    mixer_wait("i", 1)
    mixer_to_z("i", "r1", 1, plane_of[3], 2, is_mid)
    mixer_to_y("i", 1)
    gate_to_y(0, 0)
    mixer_wait("i", 3, is_mid)
    mixer_to_z("i", "r3", 3, plane_of[1], 2, is_mid)

    wires.wait("tx", tok.at[t_x])
    wires.send("txc", tok.at[t_x], tok.at[t_x], near_c)

    mixer_wait("o", 1)
    mixer_to_z("o", "r1", 1, plane_of[3], 2, is_mid)
    gate_own_to_z(0, 3, is_mid)
    mixer_wait("i", 2)
    late_to_y("i", "s")
    mixer_to_z("i", "r2", 2, plane_of[1], 3, is_mid)
    mixer_wait("o", 3, is_mid)
    mixer_to_z("o", "r3", 3, plane_of[1], 2, is_mid)
    mixer_to_x(0, y, "a")
    here("gate")
    per = LANES // group
    runs = channels // LANES
    for j in range(runs):
        for direction in range(2):
            for kind in range(2):
                dense = None
                for a in range(per):
                    spread_row = lax.broadcasted_iota(jnp.int32, (group, LANES), 0)
                    spread_lane = lax.broadcasted_iota(jnp.int32, (group, LANES), 1)
                    spread = (spread_lane == spread_row + a * group).astype(jnp.bfloat16)
                    lift_row = lax.broadcasted_iota(jnp.int32, (LANES, group), 0)
                    lift_lane = lax.broadcasted_iota(jnp.int32, (LANES, group), 1)
                    lift = (lift_row == lift_lane + a * group).astype(jnp.bfloat16)
                    block_map = gates_raw[kind, direction, j * per + a]
                    block_map = jnp.dot(block_map, spread, preferred_element_type=jnp.float32).astype(jnp.bfloat16)
                    block_map = jnp.dot(lift, block_map, preferred_element_type=jnp.float32)
                    dense = block_map if dense is None else dense + block_map
                gates[j, :, pl.ds((direction * 2 + kind) * LANES, LANES)] = dense.astype(jnp.bfloat16)

    mixer_wait("i", 3, is_end)
    late_to_y("i", "t")
    mixer_to_y("o", 1)
    mixer_wait("o", 2)
    late_to_y("o", "s")
    mixer_to_z("o", "r2", 2, plane_of[1], 3, is_mid)
    gate_own_to_z(0, 2, is_mid)
    gate_own_to_z(0, 1, None)
    gate_pass(1, 0, is_mid)
    wires.wait("tc", tok.at[t_c])
    wires.wait("txc", tok.at[t_xc])
    fine = 16

    with jax.named_scope("norm"):

        @pl.loop(0, length // fine, unroll=2)
        def _(r):
            rows = rows_of(r, fine)
            values = jnp.concatenate([tok[i, rows, :] for i in range(tok.shape[0])], axis=1).astype(jnp.float32)
            normed[rows, :] = rms_scale(values, mixer_gain[...]).astype(jnp.bfloat16)

    mixer_wait("o", 3, is_end)
    late_to_y("o", "t")
    gate_to_y(0, 1)
    gate_own_to_z(1, 2, is_mid)
    gate_own_to_z(1, 3, is_mid)
    gate_own_to_z(1, 1, None)
    here("dn")
    down_own_to_z(2, is_end)
    gate_pass(1, 1, is_mid)
    wires.wait("oy0", out_slot(0, 1 - y))
    mixer_to_x(0, 1 - y, "b")
    mixer_to_x(1, y, "a")
    for k in (0, 1):
        wires.wait(f"iy{k}", in_slot(k, 1 - y))
    for tag in ("s", "t"):
        wires.wait(f"iy{tag}", late_slot("i", tag, 1 - y))

    with jax.named_scope("in_proj"):

        @pl.loop(0, 2)
        def _(j):
            at = rows_of(j, channels)
            product = jnp.dot(normed[...], w_in[:, at], preferred_element_type=jnp.float32)
            both_x[:, at] = product.astype(jnp.bfloat16)


    own_channels = pl.multiple_of(t * channels, LANES)

    with jax.named_scope("scan"):

        @pl.loop(0, runs)
        def _(j):
            at = pl.ds(pl.multiple_of(j * LANES, LANES), LANES)
            gate_at = pl.ds(pl.multiple_of(channels + j * LANES, LANES), LANES)
            table_at = pl.ds(pl.multiple_of(own_channels + j * LANES, LANES), LANES)
            recur = both_x[:, at].astype(jnp.float32)
            row = lax.broadcasted_iota(jnp.int32, recur.shape, 0)
            taps = conv_taps[:, table_at].astype(jnp.float32)
            conv = taps[2:3] * recur
            for tap, shift in ((0, 2), (1, 1), (3, length - 1)):
                inside = row < length - 1 if tap == 3 else row >= shift
                conv = conv + taps[tap : tap + 1] * jnp.where(inside, pltpu.roll(recur, shift, 0), 0.0)
            first = conv.astype(jnp.bfloat16)
            rest = conv - first.astype(jnp.float32)
            second_part = rest.astype(jnp.bfloat16)
            third_part = (rest - second_part.astype(jnp.float32)).astype(jnp.bfloat16)
            decay = decay_param[:, table_at]
            slope = -SHRINK * (jnp.maximum(-decay, 0.0) + log_one_plus(jnp.exp(-jnp.abs(decay))))
            total = None
            for direction in range(2):
                logits = []
                for kind in range(2):
                    weight = gates[j, :, pl.ds((direction * 2 + kind) * LANES, LANES)]
                    logits.append(
                        jnp.dot(third_part, weight, preferred_element_type=jnp.float32)
                        + jnp.dot(second_part, weight, preferred_element_type=jnp.float32)
                        + jnp.dot(first, weight, preferred_element_type=jnp.float32)
                    )
                state = scan_pair(conv, logits, slope[direction : direction + 1], direction == 1)
                total = state if total is None else total + state
            value = both_x[:, gate_at].astype(jnp.float32)
            inner = 0.7978845608028654 * (value + 0.044715 * (value * value * value))
            gelu = value * (0.5 * (1.0 + jnp.tanh(inner)))
            recur_all[:, table_at] = (total * gelu * recur_gain[:, table_at]).astype(jnp.bfloat16)

    mine = recur_all.at[:, rows_of(t, channels)]
    wires.send("rx", mine, mine, near_x)
    wires.send("rc", mine, mine, near_c)
    wires.wait("oy1", out_slot(1, 1 - y))
    mixer_to_x(1, 1 - y, "b")
    late_to_x("s", y, "a")
    late_to_x("t", y, "a")
    gate_pass(1, 0, is_end)
    wires.send("dy00", down_slot(0, y), down_slot(0, y), near_y, only=is_end)
    gate_pass(3, 0, is_mid)
    for tag in ("s", "t"):
        wires.wait(f"oy{tag}", late_slot("o", tag, 1 - y))
        late_to_x(tag, 1 - y, "b")
    wires.send("oc1", w_out.at[:, rows_of(t, channels), :], w_out.at[:, rows_of(t, channels), :], near_c)
    for k in (0, 1):
        for side, row in (("a", y), ("b", 1 - y)):
            wires.wait(f"ox{side}{k}", w_out.at[block(k, row), rows_of(t_x, channels), :])
    for tag in ("s", "t"):
        for side, row in (("a", y), ("b", 1 - y)):
            wires.wait(f"ox{side}{tag}", w_out.at[late_at[tag] + row, rows_of(t_x, channels), :])
    wires.send("oc2", w_out.at[:, rows_of(t_x, channels), :], w_out.at[:, rows_of(t_x, channels), :], near_c)
    theirs = recur_all.at[:, rows_of(t_x, channels)]
    wires.wait("rx", theirs)
    wires.send("rxc", theirs, theirs, near_c)
    wires.wait("oc1", w_out.at[:, rows_of(t_c, channels), :])
    wires.wait("oc2", w_out.at[:, rows_of(t_xc, channels), :])
    wires.wait("rc", recur_all.at[:, rows_of(t_c, channels)])
    wires.wait("rxc", recur_all.at[:, rows_of(t_xc, channels)])

    gate_pass(2, 0, is_end)
    with jax.named_scope("branch_dot"):

        @pl.loop(0, blocks)
        def _(b):
            branch[:, rows_of(b, depth)] = jnp.dot(recur_all[...], w_out[b], preferred_element_type=jnp.float32)

    def quarter(s, at, piece):
        return channel_in.at[s, pl.ds(piece * (length // 2), length // 2), rows_of(at, width)]

    for piece in range(2):
        with jax.named_scope(f"branch_norm{piece}"):

            @pl.loop(piece * length // 2 // fine, (piece + 1) * length // 2 // fine, unroll=2)
            def _(r):
                rows = rows_of(r, fine)
                values = jnp.concatenate([tok[i, rows, :] for i in range(tok.shape[0])], axis=1).astype(jnp.float32)
                middle = (values + rms_scale(branch[rows, :], mixer_post[...])).astype(jnp.bfloat16)
                mid[rows, :] = middle
                channel_in[0, rows, :] = rms_scale(middle.astype(jnp.float32), channel_gain[...]).astype(jnp.bfloat16)

        wires.send(f"cz{piece}", quarter(0, t, piece), quarter(1, t, piece), plane_of[1])

    down_own_to_z(2, is_mid)
    gate_pass(2, 0, is_mid)
    gate_pass(1, 1, is_end)
    gate_pass(3, 1, is_mid)
    gate_pass(3, 0, is_end)
    down_own_to_z(3, is_mid)
    down_own_to_z(1, is_end)
    wires.wait("cz0", quarter(1, t, 0))
    wires.send("cx0", quarter(1, t, 0), quarter(1, t, 0), near_x)
    wires.send("cca0", quarter(1, t, 0), quarter(1, t, 0), near_c)
    gate_pass(2, 1)
    wires.wait("cz1", quarter(1, t, 1))
    wires.send("cx1", quarter(1, t, 1), quarter(1, t, 1), near_x)
    wires.send("cca1", quarter(1, t, 1), quarter(1, t, 1), near_c)
    gate_pass(3, 1, is_end)
    wires.send("dy00", down_slot(0, y), down_slot(0, y), near_y, only=is_mid)
    for piece in range(2):
        wires.wait(f"cx{piece}", quarter(1, t_x, piece))
        wires.send(f"ccb{piece}", quarter(1, t_x, piece), quarter(1, t_x, piece), near_c)
    for piece in range(2):
        wires.wait(f"cca{piece}", quarter(1, t_c, piece))
        wires.wait(f"ccb{piece}", quarter(1, t_xc, piece))
    down_own_to_z(1, is_mid)
    down_come(1, is_mid)
    wires.send("dr", down_slot(1, y), down_slot(1, y), plane_of[2], "dz3", is_mid)
    down_come(3, is_mid)
    down_pass(2, is_mid)
    down_on(3, is_mid)
    down_on(1, is_mid)
    down_pass(2, is_end)
    for k in range(PLANES):
        for piece in range(2):
            wires.wait(f"gy{piece}{k}", gate_slot(k, 1 - y, piece))

    def gate_up(first, last):
        with jax.named_scope(f"gate_up{first}"):

            @pl.loop(first, last)
            def _(n):
                at = pl.ds(pl.multiple_of(n * 2 * LANES, 2 * LANES), 2 * LANES)
                store = pl.ds(pl.multiple_of(n * LANES, LANES), LANES)
                for s in range(2):
                    product = jnp.dot(channel_in[s], w_gate_up[:, at], preferred_element_type=jnp.float32)
                    gate_value, up_value = product[:, :LANES], product[:, LANES:]
                    hidden[s, :, store] = (jax.nn.silu(gate_value) * up_value).astype(jnp.bfloat16)

    gate_up(0, full - 1)
    down_pass(3, is_end)
    gate_up(full - 1, full)

    lane_tail = lax.broadcasted_iota(jnp.int32, (length, LANES), 1)
    for s in range(2):
        product = jnp.dot(channel_in[s], w_gate_up[:, edge_at], preferred_element_type=jnp.float32)
        value = jax.nn.silu(product) * pltpu.roll(product, narrow, 1)
        hidden[s, :, pl.ds(wide, LANES)] = jnp.where(lane_tail < narrow, value, 0.0).astype(jnp.bfloat16)

    mine_odd = lax.rem(zi + c, 2)
    mine_late = lax.rem(zp + x, 2)

    def pieces(kk, late):
        return halves if kk == 0 and late else whole

    def products(k, late, at, size):
        row = 1 - y if late else y
        with jax.named_scope(f"products{k}{late}"):
            for s in range(2):
                weight = w_down[block(k, row), :, pl.ds(at, size)]
                value = jnp.dot(hidden[s], weight, preferred_element_type=jnp.float32)
                part[k, late, s, :, pl.ds(at, size)] = value.astype(jnp.bfloat16)
        kk = k // 2
        for start, share in pieces(kk, late):
            if at <= start < at + size:
                columns = pl.ds(start, share)
                wires.send(
                    f"pc{k}{late}{start}",
                    part.at[k, late, :, :, columns],
                    part_in.at[kk, late, :, :, columns],
                    near_c,
                    f"pc{kk}{late}{start}",
                    mine_odd != k % 2,
                )

    def chip_sum(kk, late, at, size, only=None):
        columns = pl.ds(at, size)

        def run():
            wires.wait(f"pc{kk}{late}{at}", part_in.at[kk, late, :, :, columns])
            with jax.named_scope(f"chip_sum{kk}{late}"):
                kept = 2 * kk + mine_odd
                give = part[kept, late, 1, :, columns].astype(jnp.float32)
                give = give + part_in[kk, late, 1, :, columns].astype(jnp.float32)
                plane_send[kk, late, :, columns] = give.astype(jnp.bfloat16)

        guarded(only, run)
        tag = "" if only is None else "e" if only is even else "o"
        wires.send(
            f"pz{kk}{late}{at}{tag}",
            plane_send.at[kk, late, :, columns],
            plane_in.at[kk, late, :, columns],
            plane_of[1],
            f"pz{kk}{late}{at}",
            only,
        )

    def plane_sum(kk, late, at, size):
        columns = pl.ds(at, size)
        wires.wait(f"pz{kk}{late}{at}", plane_in.at[kk, late, :, columns])
        kept = 2 * kk + mine_odd
        with jax.named_scope(f"plane_sum{kk}{late}"):
            value = part[kept, late, 0, :, columns].astype(jnp.float32)
            value = value + part_in[kk, late, 0, :, columns].astype(jnp.float32)
            value = value + plane_in[kk, late, :, columns].astype(jnp.float32)

            def keep():
                own_sum[late, :, columns] = value

            def hand():
                chip_send[late, :, columns] = value.astype(jnp.bfloat16)

            pl.when(mine_late == kk)(keep)
            pl.when(mine_late != kk)(hand)
        for start, share in halves if late else whole:
            if at <= start < at + size:
                share_at = pl.ds(start, share)
                wires.send(
                    f"px{kk}{late}{start}",
                    chip_send.at[late, :, share_at],
                    chip_in.at[late, :, share_at],
                    near_x,
                    f"px{late}{start}",
                    mine_late != kk,
                )

    def pair_sum(kk, s):
        kept = 2 * kk + mine_odd
        return part[kept, 0, s].astype(jnp.float32) + part_in[kk, 0, s].astype(jnp.float32)

    def chip_give(kk):
        def run():
            wires.wait(f"pc{kk}00", part_in.at[kk, 0])
            with jax.named_scope(f"chip_give{kk}"):
                for s in range(2):
                    early_send[s] = pair_sum(kk, s).astype(jnp.bfloat16)

        passing = mine_late != kk
        pl.when(passing)(run)
        wires.send(f"px{kk}0", early_send, early_in, near_x, "px00", passing)

    def chip_take(kk):
        def run():
            wires.wait(f"pc{kk}00", part_in.at[kk, 0])
            wires.wait("px00", early_in)
            with jax.named_scope(f"chip_take{kk}"):
                own_sum[0] = pair_sum(kk, 0) + early_in[0].astype(jnp.float32)
                plane_send[1 - kk, 0] = (pair_sum(kk, 1) + early_in[1].astype(jnp.float32)).astype(jnp.bfloat16)

        taking = mine_late == kk
        pl.when(taking)(run)
        wires.send(f"pz{kk}0", plane_send.at[1 - kk, 0], plane_in.at[0, 0], plane_of[1], "pz00", taking)

    def down_wait(k):
        for at, size in halves if k == 1 else whole:
            wires.wait(f"dy{k}{at}", down_piece(k, 1 - y, at, size))

    even = mine_odd == 0
    uneven = mine_odd == 1
    all_of = (0, depth)
    products(0, 0, *all_of)
    products(2, 0, *all_of)
    products(3, 0, *all_of)
    down_pass(1, is_end)
    chip_give(1)
    products(1, 0, *all_of)
    chip_give(0)
    down_wait(0)
    products(0, 1, *all_of)
    for at, size in halves:
        chip_sum(0, 1, at, size, even)
    down_wait(2)
    products(2, 1, *all_of)
    down_wait(3)
    products(3, 1, *all_of)
    chip_sum(1, 1, *all_of)
    for at, size in halves:
        wires.wait(f"dy1{at}", down_piece(1, 1 - y, at, size))
        products(1, 1, at, size)
        chip_sum(0, 1, at, size, uneven)
    chip_take(1)
    chip_take(0)
    plane_sum(1, 1, *all_of)
    for at, size in halves:
        plane_sum(0, 1, at, size)

    line = None
    for late, (start, share) in [(0, whole[0]), (1, halves[0]), (1, halves[1])]:
        columns = pl.ds(start, share)
        if late:
            arrived = chip_in.at[late, :, columns]
            wires.wait(f"px{late}{start}", arrived)
        else:
            arrived = plane_in.at[0, 0]
            wires.wait("pz00", arrived)
        with jax.named_scope(f"own_sum{late}"):
            total = own_sum[late, :, columns] + arrived[...].astype(jnp.float32)
            own_sum[late, :, columns] = total
            square = total * total
            folded = square[:, :LANES]
            for n in range(1, share // LANES):
                folded = folded + square[:, n * LANES : (n + 1) * LANES]
            found = jnp.sum(folded.T, axis=0, keepdims=True)
            line = found if line is None else line + found
    energy[t] = jnp.broadcast_to(line, energy.shape[1:])
    wires.send("ex", energy.at[t], energy.at[t], near_x)
    wires.send("exc", energy.at[t], energy.at[t], far_x)
    wires.send("ec", energy.at[t], energy.at[t], near_c)
    wires.wait("ex", energy.at[t_x])
    wires.wait("exc", energy.at[t_xc])
    wires.wait("ec", energy.at[t_c])
    line = energy[0, 0:1, :]
    for i in range(1, energy.shape[0]):
        line = line + energy[i, 0:1, :]
    with jax.named_scope("last"):
        scale = jnp.broadcast_to(lax.rsqrt(line / model + EPS), (LANES, length)).T
        for late, row in ((0, y), (1, 1 - y)):
            for n in range(depth // LANES):
                at = pl.ds(pl.multiple_of(row * depth + n * LANES, LANES), LANES)
                wide_at = pl.ds(pl.multiple_of(t * width + row * depth + n * LANES, LANES), LANES)
                value = own_sum[late, :, pl.ds(n * LANES, LANES)] * scale * channel_post[:, wide_at]
                out[:, at] = (mid[:, wide_at].astype(jnp.float32) + value).astype(jnp.bfloat16)
    wires.finish()


def pooled(*args):
    tokens, mixer_gain, recur_in, recur_gate, recur_out = args[0], args[1], args[2], args[5], args[9]
    hidden_gate, hidden_down = args[12], args[14]
    length, width = tokens.shape
    depth, channels = recur_in.shape
    model = mixer_gain.shape[0]
    units = hidden_gate.shape[1]
    half = units // 2
    padded = half // LANES * LANES + LANES
    blocks = PLANES * ROWS
    shares = CHIPS * CORES
    group = recur_gate.shape[-1]
    runs = channels // LANES
    bf16, f32 = jnp.bfloat16, jnp.float32
    anywhere = pl.BlockSpec(memory_space=pl.ANY)
    vmem = pl.BlockSpec(memory_space=pltpu.VMEM)
    small = (1, 4, 7, 8, 10, 11, 15)
    args = [arg.reshape(1, -1) if arg.ndim == 1 else arg for arg in args]
    scratch = [
        pltpu.VMEM((shares, length, width), bf16),
        pltpu.VMEM((length, model), bf16),
        pltpu.VMEM((model, 2 * channels), bf16),
        pltpu.VMEM((length, 2 * channels), bf16),
        pltpu.VMEM((2, 2, channels // group, group, group), bf16),
        pltpu.VMEM((runs, LANES, 4 * LANES), bf16),
        pltpu.VMEM((length, shares * channels), bf16),
        pltpu.VMEM((blocks, shares * channels, recur_out.shape[1]), bf16),
        pltpu.VMEM((length, model), f32),
        pltpu.VMEM((length, model), bf16),
        pltpu.VMEM((2, length, model), bf16),
        pltpu.VMEM((2, depth, LANES), bf16),
        pltpu.VMEM((model, units), bf16),
        pltpu.VMEM((depth, units), bf16),
        pltpu.VMEM((2, length, padded), bf16),
        pltpu.VMEM((blocks, padded, hidden_down.shape[1]), bf16),
        pltpu.VMEM((half, hidden_down.shape[1]), bf16),
        pltpu.VMEM((PLANES, 2, 2, length, depth), bf16),
        pltpu.VMEM((2, 2, 2, length, depth), bf16),
        pltpu.VMEM((2, length, depth), bf16),
        pltpu.VMEM((2, length, depth), bf16),
        pltpu.VMEM((2, length, depth), f32),
        pltpu.VMEM((2, 2, length, depth), bf16),
        pltpu.VMEM((2, 2, length, depth), bf16),
        pltpu.VMEM((2, length, depth), bf16),
        pltpu.VMEM((2, length, depth), bf16),
        pltpu.VMEM((shares, 8, length), f32),
        pltpu.SemaphoreType.DMA((128,)),
        pltpu.SemaphoreType.DMA((128,)),
        pltpu.SemaphoreType.DMA((40,)),
    ]
    return pl.pallas_call(
        pooled_kernel,
        out_shape=jax.ShapeDtypeStruct((length, width), bf16),
        in_specs=[vmem if index in small else anywhere for index in range(len(args))],
        out_specs=vmem,
        scratch_shapes=scratch,
        compiler_params=pltpu.CompilerParams(
            collective_id=0, has_side_effects=True, vmem_limit_bytes=63 * 2**20
        ),
    )(*args)


def solution(mesh):
    in_specs = (
        P("fs", "tp"),
        P(),
        P("fs", "tp"),
        P("fs", "tp"),
        P(),
        P(),
        P(),
        P(),
        P(),
        P("tp", "fs"),
        P(),
        P(),
        P("fs", "tp"),
        P("fs", "tp"),
        P("tp", "fs"),
        P(),
    )
    out_specs = P("fs", "tp")

    def body(*args):
        if pooled_fits(mesh, args):
            return pooled(*args)
        return on_device(snake_order(mesh), mesh.shape["tp"], *args)

    return jax.shard_map(body, mesh=mesh, in_specs=in_specs, out_specs=out_specs, check_vma=False)
```
